128 devices in a mesh: sp: 16 (over z, y), dp: 8 (over x, core).
Axes of the slice: x: 4, y: 4, z: 4, core: 2. Of those that a mesh axis runs over, the one named last changes fastest.
Arguments:
- skip_connection_stream: bfloat16 [8, 2048, 2048], P('dp', 'sp'), may hold values from -6 to 6
- emitted_valve_unscaled: bfloat16 [8, 2048, 1024], P('dp', 'sp'), may hold values from -6 to 6
- channel_source_mapped: bfloat16 [8, 2048, 1024], P('dp', 'sp'), may hold values from -6 to 6
- hidden_source_mapped: bfloat16 [8, 2048, 256], P('dp', 'sp'), may hold values from -6 to 6
- probe_mapped_values: bfloat16 [8, 2048, 256], P('dp', 'sp'), may hold values from -6 to 6
- increment_premapped: float32 [8, 2048, 16], P('dp', None, 'sp'), may hold values from -6 to 6
- extra_log_fading: float32 [8, 2048, 16], P('dp', None, 'sp'), may hold values from -2 to 0
- channel_fading_speed: float32 [16], replicated, may hold values from 0 to 1, as said below
- channel_source_kernel: float32 [4, 1024], replicated, may hold values from -3 to 3
- hidden_source_kernel: float32 [4, 256], replicated, may hold values from -3 to 3
- probe_kernel_coefficients: float32 [4, 256], replicated, may hold values from -3 to 3
- cluster_scaling_factor: float32 [1024], replicated, may hold values from 0.1 to 1.9
- emitted_mapping_matrix: bfloat16 [1024, 2048], replicated, may hold values from -0.1875 to 0.1875
- standardize_scaling: float32 [2048], replicated, may hold values from 0.1 to 1.9
- standardize_offset: float32 [2048], replicated, may hold values from -2 to 2
- chosen_specialist_ids: int32 [8, 2048, 2], P('dp', 'sp'), may hold values from 0 to 15, all different within a row; in each aligned block of 128 rows (0 to 127, 128 to 255, ..., all dimensions but the last counted through in order) at most 24 rows name the same one
- specialist_mixing_shares: float32 [8, 2048, 2], P('dp', 'sp'), may hold values from 0.2 to 1
- specialist_gating_matrices: bfloat16 [16, 2048, 5120], P('sp', None, 'dp'), may hold values from -0.125 to 0.125
- raising_matrices: bfloat16 [16, 2048, 5120], P('sp', None, 'dp'), may hold values from -0.125 to 0.125
- lowering_matrices: bfloat16 [16, 5120, 2048], P('sp', 'dp'), may hold values from -0.078125 to 0.078125
Outputs:
- layer_out: bfloat16 [8, 2048, 2048], P('dp', 'sp')
The draws below stay inside these ranges and needn't reach their ends.
Inputs may be any that keep to these rules, and one draw needn't show every extreme that they name: `chosen_specialist_ids`: each row names two different experts. The rows of one device name no expert more than 24 times, a bound that some block reaches. `channel_fading_speed`: Positive.
All inputs are finite; a program needn't handle non-finite values.
Results may differ from the reference program's by a relative error of at most 0.015.
Values may be sent and summed in bfloat16 or wider, within the bound.
A program may use at most 128 MiB of HBM per device.

```python
import math
import jax
import jax.numpy as jnp
import numpy as np
from jax import lax

D = 2048
HEADS = 16
HEAD_DIM = 64
GROUPS = 4
STATE = 64
FF = 5120
KERNEL = 4
BLK = 128
TOK = 128
INNER = 1024
EXPERTS = 16
CAP = 24
FF_PART = 640
LEN = 2048
BATCH = 8
N_SP = 16
N_DP = 8


def draw_increment_premapped(key, part):
    noise_key, shift_key = jax.random.split(key)
    block_count = LEN // TOK
    shifted = jax.random.uniform(shift_key, (BATCH, block_count, 1, HEADS), jnp.float32, -1.2, 1.2)
    noise = jax.random.normal(noise_key, (BATCH, block_count, TOK, HEADS), jnp.float32)
    return jnp.clip(noise + shifted, -6.0, 6.0).reshape(BATCH, LEN, HEADS)


def draw_extra_log_fading(key, part):
    spot_key, loss_key = jax.random.split(key)
    spots = jax.random.randint(spot_key, (BATCH, 1, HEADS, 2), 0, LEN)
    losses = jax.random.uniform(loss_key, (BATCH, 1, HEADS, 2), jnp.float32, 0.2, 0.5)
    matched = jnp.arange(LEN)[None, :, None, None] == spots
    return jnp.sum(jnp.where(matched, jnp.log(1.0 - losses), 0.0), axis=3)


def draw_channel_fading_speed(key, part):
    pick_key, fast_key, slow_key = jax.random.split(key, 3)
    fast_share = 0.5
    quick = jax.random.bernoulli(pick_key, fast_share, (HEADS,))
    fast_rate = jnp.exp(jax.random.uniform(fast_key, (HEADS,), jnp.float32, math.log(0.03), math.log(0.1))) / 0.8
    slow_rate = jnp.exp(jax.random.uniform(slow_key, (HEADS,), jnp.float32, math.log(0.2), math.log(0.8))) / (0.8 * LEN)
    return jnp.where(quick, fast_rate, slow_rate)


def block_scale(rng, extent, cuts, least, high):
    def one(dim, blocks):
        heights = jax.random.uniform(jax.random.fold_in(jax.random.fold_in(rng, 6), dim), (blocks,), jnp.float32, least / len(cuts), high / len(cuts))
        return jnp.repeat(jnp.exp(heights), extent[dim] // blocks).reshape((-1,) + (1,) * (len(extent) - dim - 1))

    gain = one(*cuts[0])
    for cut in cuts[1:]:
        gain = gain * one(*cut)
    return gain


def deal_out(stream_key, own, number, rows, number_of, top, reach, skew):
    sequence = jax.random.permutation(stream_key, number_of)
    crowded, common = portions_of(number_of, rows * top, reach, skew, True), portions_of(number_of, rows * top, reach, skew, False)
    places = jnp.arange(number_of)

    def named(lengths, rotation):
        used = int((lengths > 0).sum())
        fixed = max(1, used // 4)
        passed = fixed + (places - fixed + rotation * (used - fixed)) % max(1, number_of - fixed)
        return jnp.zeros((number_of,), jnp.int32).at[sequence[jnp.where(places < fixed, places, passed)]].set(jnp.asarray(lengths, jnp.int32))

    lengths = jnp.where(number % 4 == 0, named(crowded, number // 4), named(common, number - number // 4 - 1))
    mixed = jax.random.permutation(jax.random.fold_in(own, 3), number_of)
    donor, taker = mixed[0:number_of // 2 * 2:2], mixed[1:number_of // 2 * 2:2]
    room = jnp.minimum(lengths[donor] - 1, reach - lengths[taker]) // 2
    room = jnp.where((donor == sequence[0]) | (taker == sequence[0]) | (lengths[taker] == 0), 0, jnp.maximum(room, 0))
    passed = jax.random.randint(jax.random.fold_in(own, 4), (number_of // 2,), 0, 1 << 20) % (room + 1)
    lengths = lengths.at[donor].add(-passed).at[taker].add(passed)
    members = jnp.searchsorted(jnp.cumsum(lengths), jnp.arange(rows * top), side="right").astype(jnp.int32)
    grid = members.reshape(top, rows).T
    grid = grid[jax.random.permutation(jax.random.fold_in(own, 1), rows)]
    rotation = jax.random.randint(jax.random.fold_in(own, 2), (rows, 1), 0, top)
    return jnp.take_along_axis(grid, (jnp.arange(top)[None, :] + rotation) % top, axis=1)


def portions_of(amount, total, limit, lean, full):
    loads = [(1 << 20) // math.isqrt(grade ** lean) + 1 for grade in range(1, amount + 1)]
    largest = limit if full else min(limit, max(-(-total // amount), total * loads[0] // sum(loads)))
    least = 1 if total - largest >= amount - 1 else 0
    given, rest = [largest] + [least] * (amount - 1), total - largest - least * (amount - 1)
    while rest > 0:
        free = [i for i in range(1, amount) if given[i] < largest] or [i for i in range(1, amount) if given[i] < limit]
        whole, left = sum([loads[i] for i in free]), rest
        for i in free:
            more = min(limit - given[i], max(1, left * loads[i] // whole), rest)
            given[i] = given[i] + more
            rest = rest - more
    return np.array(given)


def bell_draw(rng, dims, scale, limit, cuts=(), held_as=jnp.bfloat16):
    array = scale * jax.random.normal(rng, dims, jnp.float32)
    if cuts:
        array = array * block_scale(rng, dims, cuts, -0.22, 0.18)
    return jnp.clip(array, -limit, limit).astype(held_as)


def setup_inputs(seed: int = 0) -> dict:
    key_list = jax.random.split(jax.random.key(seed), 21)
    skip_connection_stream = bell_draw(key_list[0], (BATCH, LEN, D), 1.0, 6.0, ((0, 8), (1, 16)))
    emitted_valve_unscaled = bell_draw(key_list[1], (BATCH, LEN, INNER), 1.0, 6.0, ((0, 8), (1, 16)))
    channel_source_mapped = bell_draw(key_list[2], (BATCH, LEN, INNER), 1.0, 6.0, ((0, 8), (1, 16)))
    hidden_source_mapped = bell_draw(key_list[3], (BATCH, LEN, GROUPS * STATE), 1.0, 6.0, ((0, 8), (1, 16)))
    probe_mapped_values = bell_draw(key_list[4], (BATCH, LEN, GROUPS * STATE), 1.0, 6.0, ((0, 8), (1, 16)))
    increment_premapped = draw_increment_premapped(jax.random.fold_in(key_list[20], 71), 0)
    extra_log_fading = draw_extra_log_fading(jax.random.fold_in(key_list[20], 71), 0)
    channel_fading_speed = draw_channel_fading_speed(jax.random.fold_in(key_list[20], 71), 0)
    channel_source_kernel = bell_draw(key_list[8], (KERNEL, INNER), KERNEL ** -0.5, 3.0, (), jnp.float32)
    hidden_source_kernel = bell_draw(key_list[9], (KERNEL, GROUPS * STATE), KERNEL ** -0.5, 3.0, (), jnp.float32)
    probe_kernel_coefficients = bell_draw(key_list[10], (KERNEL, GROUPS * STATE), KERNEL ** -0.5, 3.0, (), jnp.float32)
    cluster_scaling_factor = jnp.clip(1.0 + 0.18 * jax.random.normal(key_list[11], (INNER,), jnp.float32), 0.1, 1.9)
    emitted_mapping_matrix = bell_draw(key_list[12], (INNER, D), INNER ** -0.5, 0.1875)
    standardize_scaling = jnp.clip(1.0 + 0.18 * jax.random.normal(key_list[13], (D,), jnp.float32), 0.1, 1.9)
    standardize_offset = bell_draw(key_list[14], (D,), 0.3, 2.0, (), jnp.float32)
    chosen_specialist_ids_keys = jax.random.split(jax.random.fold_in(key_list[15], 1), BATCH * LEN // TOK)
    chosen_specialist_ids_turns = jax.random.permutation(jax.random.fold_in(key_list[15], 3), BATCH * LEN // TOK)
    chosen_specialist_ids = jax.vmap(lambda own, number: deal_out(jax.random.fold_in(key_list[15], 2), own, number, TOK, EXPERTS, 2, CAP, 2))(chosen_specialist_ids_keys, chosen_specialist_ids_turns).reshape((BATCH, LEN, 2))
    specialist_mixing_shares = jnp.clip(0.2 + 0.8 * jax.random.uniform(key_list[16], (BATCH, LEN, 2), jnp.float32) ** block_scale(key_list[16], (BATCH, LEN, 2), ((0, 8), (1, 16)), -0.2, 0.2), 0.2, 1.0)
    specialist_gating_matrices = bell_draw(key_list[17], (EXPERTS, D, FF), D ** -0.5, 0.125, ((0, 16), (2, 8)))
    raising_matrices = bell_draw(key_list[18], (EXPERTS, D, FF), D ** -0.5, 0.125, ((0, 16), (2, 8)))
    lowering_matrices = bell_draw(key_list[19], (EXPERTS, FF, D), FF ** -0.5, 0.078125, ((0, 16), (1, 8)))
    return dict(skip_connection_stream=skip_connection_stream, emitted_valve_unscaled=emitted_valve_unscaled, channel_source_mapped=channel_source_mapped, hidden_source_mapped=hidden_source_mapped, probe_mapped_values=probe_mapped_values, increment_premapped=increment_premapped, extra_log_fading=extra_log_fading, channel_fading_speed=channel_fading_speed, channel_source_kernel=channel_source_kernel, hidden_source_kernel=hidden_source_kernel, probe_kernel_coefficients=probe_kernel_coefficients, cluster_scaling_factor=cluster_scaling_factor, emitted_mapping_matrix=emitted_mapping_matrix, standardize_scaling=standardize_scaling, standardize_offset=standardize_offset, chosen_specialist_ids=chosen_specialist_ids, specialist_mixing_shares=specialist_mixing_shares, specialist_gating_matrices=specialist_gating_matrices, raising_matrices=raising_matrices, lowering_matrices=lowering_matrices)


rms_eps = 1e-06
norm_eps = 1e-05

def causal_conv(series, tap_weights, rim_rows):
    padded = jnp.concatenate([rim_rows, series], axis=0).astype(jnp.float32)
    length = series.shape[0]
    running = jnp.zeros(series.shape, jnp.float32)
    for tap_index in range(tap_weights.shape[0]):
        running = running + tap_weights[tap_index].astype(jnp.float32) * lax.slice_in_dim(padded, tap_index, tap_index + length, axis=0)
    return jax.nn.silu(running).astype(jnp.bfloat16)

def ssd_blocks(x_conv, b_conv, c_conv, increment_delta, fading_exponent, init_state, block_len):
    length, head_count, head_width = x_conv.shape
    state_width = b_conv.shape[2]
    block_count = length // block_len
    x_block = x_conv.reshape(block_count, block_len, head_count, head_width).astype(jnp.float32)
    b_block = b_conv.reshape(block_count, block_len, head_count, state_width).astype(jnp.float32)
    c_block = c_conv.reshape(block_count, block_len, head_count, state_width).astype(jnp.float32)
    cumulative = jnp.cumsum(jnp.transpose(fading_exponent.reshape(block_count, block_len, head_count), (0, 2, 1)), axis=2)
    step_heads = jnp.transpose(increment_delta.reshape(block_count, block_len, head_count), (0, 2, 1))
    causal = jnp.arange(block_len)[:, None] >= jnp.arange(block_len)[None, :]
    within = jnp.exp(jnp.where(causal, cumulative[:, :, :, None] - cumulative[:, :, None, :], -jnp.inf))
    scores = jnp.einsum('cthn,cshn->chts', c_block, b_block)
    mixing = (scores * within * step_heads[:, :, None, :]).astype(jnp.bfloat16)
    diag_out = jnp.einsum('chts,cshp->cthp', mixing.astype(jnp.float32), x_block)
    tail_decay = jnp.exp(cumulative[:, :, -1:] - cumulative) * step_heads
    scaled = (x_block * jnp.transpose(tail_decay, (0, 2, 1))[:, :, :, None]).astype(jnp.bfloat16)
    block_state = jnp.einsum('cshp,cshn->chpn', scaled.astype(jnp.float32), b_block)
    totals = cumulative[:, :, -1]
    through = jnp.cumsum(totals, axis=0)
    before = through - totals
    earlier = jnp.arange(block_count)[:, None] > jnp.arange(block_count)[None, :]
    carry_weight = jnp.exp(jnp.where(earlier[:, :, None], before[:, None, :] - through[None, :, :], -jnp.inf))
    entering = jnp.einsum('cjh,jhpn->chpn', carry_weight, block_state, precision=lax.Precision.HIGHEST) + jnp.exp(before)[:, :, None, None] * init_state[None]
    reach_decay = jnp.transpose(jnp.exp(cumulative), (0, 2, 1))
    carried_out = jnp.einsum('cthn,chpn->cthp', c_block, entering, precision=lax.Precision.HIGHEST) * reach_decay[:, :, :, None]
    outcome = (diag_out + carried_out).reshape(length, head_count, head_width)
    final_state = jnp.einsum('jh,jhpn->hpn', jnp.exp(through[-1][None, :] - through), block_state, precision=lax.Precision.HIGHEST) + jnp.exp(through[-1])[:, None, None] * init_state
    return (outcome, final_state, through[-1])

def reference(skip_connection_stream, emitted_valve_unscaled, channel_source_mapped, hidden_source_mapped, probe_mapped_values, increment_premapped, extra_log_fading, channel_fading_speed, channel_source_kernel, hidden_source_kernel, probe_kernel_coefficients, cluster_scaling_factor, emitted_mapping_matrix, standardize_scaling, standardize_offset, chosen_specialist_ids, specialist_mixing_shares, specialist_gating_matrices, raising_matrices, lowering_matrices):
    per_group = HEADS // GROUPS
    tap_weights = jnp.concatenate([channel_source_kernel, hidden_source_kernel, probe_kernel_coefficients], axis=1)

    def lone_token_list(token_segments):
        channel_source_list, hidden_source_list, probe_value_list, increment_list, extra_fading_list = token_segments
        joined_rows = jnp.concatenate([channel_source_list, hidden_source_list, probe_value_list], axis=1)
        rim_rows = jnp.zeros((KERNEL - 1, joined_rows.shape[1]), jnp.bfloat16)
        convolved = causal_conv(joined_rows, tap_weights, rim_rows)
        x_conv = convolved[:, :INNER].reshape(LEN, HEADS, HEAD_DIM)
        b_conv = jnp.repeat(convolved[:, INNER:INNER + GROUPS * STATE].reshape(LEN, GROUPS, STATE), per_group, axis=1)
        c_conv = jnp.repeat(convolved[:, INNER + GROUPS * STATE:].reshape(LEN, GROUPS, STATE), per_group, axis=1)
        increment_delta = jax.nn.softplus(increment_list)
        fading_exponent = extra_fading_list - channel_fading_speed[None, :] * increment_delta
        init_state = jnp.zeros((HEADS, HEAD_DIM, STATE), jnp.float32)
        outcome, final_state, total_decay = ssd_blocks(x_conv, b_conv, c_conv, increment_delta, fading_exponent, init_state, BLK)
        return outcome.reshape(LEN, INNER).astype(jnp.bfloat16)
    blending_outcome = lax.map(lone_token_list, (channel_source_mapped, hidden_source_mapped, probe_mapped_values, increment_premapped, extra_log_fading))
    all_rows = BATCH * LEN
    gated = blending_outcome.reshape(all_rows, INNER).astype(jnp.float32) * jax.nn.silu(emitted_valve_unscaled.reshape(all_rows, INNER).astype(jnp.float32))
    grouped = gated.reshape(all_rows, GROUPS, INNER // GROUPS)
    grouped = grouped * lax.rsqrt(lax.optimization_barrier(jnp.mean(grouped * grouped, axis=-1, keepdims=True)) + rms_eps)
    group_normed = (grouped.reshape(all_rows, INNER) * cluster_scaling_factor[None, :]).astype(jnp.bfloat16)
    pre_norm = skip_connection_stream.reshape(all_rows, D).astype(jnp.float32) + jnp.dot(group_normed, emitted_mapping_matrix, preferred_element_type=jnp.float32)
    centre = lax.optimization_barrier(jnp.mean(pre_norm, axis=-1, keepdims=True))
    variance = lax.optimization_barrier(jnp.mean(jnp.square(pre_norm - centre), axis=-1, keepdims=True))
    normed = ((pre_norm - centre) * lax.rsqrt(variance + norm_eps) * standardize_scaling[None, :] + standardize_offset[None, :]).astype(jnp.bfloat16)
    flat_ids = chosen_specialist_ids.reshape(-1).astype(jnp.int32)
    flat_weights = specialist_mixing_shares.reshape(-1).astype(jnp.float32)
    owner = (jnp.arange(all_rows * 2, dtype=jnp.int32) // 2).astype(jnp.int32)
    buffer_rows = N_SP * N_DP * CAP
    padded_rows = jnp.concatenate([normed, jnp.zeros((1, D), jnp.bfloat16)], axis=0)

    def one_expert(running, expert):
        matched = flat_ids == expert
        ranked = jnp.cumsum(matched.astype(jnp.int32)) - 1
        placed = jnp.where(matched, ranked, buffer_rows).astype(jnp.int32)
        source = jnp.full((buffer_rows + 1,), all_rows, jnp.int32).at[placed].set(owner)[:buffer_rows]
        weight_at = jnp.zeros((buffer_rows + 1,), jnp.float32).at[placed].set(flat_weights)[:buffer_rows]
        rows_in = padded_rows[source]
        gate_val = jnp.dot(rows_in, specialist_gating_matrices[expert], preferred_element_type=jnp.float32)
        up_val = jnp.dot(rows_in, raising_matrices[expert], preferred_element_type=jnp.float32)
        hidden = (jax.nn.silu(gate_val) * up_val).astype(jnp.bfloat16)
        expert_sum = jnp.zeros((buffer_rows, D), jnp.float32)
        for part_index in range(N_DP):
            lower = part_index * FF_PART
            partial_value = jnp.dot(hidden[:, lower:lower + FF_PART], lowering_matrices[expert, lower:lower + FF_PART], preferred_element_type=jnp.float32).astype(jnp.bfloat16)
            expert_sum = expert_sum + lax.optimization_barrier(partial_value).astype(jnp.float32)
        expert_out = expert_sum.astype(jnp.bfloat16)
        running = running.at[source].add(weight_at[:, None] * expert_out.astype(jnp.float32))
        return (running, None)
    routed_sum, unused = lax.scan(one_expert, jnp.zeros((all_rows + 1, D), jnp.float32), jnp.arange(EXPERTS, dtype=jnp.int32))
    layer_out = (normed.astype(jnp.float32) + routed_sum[:all_rows]).astype(jnp.bfloat16)
    return layer_out.reshape(BATCH, LEN, D)
```

```python
import jax
import jax.numpy as jnp
from jax import lax
from jax.experimental import pallas as pl
from jax.experimental.pallas import tpu as pltpu
from jax.sharding import PartitionSpec as P

HEADS = 16
HEAD_DIM = 64
GROUPS = 4
STATE = 64
KERNEL = 4
BLK = 128


rms_eps = 1e-06
norm_eps = 1e-05


MESH = pl.DeviceIdType.MESH


def expert_kernel(
    rows, gate_w, raise_w, lower_w, out,
    gathered, partial, relayed, summed, gate_v, raise_v, lower_v, hidden,
    weight_sem, weight_send, weight_recv, go_send, go_recv, ring_send, ring_recv,
    sum_send, sum_recv, back_send, back_recv,
):
    sp = lax.axis_index("sp")
    dp = lax.axis_index("dp")
    z, y = lax.div(sp, 4), lax.rem(sp, 4)
    x, core = lax.div(dp, 2), lax.rem(dp, 2)
    right = (sp, lax.rem(x + 1, 4) * 2 + core)
    left = (sp, lax.rem(x + 3, 4) * 2 + core)
    twin = (sp, x * 2 + 1 - core)
    width = rows.shape[2]
    part = gate_w.shape[1]

    def ahead(o):
        return lax.rem(z + lax.div(o, 4), 4) * 4 + lax.rem(y + lax.rem(o, 4), 4)

    def behind(o):
        return lax.rem(z + 4 - lax.div(o, 4), 4) * 4 + lax.rem(y + 4 - lax.rem(o, 4), 4)

    barrier = pltpu.get_barrier_semaphore()

    def greet(o, carry):
        pl.semaphore_signal(barrier, inc=1, device_id=(ahead(o), dp), device_id_type=MESH)
        return carry

    lax.fori_loop(1, 16, greet, 0)
    for friend in (left, right, twin):
        pl.semaphore_signal(barrier, inc=1, device_id=friend, device_id_type=MESH)
    pl.semaphore_wait(barrier, 18)

    def go(o):
        return pltpu.make_async_remote_copy(
            src_ref=rows.at[pl.ds(3 * ahead(o), 3)],
            dst_ref=gathered.at[0, pl.ds(3 * o, 3)],
            send_sem=go_send.at[o],
            recv_sem=go_recv.at[o],
            device_id=(ahead(o), dp),
            device_id_type=MESH,
        )

    own_rows = pltpu.make_async_copy(
        rows.at[pl.ds(3 * sp, 3)], gathered.at[0, pl.ds(0, 3)], go_send.at[0]
    )
    own_rows.start()

    def start_go(o, carry):
        go(o).start()
        return carry

    lax.fori_loop(1, 16, start_go, 0)
    loads, gifts = [], []
    for k, (source, target) in enumerate(
        ((gate_w, gate_v), (raise_w, raise_v), (lower_w, lower_v))
    ):
        if k < 2:
            mine, theirs = target.at[:, pl.ds(0, part)], target.at[:, pl.ds(part, part)]
        else:
            mine, theirs = target.at[pl.ds(0, part)], target.at[pl.ds(part, part)]
        loads.append(pltpu.make_async_copy(source, mine, weight_sem.at[k]))
        gifts.append(
            pltpu.make_async_remote_copy(
                src_ref=source,
                dst_ref=theirs,
                send_sem=weight_send.at[k],
                recv_sem=weight_recv.at[k],
                device_id=twin,
                device_id_type=MESH,
            )
        )
    for copy in loads + gifts:
        copy.start()

    def group(g):
        return pl.ds(12 * g, 12)

    def ring(src_slot, dst_slot, g, target, lane):
        return pltpu.make_async_remote_copy(
            src_ref=gathered.at[src_slot, group(g)],
            dst_ref=gathered.at[dst_slot, group(g)],
            send_sem=ring_send.at[lane, g],
            recv_sem=ring_recv.at[dst_slot - 1, g],
            device_id=target,
            device_id_type=MESH,
        )

    def to_right(g):
        return ring(0, 1, g, right, 0)

    def to_left(g):
        return ring(0, 2, g, left, 1)

    def onward(g):
        return ring(1, 3, g, right, 2) if g < 2 else ring(2, 3, g, left, 2)

    for g in range(4):
        if g == 0:
            own_rows.wait()

        def wait_go(o, carry):
            go(o).wait_recv()
            return carry

        lax.fori_loop(max(4 * g, 1), 4 * g + 4, wait_go, 0)
        to_right(g).start()
        to_left(g).start()

    for copy in loads:
        copy.wait()
    for copy in gifts:
        copy.wait()

    tile = 256

    def unit(slot, half):
        rows_here = gathered.at[slot, pl.ds(24 * half, 24)].reshape(192, width)
        block = rows_here[...]

        def up(k, carry):
            cols = pl.ds(pl.multiple_of(k * tile, tile), tile)
            gate_val = jnp.dot(block, gate_v[:, cols], preferred_element_type=jnp.float32)
            up_val = jnp.dot(block, raise_v[:, cols], preferred_element_type=jnp.float32)
            hidden[:, cols] = (jax.nn.silu(gate_val) * up_val).astype(jnp.bfloat16)
            return carry

        lax.fori_loop(0, 2 * part // tile, up, 0)
        target = partial.at[slot, pl.ds(24 * half, 24)].reshape(192, width)

        def down(k, carry):
            cols = pl.ds(pl.multiple_of(k * tile, tile), tile)
            target[:, cols] = jnp.dot(
                hidden[...], lower_v[:, cols], preferred_element_type=jnp.float32
            ).astype(jnp.bfloat16)
            return carry

        lax.fori_loop(0, width // tile, down, 0)

    def sum_direct(slot, g):
        side = 0 if slot == 2 else 1
        return pltpu.make_async_remote_copy(
            src_ref=partial.at[slot, group(g)],
            dst_ref=summed.at[side, group(g)],
            send_sem=sum_send.at[side, g],
            recv_sem=sum_recv.at[side, g],
            device_id=right if slot == 2 else left,
            device_id_type=MESH,
        )

    def sum_relay(g):
        return pltpu.make_async_remote_copy(
            src_ref=partial.at[3, group(g)],
            dst_ref=relayed.at[group(g)],
            send_sem=sum_send.at[2, g],
            recv_sem=sum_recv.at[2, g],
            device_id=right if g < 2 else left,
            device_id_type=MESH,
        )

    unit(0, 0)
    to_right(0).wait_recv()
    onward(0).start()
    unit(0, 1)
    to_right(1).wait_recv()
    onward(1).start()
    unit(1, 0)
    to_left(0).wait_recv()
    to_left(1).wait_recv()
    unit(2, 0)
    to_left(2).wait_recv()
    onward(2).start()
    to_left(3).wait_recv()
    onward(3).start()
    sum_direct(1, 0).start()
    sum_direct(1, 1).start()
    unit(2, 1)
    sum_direct(2, 2).start()
    sum_direct(2, 3).start()
    to_right(2).wait_recv()
    to_right(3).wait_recv()
    unit(1, 1)
    onward(0).wait_recv()
    onward(1).wait_recv()
    unit(3, 0)
    sum_relay(0).start()
    sum_relay(1).start()
    onward(2).wait_recv()
    onward(3).wait_recv()
    unit(3, 1)
    sum_relay(2).start()
    sum_relay(3).start()
    for g in (0, 2, 1, 3):
        slot = 2 if g < 2 else 1
        sum_relay(g).wait_recv()
        partial[slot, group(g)] = (
            partial[slot, group(g)].astype(jnp.float32)
            + relayed[group(g)].astype(jnp.float32)
        ).astype(jnp.bfloat16)
        sum_direct(slot, g).start()

    def back(o):
        return pltpu.make_async_remote_copy(
            src_ref=partial.at[0, pl.ds(3 * o, 3)],
            dst_ref=out.at[pl.ds(3 * sp, 3)],
            send_sem=back_send.at[o],
            recv_sem=back_recv.at[o],
            device_id=(behind(o), dp),
            device_id_type=MESH,
        )

    def start_back(o, carry):
        back(o).start()
        return carry

    own_back = pltpu.make_async_copy(
        partial.at[0, pl.ds(0, 3)], out.at[pl.ds(3 * sp, 3)], back_send.at[0]
    )
    for g in (0, 2, 1, 3):
        sum_direct(2, g).wait_recv()
        sum_direct(1, g).wait_recv()
        partial[0, group(g)] = (
            partial[0, group(g)].astype(jnp.float32)
            + summed[0, group(g)].astype(jnp.float32)
            + summed[1, group(g)].astype(jnp.float32)
        ).astype(jnp.bfloat16)
        if g == 0:
            own_back.start()
        lax.fori_loop(max(4 * g, 1), 4 * g + 4, start_back, 0)

    for g in range(4):
        to_right(g).wait_send()
        to_left(g).wait_send()
        onward(g).wait_send()
        sum_direct(1, g).wait_send()
        sum_direct(2, g).wait_send()
        sum_relay(g).wait_send()
    own_back.wait()

    def drain(o, carry):
        go(o).wait_send()
        back(o).wait_send()
        back(o).wait_recv()
        return carry

    lax.fori_loop(1, 16, drain, 0)


def run_experts(rows, gate_w, raise_w, lower_w):
    width = rows.shape[2]
    part = gate_w.shape[1]
    any_space = pl.BlockSpec(memory_space=pl.ANY)
    return pl.pallas_call(
        expert_kernel,
        out_shape=jax.ShapeDtypeStruct(rows.shape, jnp.bfloat16),
        in_specs=[any_space] * 4,
        out_specs=any_space,
        scratch_shapes=[
            pltpu.VMEM((4, 48, 8, width), jnp.bfloat16),
            pltpu.VMEM((4, 48, 8, width), jnp.bfloat16),
            pltpu.VMEM((48, 8, width), jnp.bfloat16),
            pltpu.VMEM((2, 48, 8, width), jnp.bfloat16),
            pltpu.VMEM((width, 2 * part), jnp.bfloat16),
            pltpu.VMEM((width, 2 * part), jnp.bfloat16),
            pltpu.VMEM((2 * part, width), jnp.bfloat16),
            pltpu.VMEM((192, 2 * part), jnp.bfloat16),
            pltpu.SemaphoreType.DMA((3,)),
            pltpu.SemaphoreType.DMA((3,)),
            pltpu.SemaphoreType.DMA((3,)),
            pltpu.SemaphoreType.DMA((16,)),
            pltpu.SemaphoreType.DMA((16,)),
            pltpu.SemaphoreType.DMA((3, 4)),
            pltpu.SemaphoreType.DMA((3, 4)),
            pltpu.SemaphoreType.DMA((3, 4)),
            pltpu.SemaphoreType.DMA((3, 4)),
            pltpu.SemaphoreType.DMA((16,)),
            pltpu.SemaphoreType.DMA((16,)),
        ],
        compiler_params=pltpu.CompilerParams(
            collective_id=0, has_side_effects=True, vmem_limit_bytes=60 * 1024 * 1024
        ),
        name="routed_experts",
    )(rows, gate_w, raise_w, lower_w)


def causal_conv(series, tap_weights, rim_rows):
    padded = jnp.concatenate([rim_rows, series], axis=0).astype(jnp.float32)
    length = series.shape[0]
    running = jnp.zeros(series.shape, jnp.float32)
    for tap_index in range(tap_weights.shape[0]):
        running = running + tap_weights[tap_index] * lax.slice_in_dim(
            padded, tap_index, tap_index + length, axis=0
        )
    return jax.nn.silu(running).astype(jnp.bfloat16)


def ssd_blocks(x_conv, b_conv, c_conv, increment_delta, fading_exponent, init_state, block_len):
    length, head_count, head_width = x_conv.shape
    state_width = b_conv.shape[2]
    block_count = length // block_len
    x_block = x_conv.reshape(block_count, block_len, head_count, head_width)
    b_block = b_conv.reshape(block_count, block_len, head_count, state_width)
    c_block = c_conv.reshape(block_count, block_len, head_count, state_width)
    cumulative = jnp.cumsum(
        jnp.transpose(fading_exponent.reshape(block_count, block_len, head_count), (0, 2, 1)),
        axis=2,
    )
    step_heads = jnp.transpose(
        increment_delta.reshape(block_count, block_len, head_count), (0, 2, 1)
    )
    causal = jnp.arange(block_len)[:, None] >= jnp.arange(block_len)[None, :]
    within = jnp.exp(
        jnp.where(causal, cumulative[:, :, :, None] - cumulative[:, :, None, :], -jnp.inf)
    )
    scores = jnp.einsum("cthn,cshn->chts", c_block, b_block, preferred_element_type=jnp.float32)
    mixing = (scores * within * step_heads[:, :, None, :]).astype(jnp.bfloat16)
    diag_out = jnp.einsum("chts,cshp->cthp", mixing, x_block, preferred_element_type=jnp.float32)
    tail_decay = jnp.exp(cumulative[:, :, -1:] - cumulative) * step_heads
    scaled = (
        x_block.astype(jnp.float32) * jnp.transpose(tail_decay, (0, 2, 1))[:, :, :, None]
    ).astype(jnp.bfloat16)
    block_state = jnp.einsum("cshp,cshn->chpn", scaled, b_block, preferred_element_type=jnp.float32)
    totals = cumulative[:, :, -1]
    through = jnp.cumsum(totals, axis=0)
    before = through - totals
    earlier = jnp.arange(block_count)[:, None] > jnp.arange(block_count)[None, :]
    carry_weight = jnp.exp(
        jnp.where(earlier[:, :, None], before[:, None, :] - through[None, :, :], -jnp.inf)
    )
    entering = (
        jnp.einsum("cjh,jhpn->chpn", carry_weight, block_state)
        + jnp.exp(before)[:, :, None, None] * init_state[None]
    )
    reach_decay = jnp.transpose(jnp.exp(cumulative), (0, 2, 1))
    carried_out = (
        jnp.einsum("cthn,chpn->cthp", c_block.astype(jnp.float32), entering)
        * reach_decay[:, :, :, None]
    )
    outcome = (diag_out + carried_out).reshape(length, head_count, head_width)
    final_state = (
        jnp.einsum("jh,jhpn->hpn", jnp.exp(through[-1][None, :] - through), block_state)
        + jnp.exp(through[-1])[:, None, None] * init_state
    )
    return (outcome, final_state, through[-1])


def per_device(
    skip_connection_stream,
    emitted_valve_unscaled,
    channel_source_mapped,
    hidden_source_mapped,
    probe_mapped_values,
    increment_premapped,
    extra_log_fading,
    channel_fading_speed,
    channel_source_kernel,
    hidden_source_kernel,
    probe_kernel_coefficients,
    cluster_scaling_factor,
    emitted_mapping_matrix,
    standardize_scaling,
    standardize_offset,
    chosen_specialist_ids,
    specialist_mixing_shares,
    specialist_gating_matrices,
    raising_matrices,
    lowering_matrices,
):
    sp_size = lax.axis_size("sp")
    sp_index = lax.axis_index("sp")
    tok_rows = skip_connection_stream.shape[1]
    model_width = skip_connection_stream.shape[2]
    inner_width = HEADS * HEAD_DIM
    per_group = HEADS // GROUPS
    paired = HEAD_DIM + 2 * STATE
    head_count = HEADS // sp_size
    first_head = sp_index * head_count
    x_heads = channel_source_mapped[0].reshape(tok_rows, HEADS, HEAD_DIM)
    b_heads = jnp.repeat(
        hidden_source_mapped[0].reshape(tok_rows, GROUPS, STATE), per_group, axis=1
    )
    c_heads = jnp.repeat(probe_mapped_values[0].reshape(tok_rows, GROUPS, STATE), per_group, axis=1)
    payload = jnp.concatenate([x_heads, b_heads, c_heads], axis=2)
    arrived = lax.all_to_all(payload, "sp", split_axis=1, concat_axis=0, tiled=True)
    taps_x = lax.dynamic_slice_in_dim(
        channel_source_kernel.reshape(KERNEL, HEADS, HEAD_DIM), first_head, head_count, 1
    )
    taps_b = lax.dynamic_slice_in_dim(
        jnp.repeat(hidden_source_kernel.reshape(KERNEL, GROUPS, STATE), per_group, axis=1),
        first_head,
        head_count,
        1,
    )
    taps_c = lax.dynamic_slice_in_dim(
        jnp.repeat(probe_kernel_coefficients.reshape(KERNEL, GROUPS, STATE), per_group, axis=1),
        first_head,
        head_count,
        1,
    )
    rim_rows = jnp.zeros((KERNEL - 1, head_count, paired), jnp.bfloat16)
    convolved = causal_conv(arrived, jnp.concatenate([taps_x, taps_b, taps_c], axis=2), rim_rows)
    increment_delta = jax.nn.softplus(increment_premapped[0])
    speeds_per_channel = lax.dynamic_slice_in_dim(channel_fading_speed, first_head, head_count, 0)
    fading_exponent = extra_log_fading[0] - speeds_per_channel[None, :] * increment_delta
    init_state = jnp.zeros((head_count, HEAD_DIM, STATE), jnp.float32)
    outcome, final_state, total_decay = ssd_blocks(
        convolved[:, :, :HEAD_DIM],
        convolved[:, :, HEAD_DIM : HEAD_DIM + STATE],
        convolved[:, :, HEAD_DIM + STATE :],
        increment_delta,
        fading_exponent,
        init_state,
        BLK,
    )
    returned_rows = lax.all_to_all(
        outcome.astype(jnp.bfloat16), "sp", split_axis=0, concat_axis=1, tiled=True
    )
    blending_outcome = returned_rows.reshape(tok_rows, inner_width)
    gated = blending_outcome.astype(jnp.float32) * jax.nn.silu(
        emitted_valve_unscaled[0].astype(jnp.float32)
    )
    grouped = gated.reshape(tok_rows, GROUPS, inner_width // GROUPS)
    grouped = grouped * lax.rsqrt(jnp.mean(grouped * grouped, axis=-1, keepdims=True) + rms_eps)
    group_normed = (
        grouped.reshape(tok_rows, inner_width) * cluster_scaling_factor[None, :]
    ).astype(jnp.bfloat16)
    pre_norm = skip_connection_stream[0].astype(jnp.float32) + jnp.dot(
        group_normed, emitted_mapping_matrix, preferred_element_type=jnp.float32
    )
    centre = jnp.mean(pre_norm, axis=-1, keepdims=True)
    variance = jnp.mean(jnp.square(pre_norm - centre), axis=-1, keepdims=True)
    normed = (
        (pre_norm - centre) * lax.rsqrt(variance + norm_eps) * standardize_scaling[None, :]
        + standardize_offset[None, :]
    ).astype(jnp.bfloat16)
    slot_cap = 3 * tok_rows // sp_size
    flat_ids = chosen_specialist_ids[0].reshape(-1)
    matched = (flat_ids[:, None] == jnp.arange(sp_size, dtype=jnp.int32)[None, :]).astype(jnp.int32)
    ranked = jnp.cumsum(matched, axis=0) - 1
    target = flat_ids * slot_cap + jnp.sum(matched * ranked, axis=1)
    placing = (jnp.arange(sp_size * slot_cap, dtype=jnp.int32)[:, None] == target[None, :]).astype(
        jnp.bfloat16
    )
    placing = jnp.sum(placing.reshape(sp_size * slot_cap, tok_rows, 2), axis=2)
    outgoing = (
        jnp.dot(placing, normed, preferred_element_type=jnp.float32)
        .astype(jnp.bfloat16)
        .reshape(sp_size, slot_cap, model_width)
    )

    answered = run_experts(
        outgoing.reshape(-1, 8, model_width),
        specialist_gating_matrices[0],
        raising_matrices[0],
        lowering_matrices[0],
    )
    picked = answered.reshape(sp_size * slot_cap, model_width)[target.reshape(tok_rows, 2)]
    routed_sum = jnp.sum(
        specialist_mixing_shares[0][:, :, None] * picked.astype(jnp.float32), axis=1
    )
    layer_out = (normed.astype(jnp.float32) + routed_sum).astype(jnp.bfloat16)
    return layer_out[None]


def solution(mesh):
    placed = (
        P("dp", "sp", None),
        P("dp", "sp", None),
        P("dp", "sp", None),
        P("dp", "sp", None),
        P("dp", "sp", None),
        P("dp", None, "sp"),
        P("dp", None, "sp"),
        P(),
        P(),
        P(),
        P(),
        P(),
        P(),
        P(),
        P(),
        P("dp", "sp", None),
        P("dp", "sp", None),
        P("sp", None, "dp"),
        P("sp", None, "dp"),
        P("sp", "dp", None),
    )
    return jax.shard_map(
        per_device, mesh=mesh, in_specs=placed, out_specs=P("dp", "sp", None), check_vma=False
    )
```

```python
import jax
import jax.numpy as jnp
from jax import lax
from jax.experimental import pallas as pl
from jax.experimental.pallas import tpu as pltpu
from jax.sharding import PartitionSpec as P

MESH = pl.DeviceIdType.MESH
HEADS = 16
HEAD_DIM = 64
TOK = 128
INNER = 1024
SLOTS = 24
rms_eps = 1e-06
norm_eps = 1e-05
BF16 = jnp.bfloat16
F32 = jnp.float32
EXACT = lax.Precision.HIGHEST


def dot(a, b, precision=None):
    return jnp.dot(a, b, preferred_element_type=F32, precision=precision)


def dot_nt(a, b, precision=None):
    return lax.dot_general(
        a, b, (((1,), (1,)), ((), ())), preferred_element_type=F32, precision=precision
    )


def iota(shape, dim):
    return lax.broadcasted_iota(jnp.int32, shape, dim)


def layer_kernel(
    speed, skip, valve, chan, hid, probe, step_in, fade_in, tap_x, tap_b, tap_c, group_gain, out_w,
    gain, offset, ids, shares, gate_w, raise_w, lower_w,
    result,
    joined, steps, fades, conv, state, decay, state_in, decay_in, entering, entered, inside, out_v,
    pre, normed, placing, weighing, outgoing, answers,
    gathered, partial, relayed, summed, gate_v, raise_v, lower_v, hidden,
    load_sem, rim_send, rim_recv, step_send, step_recv, state_send, state_recv,
    enter_send, enter_recv,
    weight_sem, weight_send, weight_recv, go_send, go_recv, ring_send, ring_recv,
    sum_send, sum_recv, back_send, back_recv,
):
    sp = lax.axis_index("sp")
    dp = lax.axis_index("dp")
    z, y = lax.div(sp, 4), lax.rem(sp, 4)
    x, core = lax.div(dp, 2), lax.rem(dp, 2)
    right = (sp, lax.rem(x + 1, 4) * 2 + core)
    left = (sp, lax.rem(x + 3, 4) * 2 + core)
    twin = (sp, x * 2 + 1 - core)
    width = skip.shape[1]
    part = gate_w.shape[1]

    def ahead(o):
        return lax.rem(z + lax.div(o, 4), 4) * 4 + lax.rem(y + lax.rem(o, 4), 4)

    def behind(o):
        return lax.rem(z + 4 - lax.div(o, 4), 4) * 4 + lax.rem(y + 4 - lax.rem(o, 4), 4)

    def each(low, high, work):
        def step(o, carry):
            work(o)
            return carry

        lax.fori_loop(low, high, step, 0)

    barrier = pltpu.get_barrier_semaphore()
    each(
        1, 16,
        lambda o: pl.semaphore_signal(
            barrier, inc=1, device_id=(ahead(o), dp), device_id_type=MESH
        ),
    )
    for friend in (left, right, twin):
        pl.semaphore_signal(barrier, inc=1, device_id=friend, device_id_type=MESH)

    spans = ((chan, 0, INNER), (hid, INNER, 256), (probe, INNER + 256, 256))
    own_loads = [
        pltpu.make_async_copy(
            ref, joined.at[pl.ds(1, 16), :, pl.ds(low, size)], load_sem.at[k]
        )
        for k, (ref, low, size) in enumerate(spans)
    ]
    own_loads.append(
        pltpu.make_async_copy(step_in.at[sp], steps.at[sp], load_sem.at[3])
    )
    own_loads.append(
        pltpu.make_async_copy(fade_in.at[sp], fades.at[sp], load_sem.at[4])
    )
    out_load = pltpu.make_async_copy(out_w, out_v, load_sem.at[5])
    for copy in own_loads:
        copy.start()
    loads, gifts = [], []
    for k, (source, target) in enumerate(
        ((gate_w, gate_v), (raise_w, raise_v), (lower_w, lower_v))
    ):
        if k < 2:
            mine, theirs = target.at[:, pl.ds(0, part)], target.at[:, pl.ds(part, part)]
        else:
            mine, theirs = target.at[pl.ds(0, part)], target.at[pl.ds(part, part)]
        loads.append(pltpu.make_async_copy(source, mine, weight_sem.at[k]))
        gifts.append(
            pltpu.make_async_remote_copy(
                src_ref=source,
                dst_ref=theirs,
                send_sem=weight_send.at[k],
                recv_sem=weight_recv.at[k],
                device_id=twin,
                device_id_type=MESH,
            )
        )

    pl.semaphore_wait(barrier, 18)

    def step_copy(o, source, target, which):
        return pltpu.make_async_remote_copy(
            src_ref=source.at[ahead(o)],
            dst_ref=target.at[sp],
            send_sem=step_send.at[which, o],
            recv_sem=step_recv.at[which, o],
            device_id=(ahead(o), dp),
            device_id_type=MESH,
        )

    def send_steps(o):
        step_copy(o, step_in, steps, 0).start()
        step_copy(o, fade_in, fades, 1).start()

    each(1, 16, send_steps)
    rims = [
        pltpu.make_async_remote_copy(
            src_ref=ref.at[pl.ds(15, 1)],
            dst_ref=joined.at[pl.ds(0, 1), :, pl.ds(low, size)],
            send_sem=rim_send.at[k],
            recv_sem=rim_recv.at[k],
            device_id=(lax.rem(sp + 1, 16), dp),
            device_id_type=MESH,
        )
        for k, (ref, low, size) in enumerate(spans)
    ]
    for copy in rims:
        copy.start()
    out_load.start()
    for copy in loads + gifts:
        copy.start()
    for copy in own_loads:
        copy.wait()
    for copy in rims:
        copy.wait_recv()

    def convolve(cols, taps):
        block = joined[:, :, cols].reshape(TOK + 8, 256).astype(F32)
        block = jnp.where(iota((TOK + 8, 256), 0) + 8 * sp >= 8, block, 0.0)
        running = taps[0:1] * block[5 : 5 + TOK]
        for k in range(1, 4):
            running = running + taps[k : k + 1] * block[5 + k : 5 + k + TOK]
        conv[:, cols] = jax.nn.silu(running).astype(BF16)

    def convolve_x(k):
        cols = pl.ds(pl.multiple_of(k * 256, 256), 256)
        convolve(cols, tap_x[:, cols])

    each(0, 4, convolve_x)
    convolve(pl.ds(INNER, 256), tap_b[...])
    convolve(pl.ds(INNER + 256, 256), tap_c[...])

    def wait_steps(o):
        step_copy(o, step_in, steps, 0).wait_recv()
        step_copy(o, fade_in, fades, 1).wait_recv()

    each(1, 16, wait_steps)
    row = iota((HEADS, TOK), 0)
    speeds = jnp.zeros((HEADS, TOK), F32)
    for h in range(HEADS):
        speeds = jnp.where(row == h, speed[h], speeds)
    raw = steps[...].reshape(HEADS, TOK)
    step = jnp.maximum(raw, 0.0) + jnp.log1p(jnp.exp(-jnp.abs(raw)))
    fading = fades[...].reshape(HEADS, TOK) - speeds * step
    later = iota((TOK, TOK), 0)
    sooner = iota((TOK, TOK), 1)
    causal = later >= sooner
    triangle = causal.astype(F32)
    cum_row = dot_nt(fading, triangle, EXACT)
    cum_col = dot_nt(triangle, fading, EXACT)
    step_col = dot_nt((later == sooner).astype(F32), step, EXACT)
    spread = (lax.div(iota((HEADS, INNER), 1), HEAD_DIM) == iota((HEADS, INNER), 0)).astype(F32)
    last = cum_col[TOK - 1 : TOK]
    tail_wide = dot(jnp.exp(last - cum_col) * step_col, spread, EXACT)
    decay_wide = dot(jnp.broadcast_to(jnp.exp(last), (8, HEADS)), spread, EXACT)
    for k in range(2):
        decay[k] = decay_wide[0:1, 512 * k : 512 * k + 512]
    scaled = (conv[:, 0:INNER].astype(F32) * tail_wide).astype(BF16)
    for q in range(2):
        b_pair = conv[:, INNER + 128 * q : INNER + 128 * q + 128]
        both = dot(b_pair.T, scaled[:, 512 * q : 512 * q + 512])
        state[:, 512 * q : 512 * q + 256] = both[0:64, 0:256]
        state[:, 512 * q + 256 : 512 * q + 512] = both[64:128, 256:512]

    def place_of(k):
        return (
            pl.ds(pl.multiple_of(lax.div(k, 2) * 8, 8), 8),
            pl.ds(pl.multiple_of(lax.rem(k, 2) * 512, 512), 512),
        )

    def state_copy(o):
        rows, cols = place_of(ahead(o))
        return pltpu.make_async_remote_copy(
            src_ref=state.at[rows, cols],
            dst_ref=state_in.at[sp],
            send_sem=state_send.at[0, o],
            recv_sem=state_recv.at[0, o],
            device_id=(ahead(o), dp),
            device_id_type=MESH,
        )

    def decay_copy(o):
        return pltpu.make_async_remote_copy(
            src_ref=decay.at[lax.rem(ahead(o), 2)],
            dst_ref=decay_in.at[sp],
            send_sem=state_send.at[1, o],
            recv_sem=state_recv.at[1, o],
            device_id=(ahead(o), dp),
            device_id_type=MESH,
        )

    def send_state(o):
        decay_copy(o).start()
        state_copy(o).start()

    each(1, 16, send_state)
    my_rows, my_cols = place_of(sp)
    state_in[sp] = state[my_rows, my_cols]
    decay_in[sp] = decay[lax.rem(sp, 2)]

    low_half = iota((TOK, TOK), 1) < 64
    for q in range(2):
        b_pair = conv[:, INNER + 128 * q : INNER + 128 * q + 128]
        c_pair = conv[:, INNER + 256 + 128 * q : INNER + 256 + 128 * q + 128]
        for g in range(2):
            c_one = jnp.where(low_half == (g == 0), c_pair, jnp.zeros_like(c_pair))
            scores = dot_nt(c_one, b_pair)
            for i in range(2):
                first = 8 * q + 4 * g + 2 * i
                x_pair = conv[:, 64 * first : 64 * first + 128]
                total = None
                for h in (first, first + 1):
                    gap = jnp.where(
                        causal, cum_col[:, h : h + 1] - cum_row[h : h + 1, :], -1e30
                    )
                    mixing = (scores * jnp.exp(gap) * step[h : h + 1, :]).astype(BF16)
                    x_one = jnp.where(low_half == (h == first), x_pair, jnp.zeros_like(x_pair))
                    term = dot(mixing, x_one)
                    total = term if total is None else total + term
                inside[:, 64 * first : 64 * first + 128] = total

    def placing_rows():
        expert = iota((16, TOK), 0)
        first, second = expert == ids[0:1, :], expert == ids[1:2, :]
        named = first | second
        share = jnp.where(first, shares[0:1, :], 0.0) + jnp.where(second, shares[1:2, :], 0.0)
        before = (later < sooner).astype(BF16)
        rank = dot(named.astype(F32).astype(BF16), before)
        rank = jnp.where(named, rank, -1.0)
        slot = iota((SLOTS, TOK), 0).astype(F32)
        chosen = jnp.concatenate(
            [(rank[e : e + 1, :] == slot).astype(F32) for e in range(16)], axis=0
        )
        weights = jnp.concatenate(
            [
                jnp.where(rank[e : e + 1, :] == slot, share[e : e + 1, :], 0.0)
                for e in range(16)
            ],
            axis=0,
        )
        placing[...] = chosen.astype(BF16)
        rest = weights.T
        for k in range(3):
            piece = rest.astype(BF16)
            weighing[pl.ds(TOK * k, TOK), :] = piece
            rest = rest - piece.astype(F32)

    placing_rows()

    def wait_state(o):
        decay_copy(o).wait_recv()
        state_copy(o).wait_recv()

    each(1, 16, wait_state)

    def advance(j, held):
        entering[j] = held
        return decay_in[j] * held + state_in[j]

    lax.fori_loop(0, 16, advance, jnp.zeros((8, 512), F32))

    def enter_copy(o):
        rows, cols = place_of(sp)
        return pltpu.make_async_remote_copy(
            src_ref=entering.at[ahead(o)],
            dst_ref=entered.at[rows, cols],
            send_sem=enter_send.at[o],
            recv_sem=enter_recv.at[o],
            device_id=(ahead(o), dp),
            device_id_type=MESH,
        )

    each(1, 16, lambda o: enter_copy(o).start())
    entered[my_rows, my_cols] = entering[sp]
    reach_wide = dot(jnp.exp(cum_col), spread, EXACT)
    each(1, 16, lambda o: enter_copy(o).wait_recv())

    nothing = jnp.zeros((64, 256), F32)
    blocks = []
    for q in range(2):
        c_pair = conv[:, INNER + 256 + 128 * q : INNER + 256 + 128 * q + 128]
        low, high = entered[:, 512 * q : 512 * q + 256], entered[:, 512 * q + 256 : 512 * q + 512]
        both = jnp.concatenate(
            [
                jnp.concatenate([low, nothing], axis=1),
                jnp.concatenate([nothing, high], axis=1),
            ],
            axis=0,
        )
        carried = dot(c_pair.astype(F32), both, EXACT)
        for g in range(2):
            low_col = 512 * q + 256 * g
            mixed = (
                inside[:, low_col : low_col + 256]
                + reach_wide[:, low_col : low_col + 256] * carried[:, 256 * g : 256 * g + 256]
            ).astype(BF16)
            gated = mixed.astype(F32) * jax.nn.silu(valve[:, low_col : low_col + 256].astype(F32))
            level = lax.rsqrt(jnp.mean(gated * gated, axis=1, keepdims=True) + rms_eps)
            blocks.append(
                (gated * level * group_gain[:, low_col : low_col + 256]).astype(BF16)
            )
    group_normed = jnp.concatenate(blocks, axis=1)
    out_load.wait()

    def project(k):
        cols = pl.ds(pl.multiple_of(k * 256, 256), 256)
        pre[:, cols] = skip[:, cols].astype(F32) + dot(group_normed, out_v[:, cols])

    each(0, width // 256, project)

    def standardize(k):
        rows = pl.ds(pl.multiple_of(k * 16, 16), 16)
        block = pre[rows, :]
        shifted = block - jnp.mean(block, axis=1, keepdims=True)
        level = lax.rsqrt(jnp.mean(shifted * shifted, axis=1, keepdims=True) + norm_eps)
        normed[rows, :] = (shifted * level * gain[...] + offset[...]).astype(BF16)

    each(0, TOK // 16, standardize)
    flat_outgoing = outgoing.reshape(16 * SLOTS, width)

    def route(k):
        cols = pl.ds(pl.multiple_of(k * 256, 256), 256)
        flat_outgoing[:, cols] = dot(placing[...], normed[:, cols]).astype(BF16)

    each(0, width // 256, route)

    def go(o):
        return pltpu.make_async_remote_copy(
            src_ref=outgoing.at[pl.ds(3 * ahead(o), 3)],
            dst_ref=gathered.at[0, pl.ds(3 * o, 3)],
            send_sem=go_send.at[o],
            recv_sem=go_recv.at[o],
            device_id=(ahead(o), dp),
            device_id_type=MESH,
        )

    each(1, 16, lambda o: go(o).start())
    gathered[0, 0:3] = outgoing[pl.ds(3 * sp, 3)]

    def group(g):
        return pl.ds(12 * g, 12)

    def ring(src_slot, dst_slot, g, target, lane):
        return pltpu.make_async_remote_copy(
            src_ref=gathered.at[src_slot, group(g)],
            dst_ref=gathered.at[dst_slot, group(g)],
            send_sem=ring_send.at[lane, g],
            recv_sem=ring_recv.at[dst_slot - 1, g],
            device_id=target,
            device_id_type=MESH,
        )

    def to_right(g):
        return ring(0, 1, g, right, 0)

    def to_left(g):
        return ring(0, 2, g, left, 1)

    def onward(g):
        return ring(1, 3, g, right, 2) if g < 2 else ring(2, 3, g, left, 2)

    for g in range(4):
        each(max(4 * g, 1), 4 * g + 4, lambda o: go(o).wait_recv())
        to_right(g).start()
        to_left(g).start()

    for copy in loads:
        copy.wait()
    for copy in gifts:
        copy.wait()

    tile = 256

    def unit(slot, half):
        rows_here = gathered.at[slot, pl.ds(24 * half, 24)].reshape(192, width)
        block = rows_here[...]

        def up(k):
            cols = pl.ds(pl.multiple_of(k * tile, tile), tile)
            gate_val = jnp.dot(block, gate_v[:, cols], preferred_element_type=F32)
            up_val = jnp.dot(block, raise_v[:, cols], preferred_element_type=F32)
            hidden[:, cols] = (jax.nn.silu(gate_val) * up_val).astype(BF16)

        each(0, 2 * part // tile, up)
        target = partial.at[slot, pl.ds(24 * half, 24)].reshape(192, width)

        def down(k):
            cols = pl.ds(pl.multiple_of(k * tile, tile), tile)
            target[:, cols] = jnp.dot(
                hidden[...], lower_v[:, cols], preferred_element_type=F32
            ).astype(BF16)

        each(0, width // tile, down)

    def sum_direct(slot, g):
        side = 0 if slot == 2 else 1
        return pltpu.make_async_remote_copy(
            src_ref=partial.at[slot, group(g)],
            dst_ref=summed.at[side, group(g)],
            send_sem=sum_send.at[side, g],
            recv_sem=sum_recv.at[side, g],
            device_id=right if slot == 2 else left,
            device_id_type=MESH,
        )

    def sum_relay(g):
        return pltpu.make_async_remote_copy(
            src_ref=partial.at[3, group(g)],
            dst_ref=relayed.at[group(g)],
            send_sem=sum_send.at[2, g],
            recv_sem=sum_recv.at[2, g],
            device_id=right if g < 2 else left,
            device_id_type=MESH,
        )

    unit(0, 0)
    to_right(0).wait_recv()
    onward(0).start()
    unit(0, 1)
    to_right(1).wait_recv()
    onward(1).start()
    unit(1, 0)
    to_left(0).wait_recv()
    to_left(1).wait_recv()
    unit(2, 0)
    to_left(2).wait_recv()
    onward(2).start()
    to_left(3).wait_recv()
    onward(3).start()
    sum_direct(1, 0).start()
    sum_direct(1, 1).start()
    unit(2, 1)
    sum_direct(2, 2).start()
    sum_direct(2, 3).start()
    to_right(2).wait_recv()
    to_right(3).wait_recv()
    unit(1, 1)
    onward(0).wait_recv()
    onward(1).wait_recv()
    unit(3, 0)
    sum_relay(0).start()
    sum_relay(1).start()
    onward(2).wait_recv()
    onward(3).wait_recv()
    unit(3, 1)
    sum_relay(2).start()
    sum_relay(3).start()
    for g in (0, 2, 1, 3):
        slot = 2 if g < 2 else 1
        sum_relay(g).wait_recv()
        partial[slot, group(g)] = (
            partial[slot, group(g)].astype(F32)
            + relayed[group(g)].astype(F32)
        ).astype(BF16)
        sum_direct(slot, g).start()

    def back(o):
        return pltpu.make_async_remote_copy(
            src_ref=partial.at[0, pl.ds(3 * o, 3)],
            dst_ref=answers.at[pl.ds(3 * sp, 3)],
            send_sem=back_send.at[o],
            recv_sem=back_recv.at[o],
            device_id=(behind(o), dp),
            device_id_type=MESH,
        )

    for g in (0, 2, 1, 3):
        sum_direct(2, g).wait_recv()
        sum_direct(1, g).wait_recv()
        partial[0, group(g)] = (
            partial[0, group(g)].astype(F32)
            + summed[0, group(g)].astype(F32)
            + summed[1, group(g)].astype(F32)
        ).astype(BF16)
        each(max(4 * g, 1), 4 * g + 4, lambda o: back(o).start())
        if g == 0:
            answers[pl.ds(3 * sp, 3)] = partial[0, 0:3]

    for copy in rims:
        copy.wait_send()
    for g in range(4):
        to_right(g).wait_send()
        to_left(g).wait_send()
        onward(g).wait_send()
        sum_direct(1, g).wait_send()
        sum_direct(2, g).wait_send()
        sum_relay(g).wait_send()

    def drain(o):
        step_copy(o, step_in, steps, 0).wait_send()
        step_copy(o, fade_in, fades, 1).wait_send()
        decay_copy(o).wait_send()
        state_copy(o).wait_send()
        enter_copy(o).wait_send()
        go(o).wait_send()
        back(o).wait_send()
        back(o).wait_recv()

    each(1, 16, drain)
    flat_answers = answers.reshape(16 * SLOTS, width)

    def finish(k):
        cols = pl.ds(pl.multiple_of(k * 256, 256), 256)
        terms = dot(weighing[...], flat_answers[:, cols])
        routed = terms[0:TOK] + terms[TOK : 2 * TOK] + terms[2 * TOK : 3 * TOK]
        result[:, cols] = (normed[:, cols].astype(F32) + routed).astype(BF16)

    each(0, width // 256, finish)


def per_device(
    skip_connection_stream,
    emitted_valve_unscaled,
    channel_source_mapped,
    hidden_source_mapped,
    probe_mapped_values,
    increment_premapped,
    extra_log_fading,
    channel_fading_speed,
    channel_source_kernel,
    hidden_source_kernel,
    probe_kernel_coefficients,
    cluster_scaling_factor,
    emitted_mapping_matrix,
    standardize_scaling,
    standardize_offset,
    chosen_specialist_ids,
    specialist_mixing_shares,
    specialist_gating_matrices,
    raising_matrices,
    lowering_matrices,
):
    width = skip_connection_stream.shape[2]
    part = specialist_gating_matrices.shape[2]
    far = pl.BlockSpec(memory_space=pl.ANY)
    near = pl.BlockSpec(memory_space=pltpu.VMEM)
    scalars = pl.BlockSpec(memory_space=pltpu.SMEM)
    dma = pltpu.SemaphoreType.DMA
    rows = 2 * SLOTS
    out = pl.pallas_call(
        layer_kernel,
        out_shape=jax.ShapeDtypeStruct((TOK, width), BF16),
        in_specs=[scalars, near, near] + [far] * 5 + [near] * 4 + [far] + [near] * 4 + [far] * 3,
        out_specs=near,
        scratch_shapes=[
            pltpu.VMEM((17, 8, 1536), BF16),
            pltpu.VMEM((HEADS, 1, TOK), F32),
            pltpu.VMEM((HEADS, 1, TOK), F32),
            pltpu.VMEM((TOK, 1536), BF16),
            pltpu.VMEM((64, INNER), F32),
            pltpu.VMEM((2, 1, 512), F32),
            pltpu.VMEM((16, 8, 512), F32),
            pltpu.VMEM((16, 1, 512), F32),
            pltpu.VMEM((16, 8, 512), F32),
            pltpu.VMEM((64, INNER), F32),
            pltpu.VMEM((TOK, INNER), F32),
            pltpu.VMEM((INNER, width), BF16),
            pltpu.VMEM((TOK, width), F32),
            pltpu.VMEM((TOK, width), BF16),
            pltpu.VMEM((16 * SLOTS, TOK), BF16),
            pltpu.VMEM((3 * TOK, 16 * SLOTS), BF16),
            pltpu.VMEM((rows, 8, width), BF16),
            pltpu.VMEM((rows, 8, width), BF16),
            pltpu.VMEM((4, rows, 8, width), BF16),
            pltpu.VMEM((4, rows, 8, width), BF16),
            pltpu.VMEM((rows, 8, width), BF16),
            pltpu.VMEM((2, rows, 8, width), BF16),
            pltpu.VMEM((width, 2 * part), BF16),
            pltpu.VMEM((width, 2 * part), BF16),
            pltpu.VMEM((2 * part, width), BF16),
            pltpu.VMEM((192, 2 * part), BF16),
            dma((6,)), dma((3,)), dma((3,)), dma((2, 16)), dma((2, 16)), dma((2, 16)), dma((2, 16)),
            dma((16,)), dma((16,)), dma((3,)), dma((3,)), dma((3,)), dma((16,)), dma((16,)),
            dma((3, 4)), dma((3, 4)), dma((3, 4)), dma((3, 4)), dma((16,)), dma((16,)),
        ],
        compiler_params=pltpu.CompilerParams(
            collective_id=0, has_side_effects=True, vmem_limit_bytes=62 * 1024 * 1024
        ),
        name="layer",
    )(
        channel_fading_speed,
        skip_connection_stream[0],
        emitted_valve_unscaled[0],
        channel_source_mapped.reshape(16, 8, INNER),
        hidden_source_mapped.reshape(16, 8, 256),
        probe_mapped_values.reshape(16, 8, 256),
        increment_premapped.reshape(16, 1, TOK),
        extra_log_fading.reshape(16, 1, TOK),
        channel_source_kernel,
        hidden_source_kernel,
        probe_kernel_coefficients,
        cluster_scaling_factor[None, :],
        emitted_mapping_matrix,
        standardize_scaling[None, :],
        standardize_offset[None, :],
        chosen_specialist_ids[0].T,
        specialist_mixing_shares[0].T,
        specialist_gating_matrices[0],
        raising_matrices[0],
        lowering_matrices[0],
    )
    return out[None]


def solution(mesh):
    placed = (
        P("dp", "sp", None),
        P("dp", "sp", None),
        P("dp", "sp", None),
        P("dp", "sp", None),
        P("dp", "sp", None),
        P("dp", None, "sp"),
        P("dp", None, "sp"),
        P(),
        P(),
        P(),
        P(),
        P(),
        P(),
        P(),
        P(),
        P("dp", "sp", None),
        P("dp", "sp", None),
        P("sp", None, "dp"),
        P("sp", None, "dp"),
        P("sp", "dp", None),
    )
    return jax.shard_map(
        per_device, mesh=mesh, in_specs=placed, out_specs=P("dp", "sp", None), check_vma=False
    )
```

```python
import jax
import jax.numpy as jnp
from jax import lax
from jax.experimental import pallas as pl
from jax.experimental.pallas import tpu as pltpu
from jax.sharding import PartitionSpec as P

MESH = pl.DeviceIdType.MESH
HEADS = 16
HEAD_DIM = 64
TOK = 128
INNER = 1024
SLOTS = 24
NEAR = 1280
rms_eps = 1e-06
norm_eps = 1e-05
BF16 = jnp.bfloat16
F32 = jnp.float32
EXACT = lax.Precision.HIGHEST


def dot(a, b, precision=None):
    return jnp.dot(a, b, preferred_element_type=F32, precision=precision)


def dot_nt(a, b, precision=None):
    return lax.dot_general(
        a, b, (((1,), (1,)), ((), ())), preferred_element_type=F32, precision=precision
    )


def iota(shape, dim):
    return lax.broadcasted_iota(jnp.int32, shape, dim)


def layer_kernel(
    speed, skip, valve, chan, hid, probe, step_in, fade_in, tap_x, tap_b, tap_c, group_gain, out_w,
    gain, offset, ids, shares, gate_w, raise_w, lower_w,
    result,
    joined, rim, steps, fades, names, parts, conv, state, decay, state_in, decay_in, entering,
    entered, inside, out_v, pre, normed, placing, weighing, outgoing, answers,
    tokens, far_rows, far_answers, token_sum, token_out, token_relay, token_in,
    gathered, partial, relayed, summed, gate_v, raise_v, lower_v, hidden,
    load_sem, rim_send, rim_recv, name_send, name_recv, step_send, step_recv,
    state_send, state_recv, enter_send, enter_recv,
    weight_sem, weight_send, weight_recv, go_send, go_recv, ring_send, ring_recv,
    sum_send, sum_recv, back_send, back_recv, token_send, token_recv, far_send, far_recv,
    home_send, home_recv, tsum_send, tsum_recv,
):
    sp = lax.axis_index("sp")
    dp = lax.axis_index("dp")
    z, y = lax.div(sp, 4), lax.rem(sp, 4)
    x, core = lax.div(dp, 2), lax.rem(dp, 2)
    right = (sp, lax.rem(x + 1, 4) * 2 + core)
    left = (sp, lax.rem(x + 3, 4) * 2 + core)
    across = (sp, lax.rem(x + 2, 4) * 2 + core)
    twin = (sp, x * 2 + 1 - core)
    width = skip.shape[1]
    part = gate_w.shape[1]

    def ahead(o):
        i = lax.rem(o, 4)
        return lax.rem(z + i, 4) * 4 + lax.rem(y + i + lax.div(o, 4), 4)

    def behind(o):
        i = lax.rem(o, 4)
        return lax.rem(z + 4 - i, 4) * 4 + lax.rem(y + 8 - i - lax.div(o, 4), 4)

    def each(low, high, work):
        def step(o, carry):
            work(o)
            return carry

        lax.fori_loop(low, high, step, 0)

    barrier = pltpu.get_barrier_semaphore()
    each(
        1, 16,
        lambda o: pl.semaphore_signal(
            barrier, inc=1, device_id=(ahead(o), dp), device_id_type=MESH
        ),
    )
    for friend in (left, right, across, twin):
        pl.semaphore_signal(barrier, inc=1, device_id=friend, device_id_type=MESH)

    spans = ((chan, 0, INNER), (hid, INNER, 256), (probe, INNER + 256, 256))
    own_loads = [
        pltpu.make_async_copy(
            ref, joined.at[:, :, pl.ds(low, size)], load_sem.at[k]
        )
        for k, (ref, low, size) in enumerate(spans)
    ]
    own_loads.append(
        pltpu.make_async_copy(step_in.at[sp], steps.at[sp], load_sem.at[3])
    )
    own_loads.append(
        pltpu.make_async_copy(fade_in.at[sp], fades.at[sp], load_sem.at[4])
    )
    own_loads.append(pltpu.make_async_copy(ids, names.at[0], load_sem.at[6]))
    own_loads.append(pltpu.make_async_copy(shares, parts.at[0], load_sem.at[7]))
    out_load = pltpu.make_async_copy(out_w, out_v, load_sem.at[5])
    for copy in own_loads:
        copy.start()
    loads, gifts = [], []
    for k, (source, target) in enumerate(
        ((gate_w, gate_v), (raise_w, raise_v), (lower_w, lower_v))
    ):
        if k < 2:
            mine, theirs = target.at[:, pl.ds(0, part)], target.at[:, pl.ds(part, part)]
        else:
            mine, theirs = target.at[pl.ds(0, part)], target.at[pl.ds(part, part)]
        loads.append(pltpu.make_async_copy(source, mine, weight_sem.at[k]))
        gifts.append(
            pltpu.make_async_remote_copy(
                src_ref=source,
                dst_ref=theirs,
                send_sem=weight_send.at[k],
                recv_sem=weight_recv.at[k],
                device_id=twin,
                device_id_type=MESH,
            )
        )

    out_load.start()
    for copy in loads:
        copy.start()
    for copy in own_loads:
        copy.wait()

    def filtered(block, taps):
        high = block.shape[0] - 8
        running = taps[0:1] * block[5 : 5 + high]
        for k in range(1, 4):
            running = running + taps[k : k + 1] * block[5 + k : 5 + k + high]
        return jax.nn.silu(running).astype(BF16)

    def convolve(cols, taps):
        block = joined[:, :, cols].reshape(TOK, 256).astype(F32)
        block = jnp.concatenate([jnp.zeros((8, 256), F32), block], axis=0)
        conv[:, cols] = filtered(block, taps)

    def convolve_rim(cols, taps):
        before = rim[:, :, cols].reshape(8, 256).astype(F32) * (sp > 0).astype(F32)
        block = joined[0:2, :, cols].reshape(16, 256).astype(F32)
        conv[0:16, cols] = filtered(jnp.concatenate([before, block], axis=0), taps)

    def begin(work):
        def work_x(k):
            cols = pl.ds(pl.multiple_of(k * 256, 256), 256)
            work(cols, tap_x[:, cols])

        each(0, 4, work_x)
        work(pl.ds(INNER, 256), tap_b[...])
        work(pl.ds(INNER + 256, 256), tap_c[...])

    begin(convolve)
    pl.semaphore_wait(barrier, 19)

    def step_copy(o, source, target, which):
        return pltpu.make_async_remote_copy(
            src_ref=source.at[ahead(o)],
            dst_ref=target.at[sp],
            send_sem=step_send.at[which, o],
            recv_sem=step_recv.at[which, o],
            device_id=(ahead(o), dp),
            device_id_type=MESH,
        )

    def send_steps(o):
        step_copy(o, step_in, steps, 0).start()
        step_copy(o, fade_in, fades, 1).start()

    each(1, 16, send_steps)
    rims = [
        pltpu.make_async_remote_copy(
            src_ref=ref.at[pl.ds(15, 1)],
            dst_ref=rim.at[:, :, pl.ds(low, size)],
            send_sem=rim_send.at[k],
            recv_sem=rim_recv.at[k],
            device_id=(lax.rem(sp + 1, 16), dp),
            device_id_type=MESH,
        )
        for k, (ref, low, size) in enumerate(spans)
    ]
    for copy in rims:
        copy.start()
    notes = [
        pltpu.make_async_remote_copy(
            src_ref=ref,
            dst_ref=target.at[k + 1],
            send_sem=name_send.at[which, k],
            recv_sem=name_recv.at[which, k],
            device_id=friend,
            device_id_type=MESH,
        )
        for which, (ref, target) in enumerate(((ids, names), (shares, parts)))
        for k, friend in enumerate((right, left, across))
    ]
    for copy in notes + gifts:
        copy.start()
    for copy in rims:
        copy.wait_recv()
    begin(convolve_rim)

    def wait_steps(o):
        step_copy(o, step_in, steps, 0).wait_recv()
        step_copy(o, fade_in, fades, 1).wait_recv()

    each(1, 16, wait_steps)
    row = iota((HEADS, TOK), 0)
    speeds = jnp.zeros((HEADS, TOK), F32)
    for h in range(HEADS):
        speeds = jnp.where(row == h, speed[h], speeds)
    raw = steps[...].reshape(HEADS, TOK)
    step = jnp.maximum(raw, 0.0) + jnp.log1p(jnp.exp(-jnp.abs(raw)))
    fading = fades[...].reshape(HEADS, TOK) - speeds * step
    later = iota((TOK, TOK), 0)
    sooner = iota((TOK, TOK), 1)
    causal = later >= sooner
    triangle = causal.astype(F32)
    cum_row = dot_nt(fading, triangle, EXACT)
    cum_col = dot_nt(triangle, fading, EXACT)
    step_col = dot_nt((later == sooner).astype(F32), step, EXACT)
    spread = (lax.div(iota((HEADS, INNER), 1), HEAD_DIM) == iota((HEADS, INNER), 0)).astype(F32)
    last = cum_col[TOK - 1 : TOK]
    tail_wide = dot(jnp.exp(last - cum_col) * step_col, spread, EXACT)
    decay_wide = dot(jnp.broadcast_to(jnp.exp(last), (8, HEADS)), spread, EXACT)
    for k in range(2):
        decay[k] = decay_wide[0:1, 512 * k : 512 * k + 512]
    scaled = (conv[:, 0:INNER].astype(F32) * tail_wide).astype(BF16)
    for q in range(2):
        b_pair = conv[:, INNER + 128 * q : INNER + 128 * q + 128]
        both = dot(b_pair.T, scaled[:, 512 * q : 512 * q + 512])
        state[:, 512 * q : 512 * q + 256] = both[0:64, 0:256]
        state[:, 512 * q + 256 : 512 * q + 512] = both[64:128, 256:512]

    def place_of(k):
        return (
            pl.ds(pl.multiple_of(lax.div(k, 2) * 8, 8), 8),
            pl.ds(pl.multiple_of(lax.rem(k, 2) * 512, 512), 512),
        )

    def state_copy(o):
        rows, cols = place_of(ahead(o))
        return pltpu.make_async_remote_copy(
            src_ref=state.at[rows, cols],
            dst_ref=state_in.at[sp],
            send_sem=state_send.at[0, o],
            recv_sem=state_recv.at[0, o],
            device_id=(ahead(o), dp),
            device_id_type=MESH,
        )

    def decay_copy(o):
        return pltpu.make_async_remote_copy(
            src_ref=decay.at[lax.rem(ahead(o), 2)],
            dst_ref=decay_in.at[sp],
            send_sem=state_send.at[1, o],
            recv_sem=state_recv.at[1, o],
            device_id=(ahead(o), dp),
            device_id_type=MESH,
        )

    def send_state(o):
        decay_copy(o).start()
        state_copy(o).start()

    each(1, 16, send_state)
    my_rows, my_cols = place_of(sp)
    state_in[sp] = state[my_rows, my_cols]
    decay_in[sp] = decay[lax.rem(sp, 2)]

    low_half = iota((TOK, TOK), 1) < 64
    for q in range(2):
        b_pair = conv[:, INNER + 128 * q : INNER + 128 * q + 128]
        c_pair = conv[:, INNER + 256 + 128 * q : INNER + 256 + 128 * q + 128]
        for g in range(2):
            c_one = jnp.where(low_half == (g == 0), c_pair, jnp.zeros_like(c_pair))
            scores = dot_nt(c_one, b_pair)
            for i in range(2):
                first = 8 * q + 4 * g + 2 * i
                x_pair = conv[:, 64 * first : 64 * first + 128]
                total = None
                for h in (first, first + 1):
                    gap = jnp.where(
                        causal, cum_col[:, h : h + 1] - cum_row[h : h + 1, :], -1e30
                    )
                    mixing = (scores * jnp.exp(gap) * step[h : h + 1, :]).astype(BF16)
                    x_one = jnp.where(low_half == (h == first), x_pair, jnp.zeros_like(x_pair))
                    term = dot(mixing, x_one)
                    total = term if total is None else total + term
                inside[:, 64 * first : 64 * first + 128] = total

    def placing_rows(j):
        ids, shares = names[j], parts[j]
        expert = iota((16, TOK), 0)
        first, second = expert == ids[0:1, :], expert == ids[1:2, :]
        named = first | second
        share = jnp.where(first, shares[0:1, :], 0.0) + jnp.where(second, shares[1:2, :], 0.0)
        before = (later < sooner).astype(BF16)
        rank = dot(named.astype(F32).astype(BF16), before)
        rank = jnp.where(named, rank, -1.0)
        slot = iota((SLOTS, TOK), 0).astype(F32)
        chosen = jnp.concatenate(
            [(rank[e : e + 1, :] == slot).astype(F32) for e in range(16)], axis=0
        )
        weights = jnp.concatenate(
            [
                jnp.where(rank[e : e + 1, :] == slot, share[e : e + 1, :], 0.0)
                for e in range(16)
            ],
            axis=0,
        )
        placing[j] = chosen.astype(BF16)
        rest = weights.T
        for k in range(3):
            piece = rest.astype(BF16)
            weighing[j, pl.ds(TOK * k, TOK), :] = piece
            rest = rest - piece.astype(F32)

    placing_rows(0)
    for copy in notes:
        copy.wait_recv()
    for j in range(1, 4):
        placing_rows(j)

    def wait_state(o):
        decay_copy(o).wait_recv()
        state_copy(o).wait_recv()

    each(1, 16, wait_state)

    def advance(j, held):
        entering[j] = held
        return decay_in[j] * held + state_in[j]

    lax.fori_loop(0, 16, advance, jnp.zeros((8, 512), F32))

    def enter_copy(o):
        rows, cols = place_of(sp)
        return pltpu.make_async_remote_copy(
            src_ref=entering.at[ahead(o)],
            dst_ref=entered.at[rows, cols],
            send_sem=enter_send.at[o],
            recv_sem=enter_recv.at[o],
            device_id=(ahead(o), dp),
            device_id_type=MESH,
        )

    each(1, 16, lambda o: enter_copy(o).start())
    entered[my_rows, my_cols] = entering[sp]
    reach_wide = dot(jnp.exp(cum_col), spread, EXACT)
    each(1, 16, lambda o: enter_copy(o).wait_recv())

    nothing = jnp.zeros((64, 256), F32)
    blocks = []
    for q in range(2):
        c_pair = conv[:, INNER + 256 + 128 * q : INNER + 256 + 128 * q + 128]
        low, high = entered[:, 512 * q : 512 * q + 256], entered[:, 512 * q + 256 : 512 * q + 512]
        both = jnp.concatenate(
            [
                jnp.concatenate([low, nothing], axis=1),
                jnp.concatenate([nothing, high], axis=1),
            ],
            axis=0,
        )
        carried = dot(c_pair.astype(F32), both, EXACT)
        for g in range(2):
            low_col = 512 * q + 256 * g
            mixed = (
                inside[:, low_col : low_col + 256]
                + reach_wide[:, low_col : low_col + 256] * carried[:, 256 * g : 256 * g + 256]
            ).astype(BF16)
            gated = mixed.astype(F32) * jax.nn.silu(valve[:, low_col : low_col + 256].astype(F32))
            level = lax.rsqrt(jnp.mean(gated * gated, axis=1, keepdims=True) + rms_eps)
            blocks.append(
                (gated * level * group_gain[:, low_col : low_col + 256]).astype(BF16)
            )
    group_normed = jnp.concatenate(blocks, axis=1)
    out_load.wait()

    def project(k):
        cols = pl.ds(pl.multiple_of(k * 512, 512), 512)
        pre[:, cols] = skip[:, cols].astype(F32) + dot(group_normed, out_v[:, cols])

    each(0, width // 512, project)

    def standardize(k):
        rows = pl.ds(pl.multiple_of(k * 16, 16), 16)
        block = pre[rows, :]
        shifted = block - jnp.mean(block, axis=1, keepdims=True)
        level = lax.rsqrt(jnp.mean(shifted * shifted, axis=1, keepdims=True) + norm_eps)
        normed[rows, :] = (shifted * level * gain[...] + offset[...]).astype(BF16)

    far_cols = pl.ds(NEAR, width - NEAR)

    def token_copy(lane, half):
        rows = pl.ds(64 * half, 64)
        if lane < 2:
            source = normed.at[rows, far_cols]
        else:
            source = tokens.at[half, rows]
        return pltpu.make_async_remote_copy(
            src_ref=source,
            dst_ref=tokens.at[lane, rows],
            send_sem=token_send.at[lane, half],
            recv_sem=token_recv.at[lane, half],
            device_id=(right, left, (right, left)[half])[lane],
            device_id_type=MESH,
        )

    each(0, TOK // 32, standardize)
    token_copy(0, 0).start()
    token_copy(1, 0).start()
    each(TOK // 32, TOK // 16, standardize)
    token_copy(1, 1).start()
    token_copy(0, 1).start()
    flat_outgoing = outgoing.reshape(16 * SLOTS, width)

    def route(k):
        cols = pl.ds(pl.multiple_of(k * 512, 512), 512)
        flat_outgoing[:, cols] = dot(placing[0], normed[:, cols]).astype(BF16)

    each(0, width // 512, route)

    def go(o):
        return pltpu.make_async_remote_copy(
            src_ref=outgoing.at[pl.ds(3 * ahead(o), 3)],
            dst_ref=gathered.at[0, pl.ds(3 * o, 3)],
            send_sem=go_send.at[o],
            recv_sem=go_recv.at[o],
            device_id=(ahead(o), dp),
            device_id_type=MESH,
        )

    each(1, 16, lambda o: go(o).start())
    gathered[0, 0:3] = outgoing[pl.ds(3 * sp, 3)]

    near_cols = pl.ds(0, NEAR)

    def group(g):
        return pl.ds(12 * g, 12)

    def ring(src_slot, dst_slot, g, target, lane):
        return pltpu.make_async_remote_copy(
            src_ref=gathered.at[src_slot, group(g), :, near_cols],
            dst_ref=gathered.at[dst_slot, group(g), :, near_cols],
            send_sem=ring_send.at[lane, g],
            recv_sem=ring_recv.at[dst_slot - 1, g],
            device_id=target,
            device_id_type=MESH,
        )

    def to_right(g):
        return ring(0, 1, g, right, 0)

    def to_left(g):
        return ring(0, 2, g, left, 1)

    def onward(g):
        return ring(1, 3, g, right, 2) if g < 2 else ring(2, 3, g, left, 2)

    def far_copy(j, o):
        return pltpu.make_async_remote_copy(
            src_ref=far_rows.at[j - 1, pl.ds(3 * ahead(o), 3)],
            dst_ref=gathered.at[j, pl.ds(3 * o, 3), :, far_cols],
            send_sem=far_send.at[j - 1, o],
            recv_sem=far_recv.at[j - 1, o],
            device_id=(ahead(o), dp),
            device_id_type=MESH,
        )

    def route_far(j):
        flat = far_rows.at[j - 1].reshape(16 * SLOTS, width - NEAR)
        flat[...] = dot(placing[j], tokens[j - 1]).astype(BF16)
        each(1, 16, lambda o: far_copy(j, o).start())
        gathered[j, 0:3, :, NEAR:] = far_rows[j - 1, pl.ds(3 * sp, 3)]

    def wait_far(j, half):
        each(max(8 * half, 1), 8 * half + 8, lambda o: far_copy(j, o).wait_recv())

    def pass_on(g):
        each(max(4 * g, 1), 4 * g + 4, lambda o: go(o).wait_recv())
        to_right(g).start()
        to_left(g).start()

    token_copy(0, 0).wait_recv()
    token_copy(2, 0).start()
    token_copy(1, 1).wait_recv()
    token_copy(2, 1).start()
    token_copy(0, 1).wait_recv()
    route_far(1)
    token_copy(1, 0).wait_recv()
    route_far(2)
    pass_on(0)
    token_copy(2, 0).wait_recv()
    token_copy(2, 1).wait_recv()
    route_far(3)
    pass_on(1)
    for copy in loads:
        copy.wait()
    for copy in gifts:
        copy.wait()

    tile = 256

    def home_copy(j, o):
        return pltpu.make_async_remote_copy(
            src_ref=partial.at[j, pl.ds(3 * o, 3), :, far_cols],
            dst_ref=far_answers.at[j, pl.ds(3 * sp, 3)],
            send_sem=home_send.at[j, o],
            recv_sem=home_recv.at[j, o],
            device_id=(behind(o), dp),
            device_id_type=MESH,
        )

    def unit(slot, half):
        rows_here = gathered.at[slot, pl.ds(24 * half, 24)].reshape(192, width)
        block = rows_here[...]

        def up(k):
            cols = pl.ds(pl.multiple_of(k * tile, tile), tile)
            gate_val = jnp.dot(block, gate_v[:, cols], preferred_element_type=F32)
            up_val = jnp.dot(block, raise_v[:, cols], preferred_element_type=F32)
            hidden[:, cols] = (jax.nn.silu(gate_val) * up_val).astype(BF16)

        each(0, 2 * part // tile, up)
        target = partial.at[slot, pl.ds(24 * half, 24)].reshape(192, width)

        def down(k):
            cols = pl.ds(pl.multiple_of(k * tile, tile), tile)
            target[:, cols] = jnp.dot(
                hidden[...], lower_v[:, cols], preferred_element_type=F32
            ).astype(BF16)

        each(0, width // tile, down)
        each(max(8 * half, 1), 8 * half + 8, lambda o: home_copy(slot, o).start())
        if half == 0:
            far_answers[slot, pl.ds(3 * sp, 3)] = partial[slot, 0:3, :, NEAR:]

    def sum_direct(slot, g):
        side = 0 if slot == 2 else 1
        return pltpu.make_async_remote_copy(
            src_ref=partial.at[slot, group(g), :, near_cols],
            dst_ref=summed.at[side, group(g)],
            send_sem=sum_send.at[side, g],
            recv_sem=sum_recv.at[side, g],
            device_id=right if slot == 2 else left,
            device_id_type=MESH,
        )

    def sum_relay(g):
        return pltpu.make_async_remote_copy(
            src_ref=partial.at[3, group(g), :, near_cols],
            dst_ref=relayed.at[group(g)],
            send_sem=sum_send.at[2, g],
            recv_sem=sum_recv.at[2, g],
            device_id=right if g < 2 else left,
            device_id_type=MESH,
        )

    unit(0, 0)
    pass_on(2)
    pass_on(3)
    to_right(0).wait_recv()
    onward(0).start()
    unit(0, 1)
    to_right(1).wait_recv()
    onward(1).start()
    wait_far(1, 0)
    unit(1, 0)
    to_left(2).wait_recv()
    onward(2).start()
    to_left(0).wait_recv()
    to_left(1).wait_recv()
    wait_far(2, 0)
    unit(2, 0)
    to_left(3).wait_recv()
    onward(3).start()
    sum_direct(1, 0).start()
    sum_direct(1, 1).start()
    wait_far(2, 1)
    unit(2, 1)
    sum_direct(2, 2).start()
    sum_direct(2, 3).start()
    to_right(2).wait_recv()
    to_right(3).wait_recv()
    wait_far(1, 1)
    unit(1, 1)
    onward(0).wait_recv()
    onward(1).wait_recv()
    wait_far(3, 0)
    unit(3, 0)
    sum_relay(0).start()
    sum_relay(1).start()
    onward(2).wait_recv()
    onward(3).wait_recv()
    wait_far(3, 1)
    unit(3, 1)
    sum_relay(2).start()
    sum_relay(3).start()

    def combine(j):
        each(1, 16, lambda o: home_copy(j, o).wait_recv())
        flat = far_answers.at[j].reshape(16 * SLOTS, width - NEAR)
        terms = dot(weighing[j], flat[...])
        return terms[0:TOK] + terms[TOK : 2 * TOK] + terms[2 * TOK : 3 * TOK]

    def tsum_copy(lane, half):
        rows = pl.ds(64 * half, 64)
        if lane == 2:
            source, target = token_out.at[2, rows], token_relay.at[rows]
            device = (right, left)[half]
        else:
            source, target = token_out.at[lane, rows], token_in.at[lane, rows]
            device = (right, left)[lane]
        return pltpu.make_async_remote_copy(
            src_ref=source,
            dst_ref=target,
            send_sem=tsum_send.at[lane, half],
            recv_sem=tsum_recv.at[lane, half],
            device_id=device,
            device_id_type=MESH,
        )

    def relay_add(g):
        slot = 2 if g < 2 else 1
        sum_relay(g).wait_recv()
        partial[slot, group(g), :, 0:NEAR] = (
            partial[slot, group(g), :, 0:NEAR].astype(F32) + relayed[group(g)].astype(F32)
        ).astype(BF16)
        sum_direct(slot, g).start()

    token_out[1] = combine(1).astype(BF16)
    tsum_copy(1, 0).start()
    token_out[0] = combine(2).astype(BF16)
    tsum_copy(0, 1).start()
    relay_add(0)
    relay_add(2)
    token_out[2] = combine(3).astype(BF16)
    tsum_copy(2, 0).start()
    tsum_copy(2, 1).start()
    token_sum[...] = combine(0)
    relay_add(1)
    relay_add(3)
    for half in range(2):
        lane, rows = half, pl.ds(64 * half, 64)
        tsum_copy(2, half).wait_recv()
        token_out[lane, rows] = (
            token_out[lane, rows].astype(F32) + token_relay[rows].astype(F32)
        ).astype(BF16)
        tsum_copy(lane, half).start()

    def back(o):
        return pltpu.make_async_remote_copy(
            src_ref=partial.at[0, pl.ds(3 * o, 3), :, near_cols],
            dst_ref=answers.at[pl.ds(3 * sp, 3)],
            send_sem=back_send.at[o],
            recv_sem=back_recv.at[o],
            device_id=(behind(o), dp),
            device_id_type=MESH,
        )

    for g in (0, 2, 1, 3):
        sum_direct(2, g).wait_recv()
        sum_direct(1, g).wait_recv()
        partial[0, group(g), :, 0:NEAR] = (
            partial[0, group(g), :, 0:NEAR].astype(F32)
            + summed[0, group(g)].astype(F32)
            + summed[1, group(g)].astype(F32)
        ).astype(BF16)
        each(max(4 * g, 1), 4 * g + 4, lambda o: back(o).start())
        if g == 0:
            answers[pl.ds(3 * sp, 3)] = partial[0, 0:3, :, 0:NEAR]

    for copy in rims + notes:
        copy.wait_send()
    for lane in range(3):
        for half in range(2):
            token_copy(lane, half).wait_send()
            tsum_copy(lane, half).wait_send()
            if lane < 2:
                tsum_copy(lane, half).wait_recv()
    result[:, NEAR:] = (
        normed[:, NEAR:].astype(F32)
        + token_sum[...]
        + token_in[0].astype(F32)
        + token_in[1].astype(F32)
    ).astype(BF16)
    for g in range(4):
        to_right(g).wait_send()
        to_left(g).wait_send()
        onward(g).wait_send()
        sum_direct(1, g).wait_send()
        sum_direct(2, g).wait_send()
        sum_relay(g).wait_send()

    def drain(o):
        step_copy(o, step_in, steps, 0).wait_send()
        step_copy(o, fade_in, fades, 1).wait_send()
        decay_copy(o).wait_send()
        state_copy(o).wait_send()
        enter_copy(o).wait_send()
        go(o).wait_send()
        for j in range(4):
            if j > 0:
                far_copy(j, o).wait_send()
            home_copy(j, o).wait_send()
        back(o).wait_send()
        back(o).wait_recv()

    each(1, 16, drain)
    flat_answers = answers.reshape(16 * SLOTS, NEAR)

    def finish(k):
        cols = pl.ds(pl.multiple_of(k * 256, 256), 256)
        terms = dot(weighing[0], flat_answers[:, cols])
        routed = terms[0:TOK] + terms[TOK : 2 * TOK] + terms[2 * TOK : 3 * TOK]
        result[:, cols] = (normed[:, cols].astype(F32) + routed).astype(BF16)

    each(0, NEAR // 256, finish)


def per_device(
    skip_connection_stream,
    emitted_valve_unscaled,
    channel_source_mapped,
    hidden_source_mapped,
    probe_mapped_values,
    increment_premapped,
    extra_log_fading,
    channel_fading_speed,
    channel_source_kernel,
    hidden_source_kernel,
    probe_kernel_coefficients,
    cluster_scaling_factor,
    emitted_mapping_matrix,
    standardize_scaling,
    standardize_offset,
    chosen_specialist_ids,
    specialist_mixing_shares,
    specialist_gating_matrices,
    raising_matrices,
    lowering_matrices,
):
    width = skip_connection_stream.shape[2]
    part = specialist_gating_matrices.shape[2]
    far = pl.BlockSpec(memory_space=pl.ANY)
    near = pl.BlockSpec(memory_space=pltpu.VMEM)
    scalars = pl.BlockSpec(memory_space=pltpu.SMEM)
    dma = pltpu.SemaphoreType.DMA
    rows = 2 * SLOTS
    rest = width - NEAR
    out = pl.pallas_call(
        layer_kernel,
        out_shape=jax.ShapeDtypeStruct((TOK, width), BF16),
        in_specs=[scalars, near, near] + [far] * 5 + [near] * 4 + [far] + [near] * 2 + [far] * 5,
        out_specs=near,
        scratch_shapes=[
            pltpu.VMEM((16, 8, 1536), BF16),
            pltpu.VMEM((1, 8, 1536), BF16),
            pltpu.VMEM((HEADS, 1, TOK), F32),
            pltpu.VMEM((HEADS, 1, TOK), F32),
            pltpu.VMEM((4, 2, TOK), jnp.int32),
            pltpu.VMEM((4, 2, TOK), F32),
            pltpu.VMEM((TOK, 1536), BF16),
            pltpu.VMEM((64, INNER), F32),
            pltpu.VMEM((2, 1, 512), F32),
            pltpu.VMEM((16, 8, 512), F32),
            pltpu.VMEM((16, 1, 512), F32),
            pltpu.VMEM((16, 8, 512), F32),
            pltpu.VMEM((64, INNER), F32),
            pltpu.VMEM((TOK, INNER), F32),
            pltpu.VMEM((INNER, width), BF16),
            pltpu.VMEM((TOK, width), F32),
            pltpu.VMEM((TOK, width), BF16),
            pltpu.VMEM((4, 16 * SLOTS, TOK), BF16),
            pltpu.VMEM((4, 3 * TOK, 16 * SLOTS), BF16),
            pltpu.VMEM((rows, 8, width), BF16),
            pltpu.VMEM((rows, 8, NEAR), BF16),
            pltpu.VMEM((3, TOK, rest), BF16),
            pltpu.VMEM((3, rows, 8, rest), BF16),
            pltpu.VMEM((4, rows, 8, rest), BF16),
            pltpu.VMEM((TOK, rest), F32),
            pltpu.VMEM((3, TOK, rest), BF16),
            pltpu.VMEM((TOK, rest), BF16),
            pltpu.VMEM((2, TOK, rest), BF16),
            pltpu.VMEM((4, rows, 8, width), BF16),
            pltpu.VMEM((4, rows, 8, width), BF16),
            pltpu.VMEM((rows, 8, NEAR), BF16),
            pltpu.VMEM((2, rows, 8, NEAR), BF16),
            pltpu.VMEM((width, 2 * part), BF16),
            pltpu.VMEM((width, 2 * part), BF16),
            pltpu.VMEM((2 * part, width), BF16),
            pltpu.VMEM((192, 2 * part), BF16),
            dma((8,)), dma((3,)), dma((3,)), dma((2, 3)), dma((2, 3)), dma((2, 16)), dma((2, 16)), dma((2, 16)), dma((2, 16)),
            dma((16,)), dma((16,)), dma((3,)), dma((3,)), dma((3,)), dma((16,)), dma((16,)),
            dma((3, 4)), dma((3, 4)), dma((3, 4)), dma((3, 4)), dma((16,)), dma((16,)),
            dma((3, 2)), dma((3, 2)), dma((3, 16)), dma((3, 16)), dma((4, 16)), dma((4, 16)),
            dma((3, 2)), dma((3, 2)),
        ],
        compiler_params=pltpu.CompilerParams(
            collective_id=0, has_side_effects=True, vmem_limit_bytes=62 * 1024 * 1024
        ),
        name="layer",
    )(
        channel_fading_speed,
        skip_connection_stream[0],
        emitted_valve_unscaled[0],
        channel_source_mapped.reshape(16, 8, INNER),
        hidden_source_mapped.reshape(16, 8, 256),
        probe_mapped_values.reshape(16, 8, 256),
        increment_premapped.reshape(16, 1, TOK),
        extra_log_fading.reshape(16, 1, TOK),
        channel_source_kernel,
        hidden_source_kernel,
        probe_kernel_coefficients,
        cluster_scaling_factor[None, :],
        emitted_mapping_matrix,
        standardize_scaling[None, :],
        standardize_offset[None, :],
        chosen_specialist_ids[0].T,
        specialist_mixing_shares[0].T,
        specialist_gating_matrices[0],
        raising_matrices[0],
        lowering_matrices[0],
    )
    return out[None]


def solution(mesh):
    placed = (
        P("dp", "sp", None),
        P("dp", "sp", None),
        P("dp", "sp", None),
        P("dp", "sp", None),
        P("dp", "sp", None),
        P("dp", None, "sp"),
        P("dp", None, "sp"),
        P(),
        P(),
        P(),
        P(),
        P(),
        P(),
        P(),
        P(),
        P("dp", "sp", None),
        P("dp", "sp", None),
        P("sp", None, "dp"),
        P("sp", None, "dp"),
        P("sp", "dp", None),
    )
    return jax.shard_map(
        per_device, mesh=mesh, in_specs=placed, out_specs=P("dp", "sp", None), check_vma=False
    )
```

```python
import jax
import jax.numpy as jnp
from jax import lax
from jax.experimental import pallas as pl
from jax.experimental.pallas import tpu as pltpu
from jax.sharding import PartitionSpec as P

MESH = pl.DeviceIdType.MESH
HEADS = 16
HEAD_DIM = 64
TOK = 128
INNER = 1024
SLOTS = 24
NEAR = 1280
rms_eps = 1e-06
norm_eps = 1e-05
BF16 = jnp.bfloat16
F32 = jnp.float32
EXACT = lax.Precision.HIGHEST


def dot(a, b, precision=None):
    return jnp.dot(a, b, preferred_element_type=F32, precision=precision)


def dot_nt(a, b, precision=None):
    return lax.dot_general(
        a, b, (((1,), (1,)), ((), ())), preferred_element_type=F32, precision=precision
    )


def iota(shape, dim):
    return lax.broadcasted_iota(jnp.int32, shape, dim)


def layer_kernel(
    speed, skip_in, valve_in, chan, hid, probe, step_in, fade_in, tap_x, tap_b, tap_c, group_gain, out_w,
    gain, offset, ids, shares, gate_w, raise_w, lower_w,
    result,
    skip, valve, joined, rim, steps_out, fades_out, steps, fades, names, parts, conv, state, decay, state_in, decay_in, entering,
    entered, inside, out_v, pre, normed, placing, weighing, outgoing, answers,
    tokens, far_rows, far_answers, token_sum, token_out, token_relay, token_in,
    gathered, partial, relayed, summed, gate_v, raise_v, lower_v, hidden,
    load_sem, rim_send, rim_recv, name_send, name_recv, step_send, step_recv,
    state_send, state_recv, enter_send, enter_recv,
    weight_sem, weight_send, weight_recv, go_send, go_recv, ring_send, ring_recv,
    sum_send, sum_recv, back_send, back_recv, token_send, token_recv, far_send, far_recv,
    home_send, home_recv, tsum_send, tsum_recv,
):
    sp = lax.axis_index("sp")
    dp = lax.axis_index("dp")
    z, y = lax.div(sp, 4), lax.rem(sp, 4)
    x, core = lax.div(dp, 2), lax.rem(dp, 2)
    right = (sp, lax.rem(x + 1, 4) * 2 + core)
    left = (sp, lax.rem(x + 3, 4) * 2 + core)
    across = (sp, lax.rem(x + 2, 4) * 2 + core)
    twin = (sp, x * 2 + 1 - core)
    width = skip_in.shape[1]
    part = gate_w.shape[1]

    def ahead(o):
        i = lax.rem(o, 4)
        return lax.rem(z + i, 4) * 4 + lax.rem(y + i + lax.div(o, 4), 4)

    def behind(o):
        i = lax.rem(o, 4)
        return lax.rem(z + 4 - i, 4) * 4 + lax.rem(y + 8 - i - lax.div(o, 4), 4)

    def each(low, high, work):
        def step(o, carry):
            work(o)
            return carry

        lax.fori_loop(low, high, step, 0)

    barrier = pltpu.get_barrier_semaphore()
    each(
        1, 16,
        lambda o: pl.semaphore_signal(
            barrier, inc=1, device_id=(ahead(o), dp), device_id_type=MESH
        ),
    )
    for friend in (left, right, across, twin):
        pl.semaphore_signal(barrier, inc=1, device_id=friend, device_id_type=MESH)

    spans = ((chan, 0, INNER), (hid, INNER, 256), (probe, INNER + 256, 256))
    own_loads = [
        pltpu.make_async_copy(
            ref, joined.at[:, :, pl.ds(low, size)], load_sem.at[k]
        )
        for k, (ref, low, size) in enumerate(spans)
    ]
    own_loads.append(pltpu.make_async_copy(step_in, steps_out, load_sem.at[3]))
    own_loads.append(pltpu.make_async_copy(fade_in, fades_out, load_sem.at[4]))
    own_loads.append(pltpu.make_async_copy(ids, names.at[0], load_sem.at[6]))
    own_loads.append(pltpu.make_async_copy(shares, parts.at[0], load_sem.at[7]))
    out_load = pltpu.make_async_copy(out_w, out_v, load_sem.at[5])
    late_loads = [
        pltpu.make_async_copy(skip_in, skip, load_sem.at[8]),
        pltpu.make_async_copy(valve_in, valve, load_sem.at[9]),
    ]
    for copy in own_loads:
        copy.start()
    loads, gifts = [], []
    for k, (source, target) in enumerate(
        ((gate_w, gate_v), (raise_w, raise_v), (lower_w, lower_v))
    ):
        if k < 2:
            mine, theirs = target.at[:, pl.ds(0, part)], target.at[:, pl.ds(part, part)]
        else:
            mine, theirs = target.at[pl.ds(0, part)], target.at[pl.ds(part, part)]
        loads.append(pltpu.make_async_copy(source, mine, weight_sem.at[k]))
        gifts.append(
            pltpu.make_async_remote_copy(
                src_ref=source,
                dst_ref=theirs,
                send_sem=weight_send.at[k],
                recv_sem=weight_recv.at[k],
                device_id=twin,
                device_id_type=MESH,
            )
        )

    for copy in own_loads:
        copy.wait()
    for copy in late_loads:
        copy.start()
    out_load.start()
    for copy in loads:
        copy.start()

    def filtered(block, taps):
        high = block.shape[0] - 8
        running = taps[0:1] * block[5 : 5 + high]
        for k in range(1, 4):
            running = running + taps[k : k + 1] * block[5 + k : 5 + k + high]
        return jax.nn.silu(running).astype(BF16)

    def convolve(cols, taps):
        block = joined[:, :, cols].reshape(TOK, 256).astype(F32)
        block = jnp.concatenate([jnp.zeros((8, 256), F32), block], axis=0)
        conv[:, cols] = filtered(block, taps)

    def convolve_rim(cols, taps):
        before = rim[:, :, cols].reshape(8, 256).astype(F32) * (sp > 0).astype(F32)
        block = joined[0:2, :, cols].reshape(16, 256).astype(F32)
        conv[0:16, cols] = filtered(jnp.concatenate([before, block], axis=0), taps)

    def begin(work):
        def work_x(k):
            cols = pl.ds(pl.multiple_of(k * 256, 256), 256)
            work(cols, tap_x[:, cols])

        each(0, 4, work_x)
        work(pl.ds(INNER, 256), tap_b[...])
        work(pl.ds(INNER + 256, 256), tap_c[...])

    begin(convolve)
    pl.semaphore_wait(barrier, 19)

    def step_copy(o, source, target, which):
        return pltpu.make_async_remote_copy(
            src_ref=source.at[ahead(o)],
            dst_ref=target.at[sp],
            send_sem=step_send.at[which, o],
            recv_sem=step_recv.at[which, o],
            device_id=(ahead(o), dp),
            device_id_type=MESH,
        )

    def send_steps(o):
        step_copy(o, steps_out, steps, 0).start()
        step_copy(o, fades_out, fades, 1).start()

    each(1, 16, send_steps)
    steps[sp] = steps_out[sp]
    fades[sp] = fades_out[sp]
    rims = [
        pltpu.make_async_remote_copy(
            src_ref=joined.at[pl.ds(15, 1), :, pl.ds(low, size)],
            dst_ref=rim.at[:, :, pl.ds(low, size)],
            send_sem=rim_send.at[k],
            recv_sem=rim_recv.at[k],
            device_id=(lax.rem(sp + 1, 16), dp),
            device_id_type=MESH,
        )
        for k, (_, low, size) in enumerate(spans)
    ]
    for copy in rims:
        copy.start()
    notes = [
        pltpu.make_async_remote_copy(
            src_ref=target.at[0],
            dst_ref=target.at[k + 1],
            send_sem=name_send.at[which, k],
            recv_sem=name_recv.at[which, k],
            device_id=friend,
            device_id_type=MESH,
        )
        for which, target in enumerate((names, parts))
        for k, friend in enumerate((right, left, across))
    ]
    for copy in notes + gifts:
        copy.start()
    for copy in rims:
        copy.wait_recv()
    begin(convolve_rim)

    def wait_steps(o):
        step_copy(o, steps_out, steps, 0).wait_recv()
        step_copy(o, fades_out, fades, 1).wait_recv()

    each(1, 16, wait_steps)
    row = iota((HEADS, TOK), 0)
    speeds = jnp.zeros((HEADS, TOK), F32)
    for h in range(HEADS):
        speeds = jnp.where(row == h, speed[h], speeds)
    raw = steps[...].reshape(HEADS, TOK)
    step = jnp.maximum(raw, 0.0) + jnp.log1p(jnp.exp(-jnp.abs(raw)))
    fading = fades[...].reshape(HEADS, TOK) - speeds * step
    later = iota((TOK, TOK), 0)
    sooner = iota((TOK, TOK), 1)
    causal = later >= sooner
    triangle = causal.astype(F32)
    cum_row = dot_nt(fading, triangle, EXACT)
    cum_col = dot_nt(triangle, fading, EXACT)
    step_col = dot_nt((later == sooner).astype(F32), step, EXACT)
    spread = (lax.div(iota((HEADS, INNER), 1), HEAD_DIM) == iota((HEADS, INNER), 0)).astype(F32)
    last = cum_col[TOK - 1 : TOK]
    tail_wide = dot(jnp.exp(last - cum_col) * step_col, spread, EXACT)
    decay_wide = dot(jnp.broadcast_to(jnp.exp(last), (8, HEADS)), spread, EXACT)
    for k in range(4):
        decay[k] = decay_wide[0:1, 256 * k : 256 * k + 256]
    scaled = (conv[:, 0:INNER].astype(F32) * tail_wide).astype(BF16)
    for q in range(2):
        b_pair = conv[:, INNER + 128 * q : INNER + 128 * q + 128]
        both = dot(b_pair.T, scaled[:, 512 * q : 512 * q + 512])
        state[:, 512 * q : 512 * q + 256] = both[0:64, 0:256].astype(BF16)
        state[:, 512 * q + 256 : 512 * q + 512] = both[64:128, 256:512].astype(BF16)

    def place_of(k):
        return (
            pl.ds(pl.multiple_of(lax.div(k, 4) * 16, 16), 16),
            pl.ds(pl.multiple_of(lax.rem(k, 4) * 256, 256), 256),
        )

    def state_copy(o):
        rows, cols = place_of(ahead(o))
        return pltpu.make_async_remote_copy(
            src_ref=state.at[rows, cols],
            dst_ref=state_in.at[sp],
            send_sem=state_send.at[0, o],
            recv_sem=state_recv.at[0, o],
            device_id=(ahead(o), dp),
            device_id_type=MESH,
        )

    def decay_copy(o):
        return pltpu.make_async_remote_copy(
            src_ref=decay.at[lax.rem(ahead(o), 4)],
            dst_ref=decay_in.at[sp],
            send_sem=state_send.at[1, o],
            recv_sem=state_recv.at[1, o],
            device_id=(ahead(o), dp),
            device_id_type=MESH,
        )

    def send_state(o):
        decay_copy(o).start()
        state_copy(o).start()

    each(1, 16, send_state)
    my_rows, my_cols = place_of(sp)
    state_in[sp] = state[my_rows, my_cols]
    decay_in[sp] = decay[lax.rem(sp, 4)]

    low_half = iota((TOK, TOK), 1) < 64
    for q in range(2):
        b_pair = conv[:, INNER + 128 * q : INNER + 128 * q + 128]
        c_pair = conv[:, INNER + 256 + 128 * q : INNER + 256 + 128 * q + 128]
        for g in range(2):
            c_one = jnp.where(low_half == (g == 0), c_pair, jnp.zeros_like(c_pair))
            scores = dot_nt(c_one, b_pair)
            for i in range(2):
                first = 8 * q + 4 * g + 2 * i
                x_pair = conv[:, 64 * first : 64 * first + 128]
                total = None
                for h in (first, first + 1):
                    gap = jnp.where(
                        causal, cum_col[:, h : h + 1] - cum_row[h : h + 1, :], -1e30
                    )
                    mixing = (scores * jnp.exp(gap) * step[h : h + 1, :]).astype(BF16)
                    x_one = jnp.where(low_half == (h == first), x_pair, jnp.zeros_like(x_pair))
                    term = dot(mixing, x_one)
                    total = term if total is None else total + term
                inside[:, 64 * first : 64 * first + 128] = total

    def placing_rows(j):
        ids, shares = names[j], parts[j]
        expert = iota((16, TOK), 0)
        first, second = expert == ids[0:1, :], expert == ids[1:2, :]
        named = first | second
        share = jnp.where(first, shares[0:1, :], 0.0) + jnp.where(second, shares[1:2, :], 0.0)
        before = (later < sooner).astype(BF16)
        rank = dot(named.astype(F32).astype(BF16), before)
        rank = jnp.where(named, rank, -1.0)
        slot = iota((SLOTS, TOK), 0).astype(F32)
        chosen = jnp.concatenate(
            [(rank[e : e + 1, :] == slot).astype(F32) for e in range(16)], axis=0
        )
        weights = jnp.concatenate(
            [
                jnp.where(rank[e : e + 1, :] == slot, share[e : e + 1, :], 0.0)
                for e in range(16)
            ],
            axis=0,
        )
        placing[j] = chosen.astype(BF16)
        rest = weights.T
        for k in range(2):
            piece = rest.astype(BF16)
            weighing[j, pl.ds(TOK * k, TOK), :] = piece
            rest = rest - piece.astype(F32)

    placing_rows(0)
    for copy in notes:
        copy.wait_recv()
    for j in range(1, 4):
        placing_rows(j)

    def wait_state(o):
        decay_copy(o).wait_recv()
        state_copy(o).wait_recv()

    each(1, 16, wait_state)

    def advance(j, held):
        entering[j] = held.astype(BF16)
        return decay_in[j] * held + state_in[j].astype(F32)

    lax.fori_loop(0, 16, advance, jnp.zeros((16, 256), F32))

    def enter_copy(o):
        rows, cols = place_of(sp)
        return pltpu.make_async_remote_copy(
            src_ref=entering.at[ahead(o)],
            dst_ref=entered.at[rows, cols],
            send_sem=enter_send.at[o],
            recv_sem=enter_recv.at[o],
            device_id=(ahead(o), dp),
            device_id_type=MESH,
        )

    each(1, 16, lambda o: enter_copy(o).start())
    entered[my_rows, my_cols] = entering[sp]
    reach_wide = dot(jnp.exp(cum_col), spread, EXACT)
    each(1, 16, lambda o: enter_copy(o).wait_recv())

    for copy in late_loads:
        copy.wait()
    nothing = jnp.zeros((64, 256), BF16)
    blocks = []
    for q in range(2):
        c_pair = conv[:, INNER + 256 + 128 * q : INNER + 256 + 128 * q + 128]
        low, high = entered[:, 512 * q : 512 * q + 256], entered[:, 512 * q + 256 : 512 * q + 512]
        both = jnp.concatenate(
            [
                jnp.concatenate([low, nothing], axis=1),
                jnp.concatenate([nothing, high], axis=1),
            ],
            axis=0,
        )
        carried = dot(c_pair, both)
        for g in range(2):
            low_col = 512 * q + 256 * g
            mixed = (
                inside[:, low_col : low_col + 256]
                + reach_wide[:, low_col : low_col + 256] * carried[:, 256 * g : 256 * g + 256]
            ).astype(BF16)
            gated = mixed.astype(F32) * jax.nn.silu(valve[:, low_col : low_col + 256].astype(F32))
            level = lax.rsqrt(jnp.mean(gated * gated, axis=1, keepdims=True) + rms_eps)
            blocks.append(
                (gated * level * group_gain[:, low_col : low_col + 256]).astype(BF16)
            )
    group_normed = jnp.concatenate(blocks, axis=1)
    out_load.wait()

    def project(k):
        cols = pl.ds(pl.multiple_of(k * 512, 512), 512)
        pre[:, cols] = skip[:, cols].astype(F32) + dot(group_normed, out_v[:, cols])

    each(0, width // 512, project)

    def standardize(k):
        rows = pl.ds(64 * k, 64)
        block = pre[rows, :]
        shifted = block - jnp.mean(block, axis=1, keepdims=True)
        level = lax.rsqrt(jnp.mean(shifted * shifted, axis=1, keepdims=True) + norm_eps)
        normed[rows, :] = (shifted * level * gain[...] + offset[...]).astype(BF16)

    far_cols = pl.ds(NEAR, width - NEAR)

    def token_copy(lane, half):
        rows = pl.ds(64 * half, 64)
        if lane < 2:
            source = normed.at[rows, far_cols]
        else:
            source = tokens.at[half, rows]
        return pltpu.make_async_remote_copy(
            src_ref=source,
            dst_ref=tokens.at[lane, rows],
            send_sem=token_send.at[lane, half],
            recv_sem=token_recv.at[lane, half],
            device_id=(right, left, (right, left)[half])[lane],
            device_id_type=MESH,
        )

    standardize(0)
    token_copy(0, 0).start()
    token_copy(1, 0).start()
    standardize(1)
    token_copy(1, 1).start()
    token_copy(0, 1).start()
    flat_outgoing = outgoing.reshape(16 * SLOTS, width)

    def route(k):
        cols = pl.ds(pl.multiple_of(k * 512, 512), 512)
        flat_outgoing[:, cols] = dot(placing[0], normed[:, cols]).astype(BF16)

    each(0, width // 512, route)

    def go(o):
        return pltpu.make_async_remote_copy(
            src_ref=outgoing.at[pl.ds(3 * ahead(o), 3)],
            dst_ref=gathered.at[0, pl.ds(3 * o, 3)],
            send_sem=go_send.at[o],
            recv_sem=go_recv.at[o],
            device_id=(ahead(o), dp),
            device_id_type=MESH,
        )

    each(1, 16, lambda o: go(o).start())
    gathered[0, 0:3] = outgoing[pl.ds(3 * sp, 3)]

    near_cols = pl.ds(0, NEAR)

    def group(g):
        return pl.ds(12 * g, 12)

    def ring(src_slot, dst_slot, g, target, lane):
        return pltpu.make_async_remote_copy(
            src_ref=gathered.at[src_slot, group(g), :, near_cols],
            dst_ref=gathered.at[dst_slot, group(g), :, near_cols],
            send_sem=ring_send.at[lane, g],
            recv_sem=ring_recv.at[dst_slot - 1, g],
            device_id=target,
            device_id_type=MESH,
        )

    def to_right(g):
        return ring(0, 1, g, right, 0)

    def to_left(g):
        return ring(0, 2, g, left, 1)

    def onward(g):
        return ring(1, 3, g, right, 2) if g < 2 else ring(2, 3, g, left, 2)

    def far_copy(j, o):
        return pltpu.make_async_remote_copy(
            src_ref=far_rows.at[j - 1, pl.ds(3 * ahead(o), 3)],
            dst_ref=gathered.at[j, pl.ds(3 * o, 3), :, far_cols],
            send_sem=far_send.at[j - 1, o],
            recv_sem=far_recv.at[j - 1, o],
            device_id=(ahead(o), dp),
            device_id_type=MESH,
        )

    def route_far(j):
        flat = far_rows.at[j - 1].reshape(16 * SLOTS, width - NEAR)
        flat[...] = dot(placing[j], tokens[j - 1]).astype(BF16)
        each(1, 16, lambda o: far_copy(j, o).start())
        gathered[j, 0:3, :, NEAR:] = far_rows[j - 1, pl.ds(3 * sp, 3)]

    def wait_far(j, half):
        each(max(8 * half, 1), 8 * half + 8, lambda o: far_copy(j, o).wait_recv())

    def pass_on(g):
        each(max(4 * g, 1), 4 * g + 4, lambda o: go(o).wait_recv())
        to_right(g).start()
        to_left(g).start()

    token_copy(0, 0).wait_recv()
    token_copy(2, 0).start()
    token_copy(1, 1).wait_recv()
    token_copy(2, 1).start()
    token_copy(0, 1).wait_recv()
    route_far(1)
    token_copy(1, 0).wait_recv()
    route_far(2)
    pass_on(0)
    token_copy(2, 0).wait_recv()
    token_copy(2, 1).wait_recv()
    route_far(3)
    pass_on(1)
    for copy in loads:
        copy.wait()
    for copy in gifts:
        copy.wait()

    tile = 256

    def home_copy(j, o):
        return pltpu.make_async_remote_copy(
            src_ref=partial.at[j, pl.ds(3 * o, 3), :, far_cols],
            dst_ref=far_answers.at[j, pl.ds(3 * sp, 3)],
            send_sem=home_send.at[j, o],
            recv_sem=home_recv.at[j, o],
            device_id=(behind(o), dp),
            device_id_type=MESH,
        )

    def unit(slot, half):
        block = gathered.at[slot, pl.ds(24 * half, 24)].reshape(192, width)
        for k in range(2 * part // tile):
            cols = pl.ds(k * tile, tile)
            gate_val = dot(block[...], gate_v[:, cols])
            up_val = dot(block[...], raise_v[:, cols])
            hidden[:, cols] = (jax.nn.silu(gate_val) * up_val).astype(BF16)
        target = partial.at[slot, pl.ds(24 * half, 24)].reshape(192, width)
        for k in range(width // tile):
            cols = pl.ds(k * tile, tile)
            target[:, cols] = dot(hidden[...], lower_v[:, cols]).astype(BF16)
        each(jnp.maximum(8 * half, 1), 8 * half + 8, lambda o: home_copy(slot, o).start())

        @pl.when(half == 0)
        def _():
            far_answers[slot, pl.ds(3 * sp, 3)] = partial[slot, 0:3, :, NEAR:]

    def sum_direct(slot, g):
        side = 0 if slot == 2 else 1
        return pltpu.make_async_remote_copy(
            src_ref=partial.at[slot, group(g), :, near_cols],
            dst_ref=summed.at[side, group(g)],
            send_sem=sum_send.at[side, g],
            recv_sem=sum_recv.at[side, g],
            device_id=right if slot == 2 else left,
            device_id_type=MESH,
        )

    def sum_relay(g):
        return pltpu.make_async_remote_copy(
            src_ref=partial.at[3, group(g), :, near_cols],
            dst_ref=relayed.at[group(g)],
            send_sem=sum_send.at[2, g],
            recv_sem=sum_recv.at[2, g],
            device_id=right if g < 2 else left,
            device_id_type=MESH,
        )

    def combine(j):
        each(1, 16, lambda o: home_copy(j, o).wait_recv())
        flat = far_answers.at[j].reshape(16 * SLOTS, width - NEAR)
        terms = dot(weighing[j], flat[...])
        return terms[0:TOK] + terms[TOK : 2 * TOK]

    def tsum_copy(lane, half):
        rows = pl.ds(64 * half, 64)
        if lane == 2:
            source, target = token_out.at[2, rows], token_relay.at[rows]
            device = (right, left)[half]
        else:
            source, target = token_out.at[lane, rows], token_in.at[lane, rows]
            device = (right, left)[lane]
        return pltpu.make_async_remote_copy(
            src_ref=source,
            dst_ref=target,
            send_sem=tsum_send.at[lane, half],
            recv_sem=tsum_recv.at[lane, half],
            device_id=device,
            device_id_type=MESH,
        )

    def relay_add(g):
        slot = 2 if g < 2 else 1
        sum_relay(g).wait_recv()
        partial[slot, group(g), :, 0:NEAR] = (
            partial[slot, group(g), :, 0:NEAR].astype(F32) + relayed[group(g)].astype(F32)
        ).astype(BF16)
        sum_direct(slot, g).start()

    def before_own():
        pass_on(2)
        pass_on(3)
        to_right(0).wait_recv()
        onward(0).start()

    def before_left():
        to_right(1).wait_recv()
        onward(1).start()
        wait_far(1, 0)

    def before_right():
        to_left(0).wait_recv()
        to_left(1).wait_recv()
        wait_far(2, 0)

    def before_right_rest():
        to_left(2).wait_recv()
        onward(2).start()
        to_left(3).wait_recv()
        onward(3).start()
        sum_direct(1, 0).start()
        sum_direct(1, 1).start()
        wait_far(2, 1)

    def before_left_rest():
        sum_direct(2, 2).start()
        sum_direct(2, 3).start()
        to_right(2).wait_recv()
        to_right(3).wait_recv()
        wait_far(1, 1)

    def before_across():
        token_sum[...] = combine(0)
        onward(0).wait_recv()
        onward(1).wait_recv()
        wait_far(3, 0)

    def before_across_rest():
        sum_relay(0).start()
        sum_relay(1).start()
        token_out[0] = combine(2).astype(BF16)
        onward(2).wait_recv()
        onward(3).wait_recv()
        wait_far(3, 1)

    befores = (
        before_own, before_left, before_right, before_right_rest, before_left_rest,
        before_across, before_across_rest,
    )

    def turn(u):
        for k, before in enumerate(befores):
            pl.when(u == k + 1)(before)
        slot = jnp.where(u < 2, 0, jnp.where(u >= 6, 3, jnp.where((u == 2) | (u == 5), 1, 2)))
        half = jnp.where((u == 1) | (u == 4) | (u == 5) | (u == 7), 1, 0)
        unit(slot, half)

    each(0, 8, turn)
    sum_relay(2).start()
    sum_relay(3).start()
    token_out[1] = combine(1).astype(BF16)
    relay_add(0)
    relay_add(2)
    tsum_copy(0, 1).start()
    tsum_copy(1, 0).start()
    token_out[2] = combine(3).astype(BF16)
    relay_add(1)
    relay_add(3)
    tsum_copy(2, 0).start()
    tsum_copy(2, 1).start()
    def back(o):
        return pltpu.make_async_remote_copy(
            src_ref=partial.at[0, pl.ds(3 * o, 3), :, near_cols],
            dst_ref=answers.at[pl.ds(3 * sp, 3)],
            send_sem=back_send.at[o],
            recv_sem=back_recv.at[o],
            device_id=(behind(o), dp),
            device_id_type=MESH,
        )

    for g in (0, 2, 1, 3):
        sum_direct(2, g).wait_recv()
        sum_direct(1, g).wait_recv()
        partial[0, group(g), :, 0:NEAR] = (
            partial[0, group(g), :, 0:NEAR].astype(F32)
            + summed[0, group(g)].astype(F32)
            + summed[1, group(g)].astype(F32)
        ).astype(BF16)
        each(max(4 * g, 1), 4 * g + 4, lambda o: back(o).start())
        if g == 0:
            answers[pl.ds(3 * sp, 3)] = partial[0, 0:3, :, 0:NEAR]

    for half in range(2):
        lane, rows = half, pl.ds(64 * half, 64)
        tsum_copy(2, half).wait_recv()
        token_out[lane, rows] = (
            token_out[lane, rows].astype(F32) + token_relay[rows].astype(F32)
        ).astype(BF16)
        tsum_copy(lane, half).start()

    for copy in rims + notes:
        copy.wait_send()
    for lane in range(3):
        for half in range(2):
            token_copy(lane, half).wait_send()
            tsum_copy(lane, half).wait_send()
            if lane < 2:
                tsum_copy(lane, half).wait_recv()
    result[:, NEAR:] = (
        normed[:, NEAR:].astype(F32)
        + token_sum[...]
        + token_in[0].astype(F32)
        + token_in[1].astype(F32)
    ).astype(BF16)
    for g in range(4):
        to_right(g).wait_send()
        to_left(g).wait_send()
        onward(g).wait_send()
        sum_direct(1, g).wait_send()
        sum_direct(2, g).wait_send()
        sum_relay(g).wait_send()

    def drain(o):
        step_copy(o, steps_out, steps, 0).wait_send()
        step_copy(o, fades_out, fades, 1).wait_send()
        decay_copy(o).wait_send()
        state_copy(o).wait_send()
        enter_copy(o).wait_send()
        go(o).wait_send()
        for j in range(4):
            if j > 0:
                far_copy(j, o).wait_send()
            home_copy(j, o).wait_send()
        back(o).wait_send()
        back(o).wait_recv()

    each(1, 16, drain)
    flat_answers = answers.reshape(16 * SLOTS, NEAR)

    def finish(k):
        cols = pl.ds(pl.multiple_of(k * 256, 256), 256)
        terms = dot(weighing[0], flat_answers[:, cols])
        routed = terms[0:TOK] + terms[TOK : 2 * TOK]
        result[:, cols] = (normed[:, cols].astype(F32) + routed).astype(BF16)

    each(0, NEAR // 256, finish)


def per_device(
    skip_connection_stream,
    emitted_valve_unscaled,
    channel_source_mapped,
    hidden_source_mapped,
    probe_mapped_values,
    increment_premapped,
    extra_log_fading,
    channel_fading_speed,
    channel_source_kernel,
    hidden_source_kernel,
    probe_kernel_coefficients,
    cluster_scaling_factor,
    emitted_mapping_matrix,
    standardize_scaling,
    standardize_offset,
    chosen_specialist_ids,
    specialist_mixing_shares,
    specialist_gating_matrices,
    raising_matrices,
    lowering_matrices,
):
    width = skip_connection_stream.shape[2]
    part = specialist_gating_matrices.shape[2]
    far = pl.BlockSpec(memory_space=pl.ANY)
    near = pl.BlockSpec(memory_space=pltpu.VMEM)
    scalars = pl.BlockSpec(memory_space=pltpu.SMEM)
    dma = pltpu.SemaphoreType.DMA
    rows = 2 * SLOTS
    rest = width - NEAR
    out = pl.pallas_call(
        layer_kernel,
        out_shape=jax.ShapeDtypeStruct((TOK, width), BF16),
        in_specs=[scalars] + [far] * 7 + [near] * 4 + [far] + [near] * 2 + [far] * 5,
        out_specs=near,
        scratch_shapes=[
            pltpu.VMEM((TOK, width), BF16),
            pltpu.VMEM((TOK, INNER), BF16),
            pltpu.VMEM((16, 8, 1536), BF16),
            pltpu.VMEM((1, 8, 1536), BF16),
            pltpu.VMEM((HEADS, 1, TOK), F32),
            pltpu.VMEM((HEADS, 1, TOK), F32),
            pltpu.VMEM((HEADS, 1, TOK), F32),
            pltpu.VMEM((HEADS, 1, TOK), F32),
            pltpu.VMEM((4, 2, TOK), jnp.int32),
            pltpu.VMEM((4, 2, TOK), F32),
            pltpu.VMEM((TOK, 1536), BF16),
            pltpu.VMEM((64, INNER), BF16),
            pltpu.VMEM((4, 1, 256), F32),
            pltpu.VMEM((16, 16, 256), BF16),
            pltpu.VMEM((16, 1, 256), F32),
            pltpu.VMEM((16, 16, 256), BF16),
            pltpu.VMEM((64, INNER), BF16),
            pltpu.VMEM((TOK, INNER), F32),
            pltpu.VMEM((INNER, width), BF16),
            pltpu.VMEM((TOK, width), F32),
            pltpu.VMEM((TOK, width), BF16),
            pltpu.VMEM((4, 16 * SLOTS, TOK), BF16),
            pltpu.VMEM((4, 2 * TOK, 16 * SLOTS), BF16),
            pltpu.VMEM((rows, 8, width), BF16),
            pltpu.VMEM((rows, 8, NEAR), BF16),
            pltpu.VMEM((3, TOK, rest), BF16),
            pltpu.VMEM((3, rows, 8, rest), BF16),
            pltpu.VMEM((4, rows, 8, rest), BF16),
            pltpu.VMEM((TOK, rest), F32),
            pltpu.VMEM((3, TOK, rest), BF16),
            pltpu.VMEM((TOK, rest), BF16),
            pltpu.VMEM((2, TOK, rest), BF16),
            pltpu.VMEM((4, rows, 8, width), BF16),
            pltpu.VMEM((4, rows, 8, width), BF16),
            pltpu.VMEM((rows, 8, NEAR), BF16),
            pltpu.VMEM((2, rows, 8, NEAR), BF16),
            pltpu.VMEM((width, 2 * part), BF16),
            pltpu.VMEM((width, 2 * part), BF16),
            pltpu.VMEM((2 * part, width), BF16),
            pltpu.VMEM((192, 2 * part), BF16),
            dma((10,)), dma((3,)), dma((3,)), dma((2, 3)), dma((2, 3)), dma((2, 16)), dma((2, 16)), dma((2, 16)), dma((2, 16)),
            dma((16,)), dma((16,)), dma((3,)), dma((3,)), dma((3,)), dma((16,)), dma((16,)),
            dma((3, 4)), dma((3, 4)), dma((3, 4)), dma((3, 4)), dma((16,)), dma((16,)),
            dma((3, 2)), dma((3, 2)), dma((3, 16)), dma((3, 16)), dma((4, 16)), dma((4, 16)),
            dma((3, 2)), dma((3, 2)),
        ],
        compiler_params=pltpu.CompilerParams(
            collective_id=0, has_side_effects=True, vmem_limit_bytes=62 * 1024 * 1024
        ),
        name="layer",
    )(
        channel_fading_speed,
        skip_connection_stream[0],
        emitted_valve_unscaled[0],
        channel_source_mapped.reshape(16, 8, INNER),
        hidden_source_mapped.reshape(16, 8, 256),
        probe_mapped_values.reshape(16, 8, 256),
        increment_premapped.reshape(16, 1, TOK),
        extra_log_fading.reshape(16, 1, TOK),
        channel_source_kernel,
        hidden_source_kernel,
        probe_kernel_coefficients,
        cluster_scaling_factor[None, :],
        emitted_mapping_matrix,
        standardize_scaling[None, :],
        standardize_offset[None, :],
        chosen_specialist_ids[0].T,
        specialist_mixing_shares[0].T,
        specialist_gating_matrices[0],
        raising_matrices[0],
        lowering_matrices[0],
    )
    return out[None]


def solution(mesh):
    placed = (
        P("dp", "sp", None),
        P("dp", "sp", None),
        P("dp", "sp", None),
        P("dp", "sp", None),
        P("dp", "sp", None),
        P("dp", None, "sp"),
        P("dp", None, "sp"),
        P(),
        P(),
        P(),
        P(),
        P(),
        P(),
        P(),
        P(),
        P("dp", "sp", None),
        P("dp", "sp", None),
        P("sp", None, "dp"),
        P("sp", None, "dp"),
        P("sp", "dp", None),
    )
    return jax.shard_map(
        per_device, mesh=mesh, in_specs=placed, out_specs=P("dp", "sp", None), check_vma=False
    )
```

```python
import jax
import jax.numpy as jnp
from jax import lax
from jax.experimental import pallas as pl
from jax.experimental.pallas import tpu as pltpu
from jax.sharding import PartitionSpec as P

MESH = pl.DeviceIdType.MESH
HEADS = 16
HEAD_DIM = 64
TOK = 128
INNER = 1024
SLOTS = 24
NEAR = 1152
NEAR_BACK = 1152
rms_eps = 1e-06
norm_eps = 1e-05
BF16 = jnp.bfloat16
F32 = jnp.float32
EXACT = lax.Precision.HIGHEST


def dot(a, b, precision=None):
    return jnp.dot(a, b, preferred_element_type=F32, precision=precision)


def dot_nt(a, b, precision=None):
    return lax.dot_general(
        a, b, (((1,), (1,)), ((), ())), preferred_element_type=F32, precision=precision
    )


def iota(shape, dim):
    return lax.broadcasted_iota(jnp.int32, shape, dim)


def layer_kernel(
    speed, skip_in, valve_in, chan, hid, probe, step_in, fade_in, tap_x, tap_b, tap_c, group_gain, out_w,
    gain, offset, ids, shares, gate_w, raise_w, lower_w,
    result,
    skip, valve, joined, rim, steps_out, fades_out, steps, fades, names, parts, conv, state, decay, state_in, decay_in, entering,
    entered, inside, out_v, pre, normed, placing, weighing, outgoing, answers,
    tokens, far_rows, far_answers, token_sum, token_out, token_relay, token_in,
    gathered, partial, relayed, summed, gate_v, raise_v, lower_v, hidden,
    load_sem, rim_send, rim_recv, name_send, name_recv, step_send, step_recv,
    state_send, state_recv, enter_send, enter_recv,
    weight_sem, weight_send, weight_recv, go_send, go_recv, ring_send, ring_recv,
    sum_send, sum_recv, back_send, back_recv, token_send, token_recv, far_send, far_recv,
    home_send, home_recv, tsum_send, tsum_recv,
):
    sp = lax.axis_index("sp")
    dp = lax.axis_index("dp")
    z, y = lax.div(sp, 4), lax.rem(sp, 4)
    x, core = lax.div(dp, 2), lax.rem(dp, 2)
    right = (sp, lax.rem(x + 1, 4) * 2 + core)
    left = (sp, lax.rem(x + 3, 4) * 2 + core)
    across = (sp, lax.rem(x + 2, 4) * 2 + core)
    twin = (sp, x * 2 + 1 - core)
    width = skip_in.shape[1]
    part = gate_w.shape[1]

    def ahead(o):
        i = lax.rem(o, 4)
        return lax.rem(z + i, 4) * 4 + lax.rem(y + i + lax.div(o, 4), 4)

    def behind(o):
        i = lax.rem(o, 4)
        return lax.rem(z + 4 - i, 4) * 4 + lax.rem(y + 8 - i - lax.div(o, 4), 4)

    def each(low, high, work):
        def step(o, carry):
            work(o)
            return carry

        lax.fori_loop(low, high, step, 0)

    barrier = pltpu.get_barrier_semaphore()
    each(
        1, 16,
        lambda o: pl.semaphore_signal(
            barrier, inc=1, device_id=(ahead(o), dp), device_id_type=MESH
        ),
    )
    for friend in (left, right, across, twin):
        pl.semaphore_signal(barrier, inc=1, device_id=friend, device_id_type=MESH)

    spans = ((chan, 0, INNER), (hid, INNER, 256), (probe, INNER + 256, 256))
    own_loads = [
        pltpu.make_async_copy(
            ref, joined.at[:, :, pl.ds(low, size)], load_sem.at[k]
        )
        for k, (ref, low, size) in enumerate(spans)
    ]
    own_loads.append(pltpu.make_async_copy(step_in, steps_out, load_sem.at[3]))
    own_loads.append(pltpu.make_async_copy(fade_in, fades_out, load_sem.at[4]))
    own_loads.append(pltpu.make_async_copy(ids, names.at[0], load_sem.at[6]))
    own_loads.append(pltpu.make_async_copy(shares, parts.at[0], load_sem.at[7]))
    out_load = pltpu.make_async_copy(out_w, out_v, load_sem.at[5])
    late_loads = [
        pltpu.make_async_copy(skip_in, skip, load_sem.at[8]),
        pltpu.make_async_copy(valve_in, valve, load_sem.at[9]),
    ]
    for copy in own_loads:
        copy.start()
    loads, gifts = [], []
    for k, (source, target) in enumerate(
        ((gate_w, gate_v), (raise_w, raise_v), (lower_w, lower_v))
    ):
        if k < 2:
            mine, theirs = target.at[:, pl.ds(0, part)], target.at[:, pl.ds(part, part)]
        else:
            mine, theirs = target.at[pl.ds(0, part)], target.at[pl.ds(part, part)]
        loads.append(pltpu.make_async_copy(source, mine, weight_sem.at[k]))
        gifts.append(
            pltpu.make_async_remote_copy(
                src_ref=source,
                dst_ref=theirs,
                send_sem=weight_send.at[k],
                recv_sem=weight_recv.at[k],
                device_id=twin,
                device_id_type=MESH,
            )
        )

    for copy in own_loads:
        copy.wait()
    for copy in late_loads:
        copy.start()
    out_load.start()
    for copy in loads:
        copy.start()

    def filtered(block, taps):
        high = block.shape[0] - 8
        running = taps[0:1] * block[5 : 5 + high]
        for k in range(1, 4):
            running = running + taps[k : k + 1] * block[5 + k : 5 + k + high]
        return jax.nn.silu(running).astype(BF16)

    def convolve(cols, taps):
        block = joined[:, :, cols].reshape(TOK, 256).astype(F32)
        block = jnp.concatenate([jnp.zeros((8, 256), F32), block], axis=0)
        conv[:, cols] = filtered(block, taps)

    def convolve_rim(cols, taps):
        before = rim[:, :, cols].reshape(8, 256).astype(F32) * (sp > 0).astype(F32)
        block = joined[0:2, :, cols].reshape(16, 256).astype(F32)
        conv[0:16, cols] = filtered(jnp.concatenate([before, block], axis=0), taps)

    def begin(work):
        def work_x(k):
            cols = pl.ds(pl.multiple_of(k * 256, 256), 256)
            work(cols, tap_x[:, cols])

        each(0, 4, work_x)
        work(pl.ds(INNER, 256), tap_b[...])
        work(pl.ds(INNER + 256, 256), tap_c[...])

    begin(convolve)
    pl.semaphore_wait(barrier, 19)

    def step_copy(o, source, target, which):
        return pltpu.make_async_remote_copy(
            src_ref=source.at[ahead(o)],
            dst_ref=target.at[sp],
            send_sem=step_send.at[which, o],
            recv_sem=step_recv.at[which, o],
            device_id=(ahead(o), dp),
            device_id_type=MESH,
        )

    def send_steps(o):
        step_copy(o, steps_out, steps, 0).start()
        step_copy(o, fades_out, fades, 1).start()

    each(1, 16, send_steps)
    steps[sp] = steps_out[sp]
    fades[sp] = fades_out[sp]
    rims = [
        pltpu.make_async_remote_copy(
            src_ref=joined.at[pl.ds(15, 1), :, pl.ds(low, size)],
            dst_ref=rim.at[:, :, pl.ds(low, size)],
            send_sem=rim_send.at[k],
            recv_sem=rim_recv.at[k],
            device_id=(lax.rem(sp + 1, 16), dp),
            device_id_type=MESH,
        )
        for k, (_, low, size) in enumerate(spans)
    ]
    for copy in rims:
        copy.start()
    notes = [
        pltpu.make_async_remote_copy(
            src_ref=target.at[0],
            dst_ref=target.at[k + 1],
            send_sem=name_send.at[which, k],
            recv_sem=name_recv.at[which, k],
            device_id=friend,
            device_id_type=MESH,
        )
        for which, target in enumerate((names, parts))
        for k, friend in enumerate((right, left, across))
    ]
    for copy in notes + gifts:
        copy.start()
    for copy in rims:
        copy.wait_recv()
    begin(convolve_rim)

    def wait_steps(o):
        step_copy(o, steps_out, steps, 0).wait_recv()
        step_copy(o, fades_out, fades, 1).wait_recv()

    each(1, 16, wait_steps)
    row = iota((HEADS, TOK), 0)
    speeds = jnp.zeros((HEADS, TOK), F32)
    for h in range(HEADS):
        speeds = jnp.where(row == h, speed[h], speeds)
    raw = steps[...].reshape(HEADS, TOK)
    step = jnp.maximum(raw, 0.0) + jnp.log1p(jnp.exp(-jnp.abs(raw)))
    fading = fades[...].reshape(HEADS, TOK) - speeds * step
    later = iota((TOK, TOK), 0)
    sooner = iota((TOK, TOK), 1)
    causal = later >= sooner
    triangle = causal.astype(F32)
    cum_row = dot_nt(fading, triangle, EXACT)
    cum_col = dot_nt(triangle, fading, EXACT)
    step_col = dot_nt((later == sooner).astype(F32), step, EXACT)
    spread = (lax.div(iota((HEADS, INNER), 1), HEAD_DIM) == iota((HEADS, INNER), 0)).astype(F32)
    last = cum_col[TOK - 1 : TOK]
    tail_wide = dot(jnp.exp(last - cum_col) * step_col, spread, EXACT)
    decay_wide = dot(jnp.broadcast_to(jnp.exp(last), (8, HEADS)), spread, EXACT)
    for k in range(4):
        decay[k] = decay_wide[0:1, 256 * k : 256 * k + 256]
    scaled = (conv[:, 0:INNER].astype(F32) * tail_wide).astype(BF16)
    for q in range(2):
        b_pair = conv[:, INNER + 128 * q : INNER + 128 * q + 128]
        both = dot(b_pair.T, scaled[:, 512 * q : 512 * q + 512])
        state[:, 512 * q : 512 * q + 256] = both[0:64, 0:256].astype(BF16)
        state[:, 512 * q + 256 : 512 * q + 512] = both[64:128, 256:512].astype(BF16)

    def place_of(k):
        return (
            pl.ds(pl.multiple_of(lax.div(k, 4) * 16, 16), 16),
            pl.ds(pl.multiple_of(lax.rem(k, 4) * 256, 256), 256),
        )

    def state_copy(o):
        rows, cols = place_of(ahead(o))
        return pltpu.make_async_remote_copy(
            src_ref=state.at[rows, cols],
            dst_ref=state_in.at[sp],
            send_sem=state_send.at[0, o],
            recv_sem=state_recv.at[0, o],
            device_id=(ahead(o), dp),
            device_id_type=MESH,
        )

    def decay_copy(o):
        return pltpu.make_async_remote_copy(
            src_ref=decay.at[lax.rem(ahead(o), 4)],
            dst_ref=decay_in.at[sp],
            send_sem=state_send.at[1, o],
            recv_sem=state_recv.at[1, o],
            device_id=(ahead(o), dp),
            device_id_type=MESH,
        )

    def send_state(o):
        decay_copy(o).start()
        state_copy(o).start()

    each(1, 16, send_state)
    my_rows, my_cols = place_of(sp)
    state_in[sp] = state[my_rows, my_cols]
    decay_in[sp] = decay[lax.rem(sp, 4)]

    low_half = iota((TOK, TOK), 1) < 64
    for q in range(2):
        b_pair = conv[:, INNER + 128 * q : INNER + 128 * q + 128]
        c_pair = conv[:, INNER + 256 + 128 * q : INNER + 256 + 128 * q + 128]
        for g in range(2):
            c_one = jnp.where(low_half == (g == 0), c_pair, jnp.zeros_like(c_pair))
            scores = dot_nt(c_one, b_pair)
            for i in range(2):
                first = 8 * q + 4 * g + 2 * i
                x_pair = conv[:, 64 * first : 64 * first + 128]
                total = None
                for h in (first, first + 1):
                    gap = jnp.where(
                        causal, cum_col[:, h : h + 1] - cum_row[h : h + 1, :], -1e30
                    )
                    mixing = (scores * jnp.exp(gap) * step[h : h + 1, :]).astype(BF16)
                    x_one = jnp.where(low_half == (h == first), x_pair, jnp.zeros_like(x_pair))
                    term = dot(mixing, x_one)
                    total = term if total is None else total + term
                inside[:, 64 * first : 64 * first + 128] = total

    def placing_rows(j):
        ids, shares = names[j], parts[j]
        expert = iota((16, TOK), 0)
        first, second = expert == ids[0:1, :], expert == ids[1:2, :]
        named = first | second
        share = jnp.where(first, shares[0:1, :], 0.0) + jnp.where(second, shares[1:2, :], 0.0)
        before = (later < sooner).astype(BF16)
        rank = dot(named.astype(F32).astype(BF16), before)
        rank = jnp.where(named, rank, -1.0)
        slot = iota((SLOTS, TOK), 0).astype(F32)
        chosen = jnp.concatenate(
            [(rank[e : e + 1, :] == slot).astype(F32) for e in range(16)], axis=0
        )
        weights = jnp.concatenate(
            [
                jnp.where(rank[e : e + 1, :] == slot, share[e : e + 1, :], 0.0)
                for e in range(16)
            ],
            axis=0,
        )
        placing[j] = chosen.astype(BF16)
        rest = weights.T
        for k in range(2):
            piece = rest.astype(BF16)
            weighing[j, pl.ds(TOK * k, TOK), :] = piece
            rest = rest - piece.astype(F32)

    placing_rows(0)
    for copy in notes:
        copy.wait_recv()
    for j in range(1, 4):
        placing_rows(j)

    def wait_state(o):
        decay_copy(o).wait_recv()
        state_copy(o).wait_recv()

    each(1, 16, wait_state)

    def advance(j, held):
        entering[j] = held.astype(BF16)
        return decay_in[j] * held + state_in[j].astype(F32)

    lax.fori_loop(0, 16, advance, jnp.zeros((16, 256), F32))

    def enter_copy(o):
        rows, cols = place_of(sp)
        return pltpu.make_async_remote_copy(
            src_ref=entering.at[ahead(o)],
            dst_ref=entered.at[rows, cols],
            send_sem=enter_send.at[o],
            recv_sem=enter_recv.at[o],
            device_id=(ahead(o), dp),
            device_id_type=MESH,
        )

    each(1, 16, lambda o: enter_copy(o).start())
    entered[my_rows, my_cols] = entering[sp]
    reach_wide = dot(jnp.exp(cum_col), spread, EXACT)
    each(1, 16, lambda o: enter_copy(o).wait_recv())

    for copy in late_loads:
        copy.wait()
    nothing = jnp.zeros((64, 256), BF16)
    blocks = []
    for q in range(2):
        c_pair = conv[:, INNER + 256 + 128 * q : INNER + 256 + 128 * q + 128]
        low, high = entered[:, 512 * q : 512 * q + 256], entered[:, 512 * q + 256 : 512 * q + 512]
        both = jnp.concatenate(
            [
                jnp.concatenate([low, nothing], axis=1),
                jnp.concatenate([nothing, high], axis=1),
            ],
            axis=0,
        )
        carried = dot(c_pair, both)
        for g in range(2):
            low_col = 512 * q + 256 * g
            mixed = (
                inside[:, low_col : low_col + 256]
                + reach_wide[:, low_col : low_col + 256] * carried[:, 256 * g : 256 * g + 256]
            ).astype(BF16)
            gated = mixed.astype(F32) * jax.nn.silu(valve[:, low_col : low_col + 256].astype(F32))
            level = lax.rsqrt(jnp.mean(gated * gated, axis=1, keepdims=True) + rms_eps)
            blocks.append(
                (gated * level * group_gain[:, low_col : low_col + 256]).astype(BF16)
            )
    group_normed = jnp.concatenate(blocks, axis=1)
    out_load.wait()

    def project(k):
        cols = pl.ds(512 * k, 512)
        pre[:, cols] = skip[:, cols].astype(F32) + dot(group_normed, out_v[:, cols])

    for k in range(width // 512):
        project(k)

    def standardize(k):
        rows = pl.ds(64 * k, 64)
        block = pre[rows, :]
        shifted = block - jnp.mean(block, axis=1, keepdims=True)
        level = lax.rsqrt(jnp.mean(shifted * shifted, axis=1, keepdims=True) + norm_eps)
        normed[rows, :] = (shifted * level * gain[...] + offset[...]).astype(BF16)

    far_cols = pl.ds(NEAR, width - NEAR)

    def token_copy(lane, half):
        rows = pl.ds(64 * half, 64)
        if lane < 2:
            source = normed.at[rows, far_cols]
        else:
            source = tokens.at[half, rows]
        return pltpu.make_async_remote_copy(
            src_ref=source,
            dst_ref=tokens.at[lane, rows],
            send_sem=token_send.at[lane, half],
            recv_sem=token_recv.at[lane, half],
            device_id=(right, left, (right, left)[half])[lane],
            device_id_type=MESH,
        )

    standardize(0)
    token_copy(0, 0).start()
    token_copy(1, 0).start()
    standardize(1)
    token_copy(1, 1).start()
    token_copy(0, 1).start()
    flat_outgoing = outgoing.reshape(16 * SLOTS, width)

    def route(k):
        cols = pl.ds(512 * k, 512)
        flat_outgoing[:, cols] = dot(placing[0], normed[:, cols]).astype(BF16)

    for k in range(width // 512):
        route(k)

    def go(o):
        return pltpu.make_async_remote_copy(
            src_ref=outgoing.at[pl.ds(3 * ahead(o), 3)],
            dst_ref=gathered.at[0, pl.ds(3 * o, 3)],
            send_sem=go_send.at[o],
            recv_sem=go_recv.at[o],
            device_id=(ahead(o), dp),
            device_id_type=MESH,
        )

    each(1, 16, lambda o: go(o).start())
    gathered[0, 0:3] = outgoing[pl.ds(3 * sp, 3)]

    near_cols = pl.ds(0, NEAR)
    near_back = pl.ds(0, NEAR_BACK)
    far_back = pl.ds(NEAR_BACK, width - NEAR_BACK)

    def group(g):
        return pl.ds(12 * g, 12)

    def ring(src_slot, dst_slot, g, target, lane):
        return pltpu.make_async_remote_copy(
            src_ref=gathered.at[src_slot, group(g), :, near_cols],
            dst_ref=gathered.at[dst_slot, group(g), :, near_cols],
            send_sem=ring_send.at[lane, g],
            recv_sem=ring_recv.at[dst_slot - 1, g],
            device_id=target,
            device_id_type=MESH,
        )

    def to_right(g):
        return ring(0, 1, g, right, 0)

    def to_left(g):
        return ring(0, 2, g, left, 1)

    def onward(g):
        return ring(1, 3, g, right, 2) if g < 2 else ring(2, 3, g, left, 2)

    def far_copy(j, o):
        return pltpu.make_async_remote_copy(
            src_ref=far_rows.at[j - 1, pl.ds(3 * ahead(o), 3)],
            dst_ref=gathered.at[j, pl.ds(3 * o, 3), :, far_cols],
            send_sem=far_send.at[j - 1, o],
            recv_sem=far_recv.at[j - 1, o],
            device_id=(ahead(o), dp),
            device_id_type=MESH,
        )

    def route_far(j):
        flat = far_rows.at[j - 1].reshape(16 * SLOTS, width - NEAR)
        flat[...] = dot(placing[j], tokens[j - 1]).astype(BF16)
        gathered[j, 0:3, :, NEAR:] = far_rows[j - 1, pl.ds(3 * sp, 3)]

    def send_far(j, half):
        each(max(8 * half, 1), 8 * half + 8, lambda o: far_copy(j, o).start())

    def wait_far(j, half):
        each(max(8 * half, 1), 8 * half + 8, lambda o: far_copy(j, o).wait_recv())

    def pass_on(g):
        each(max(4 * g, 1), 4 * g + 4, lambda o: go(o).wait_recv())
        to_right(g).start()
        to_left(g).start()

    token_copy(0, 0).wait_recv()
    token_copy(2, 0).start()
    token_copy(1, 1).wait_recv()
    token_copy(2, 1).start()
    token_copy(0, 1).wait_recv()
    route_far(1)
    send_far(1, 0)
    token_copy(1, 0).wait_recv()
    route_far(2)
    send_far(2, 0)
    send_far(2, 1)
    send_far(1, 1)
    pass_on(0)
    token_copy(2, 0).wait_recv()
    token_copy(2, 1).wait_recv()
    route_far(3)
    send_far(3, 0)
    send_far(3, 1)
    pass_on(1)
    for copy in loads:
        copy.wait()
    for copy in gifts:
        copy.wait()

    tile = 256

    def home_copy(j, o):
        return pltpu.make_async_remote_copy(
            src_ref=partial.at[j, pl.ds(3 * o, 3), :, far_back],
            dst_ref=far_answers.at[j, pl.ds(3 * sp, 3)],
            send_sem=home_send.at[j, o],
            recv_sem=home_recv.at[j, o],
            device_id=(behind(o), dp),
            device_id_type=MESH,
        )

    def unit(slot, half):
        block = gathered.at[slot, pl.ds(24 * half, 24)].reshape(192, width)
        for k in range(2 * part // tile):
            cols = pl.ds(k * tile, tile)
            gate_val = dot(block[...], gate_v[:, cols])
            up_val = dot(block[...], raise_v[:, cols])
            hidden[:, cols] = (jax.nn.silu(gate_val) * up_val).astype(BF16)
        target = partial.at[slot, pl.ds(24 * half, 24)].reshape(192, width)
        for k in range(width // tile):
            cols = pl.ds(k * tile, tile)
            target[:, cols] = dot(hidden[...], lower_v[:, cols]).astype(BF16)
        each(jnp.maximum(8 * half, 1), 8 * half + 8, lambda o: home_copy(slot, o).start())

        @pl.when(half == 0)
        def _():
            far_answers[slot, pl.ds(3 * sp, 3)] = partial[slot, 0:3, :, NEAR_BACK:]

    def sum_direct(slot, g):
        side = 0 if slot == 2 else 1
        return pltpu.make_async_remote_copy(
            src_ref=partial.at[slot, group(g), :, near_back],
            dst_ref=summed.at[side, group(g)],
            send_sem=sum_send.at[side, g],
            recv_sem=sum_recv.at[side, g],
            device_id=right if slot == 2 else left,
            device_id_type=MESH,
        )

    def sum_relay(g):
        return pltpu.make_async_remote_copy(
            src_ref=partial.at[3, group(g), :, near_back],
            dst_ref=relayed.at[group(g)],
            send_sem=sum_send.at[2, g],
            recv_sem=sum_recv.at[2, g],
            device_id=right if g < 2 else left,
            device_id_type=MESH,
        )

    def combine(j):
        each(1, 16, lambda o: home_copy(j, o).wait_recv())
        flat = far_answers.at[j].reshape(16 * SLOTS, width - NEAR_BACK)
        terms = dot(weighing[j], flat[...])
        return terms[0:TOK] + terms[TOK : 2 * TOK]

    def tsum_copy(lane, half):
        rows = pl.ds(64 * half, 64)
        if lane == 2:
            source, target = token_out.at[2, rows], token_relay.at[rows]
            device = (right, left)[half]
        else:
            source, target = token_out.at[lane, rows], token_in.at[lane, rows]
            device = (right, left)[lane]
        return pltpu.make_async_remote_copy(
            src_ref=source,
            dst_ref=target,
            send_sem=tsum_send.at[lane, half],
            recv_sem=tsum_recv.at[lane, half],
            device_id=device,
            device_id_type=MESH,
        )

    def relay_add(g):
        slot = 2 if g < 2 else 1
        sum_relay(g).wait_recv()
        partial[slot, group(g), :, 0:NEAR_BACK] = (
            partial[slot, group(g), :, 0:NEAR_BACK].astype(F32) + relayed[group(g)].astype(F32)
        ).astype(BF16)
        sum_direct(slot, g).start()

    def before_own():
        pass_on(2)
        pass_on(3)
        to_right(0).wait_recv()
        onward(0).start()

    def before_left():
        to_right(1).wait_recv()
        onward(1).start()
        wait_far(1, 0)

    def before_right():
        to_left(0).wait_recv()
        to_left(1).wait_recv()
        wait_far(2, 0)

    def before_right_rest():
        to_left(2).wait_recv()
        onward(2).start()
        to_left(3).wait_recv()
        onward(3).start()
        sum_direct(1, 0).start()
        sum_direct(1, 1).start()
        wait_far(2, 1)

    def before_left_rest():
        sum_direct(2, 2).start()
        sum_direct(2, 3).start()
        to_right(2).wait_recv()
        to_right(3).wait_recv()
        wait_far(1, 1)

    def before_across():
        onward(0).wait_recv()
        onward(1).wait_recv()
        wait_far(3, 0)

    def before_across_rest():
        sum_relay(0).start()
        sum_relay(1).start()
        onward(2).wait_recv()
        onward(3).wait_recv()
        wait_far(3, 1)

    befores = (
        before_own, before_left, before_right, before_right_rest, before_left_rest,
        before_across, before_across_rest,
    )

    def turn(u):
        for k, before in enumerate(befores):
            pl.when(u == k + 1)(before)
        slot = jnp.where(u < 2, 0, jnp.where(u >= 6, 3, jnp.where((u == 2) | (u == 5), 1, 2)))
        half = jnp.where((u == 1) | (u == 4) | (u == 5) | (u == 7), 1, 0)
        unit(slot, half)

    each(0, 8, turn)
    sum_relay(2).start()
    sum_relay(3).start()
    relay_add(0)
    relay_add(2)
    relay_add(1)
    relay_add(3)
    token_out[0] = combine(2).astype(BF16)
    tsum_copy(0, 1).start()
    token_out[1] = combine(1).astype(BF16)
    tsum_copy(1, 0).start()

    def back(o):
        return pltpu.make_async_remote_copy(
            src_ref=partial.at[0, pl.ds(3 * o, 3), :, near_back],
            dst_ref=answers.at[pl.ds(3 * sp, 3)],
            send_sem=back_send.at[o],
            recv_sem=back_recv.at[o],
            device_id=(behind(o), dp),
            device_id_type=MESH,
        )

    def settle(g):
        sum_direct(2, g).wait_recv()
        sum_direct(1, g).wait_recv()
        partial[0, group(g), :, 0:NEAR_BACK] = (
            partial[0, group(g), :, 0:NEAR_BACK].astype(F32)
            + summed[0, group(g)].astype(F32)
            + summed[1, group(g)].astype(F32)
        ).astype(BF16)
        each(max(4 * g, 1), 4 * g + 4, lambda o: back(o).start())
        if g == 0:
            answers[pl.ds(3 * sp, 3)] = partial[0, 0:3, :, 0:NEAR_BACK]

    settle(0)
    settle(2)
    token_out[2] = combine(3).astype(BF16)
    tsum_copy(2, 0).start()
    tsum_copy(2, 1).start()
    settle(1)
    settle(3)
    for half in range(2):
        lane, rows = half, pl.ds(64 * half, 64)
        tsum_copy(2, half).wait_recv()
        token_out[lane, rows] = (
            token_out[lane, rows].astype(F32) + token_relay[rows].astype(F32)
        ).astype(BF16)
        tsum_copy(lane, half).start()

    token_sum[...] = combine(0)
    for copy in rims + notes:
        copy.wait_send()
    for lane in range(3):
        for half in range(2):
            token_copy(lane, half).wait_send()
            tsum_copy(lane, half).wait_send()
            if lane < 2:
                tsum_copy(lane, half).wait_recv()
    result[:, NEAR_BACK:] = (
        normed[:, NEAR_BACK:].astype(F32)
        + token_sum[...]
        + token_in[0].astype(F32)
        + token_in[1].astype(F32)
    ).astype(BF16)
    for g in range(4):
        to_right(g).wait_send()
        to_left(g).wait_send()
        onward(g).wait_send()
        sum_direct(1, g).wait_send()
        sum_direct(2, g).wait_send()
        sum_relay(g).wait_send()

    def drain(o):
        step_copy(o, steps_out, steps, 0).wait_send()
        step_copy(o, fades_out, fades, 1).wait_send()
        decay_copy(o).wait_send()
        state_copy(o).wait_send()
        enter_copy(o).wait_send()
        go(o).wait_send()
        for j in range(4):
            if j > 0:
                far_copy(j, o).wait_send()
            home_copy(j, o).wait_send()
        back(o).wait_send()
        back(o).wait_recv()

    each(1, 16, drain)
    flat_answers = answers.reshape(16 * SLOTS, NEAR_BACK)

    def finish(k, size):
        cols = pl.ds(k, size)
        terms = dot(weighing[0], flat_answers[:, cols])
        routed = terms[0:TOK] + terms[TOK : 2 * TOK]
        result[:, cols] = (normed[:, cols].astype(F32) + routed).astype(BF16)

    for k in range(0, NEAR_BACK, 512):
        finish(k, min(512, NEAR_BACK - k))


def per_device(
    skip_connection_stream,
    emitted_valve_unscaled,
    channel_source_mapped,
    hidden_source_mapped,
    probe_mapped_values,
    increment_premapped,
    extra_log_fading,
    channel_fading_speed,
    channel_source_kernel,
    hidden_source_kernel,
    probe_kernel_coefficients,
    cluster_scaling_factor,
    emitted_mapping_matrix,
    standardize_scaling,
    standardize_offset,
    chosen_specialist_ids,
    specialist_mixing_shares,
    specialist_gating_matrices,
    raising_matrices,
    lowering_matrices,
):
    width = skip_connection_stream.shape[2]
    part = specialist_gating_matrices.shape[2]
    far = pl.BlockSpec(memory_space=pl.ANY)
    near = pl.BlockSpec(memory_space=pltpu.VMEM)
    scalars = pl.BlockSpec(memory_space=pltpu.SMEM)
    dma = pltpu.SemaphoreType.DMA
    rows = 2 * SLOTS
    rest = width - NEAR_BACK
    out = pl.pallas_call(
        layer_kernel,
        out_shape=pltpu.VMEM((TOK, width), BF16),
        in_specs=[scalars] + [far] * 7 + [near] * 4 + [far] + [near] * 2 + [far] * 5,
        out_specs=near,
        scratch_shapes=[
            pltpu.VMEM((TOK, width), BF16),
            pltpu.VMEM((TOK, INNER), BF16),
            pltpu.VMEM((16, 8, 1536), BF16),
            pltpu.VMEM((1, 8, 1536), BF16),
            pltpu.VMEM((HEADS, 1, TOK), F32),
            pltpu.VMEM((HEADS, 1, TOK), F32),
            pltpu.VMEM((HEADS, 1, TOK), F32),
            pltpu.VMEM((HEADS, 1, TOK), F32),
            pltpu.VMEM((4, 2, TOK), jnp.int32),
            pltpu.VMEM((4, 2, TOK), F32),
            pltpu.VMEM((TOK, 1536), BF16),
            pltpu.VMEM((64, INNER), BF16),
            pltpu.VMEM((4, 1, 256), F32),
            pltpu.VMEM((16, 16, 256), BF16),
            pltpu.VMEM((16, 1, 256), F32),
            pltpu.VMEM((16, 16, 256), BF16),
            pltpu.VMEM((64, INNER), BF16),
            pltpu.VMEM((TOK, INNER), F32),
            pltpu.VMEM((INNER, width), BF16),
            pltpu.VMEM((TOK, width), F32),
            pltpu.VMEM((TOK, width), BF16),
            pltpu.VMEM((4, 16 * SLOTS, TOK), BF16),
            pltpu.VMEM((4, 2 * TOK, 16 * SLOTS), BF16),
            pltpu.VMEM((rows, 8, width), BF16),
            pltpu.VMEM((rows, 8, NEAR_BACK), BF16),
            pltpu.VMEM((3, TOK, width - NEAR), BF16),
            pltpu.VMEM((3, rows, 8, width - NEAR), BF16),
            pltpu.VMEM((4, rows, 8, rest), BF16),
            pltpu.VMEM((TOK, rest), F32),
            pltpu.VMEM((3, TOK, rest), BF16),
            pltpu.VMEM((TOK, rest), BF16),
            pltpu.VMEM((2, TOK, rest), BF16),
            pltpu.VMEM((4, rows, 8, width), BF16),
            pltpu.VMEM((4, rows, 8, width), BF16),
            pltpu.VMEM((rows, 8, NEAR_BACK), BF16),
            pltpu.VMEM((2, rows, 8, NEAR_BACK), BF16),
            pltpu.VMEM((width, 2 * part), BF16),
            pltpu.VMEM((width, 2 * part), BF16),
            pltpu.VMEM((2 * part, width), BF16),
            pltpu.VMEM((192, 2 * part), BF16),
            dma((10,)), dma((3,)), dma((3,)), dma((2, 3)), dma((2, 3)), dma((2, 16)), dma((2, 16)), dma((2, 16)), dma((2, 16)),
            dma((16,)), dma((16,)), dma((3,)), dma((3,)), dma((3,)), dma((16,)), dma((16,)),
            dma((3, 4)), dma((3, 4)), dma((3, 4)), dma((3, 4)), dma((16,)), dma((16,)),
            dma((3, 2)), dma((3, 2)), dma((3, 16)), dma((3, 16)), dma((4, 16)), dma((4, 16)),
            dma((3, 2)), dma((3, 2)),
        ],
        compiler_params=pltpu.CompilerParams(
            collective_id=0, has_side_effects=True, vmem_limit_bytes=62 * 1024 * 1024
        ),
        name="layer",
    )(
        channel_fading_speed,
        skip_connection_stream[0],
        emitted_valve_unscaled[0],
        channel_source_mapped.reshape(16, 8, INNER),
        hidden_source_mapped.reshape(16, 8, 256),
        probe_mapped_values.reshape(16, 8, 256),
        increment_premapped.reshape(16, 1, TOK),
        extra_log_fading.reshape(16, 1, TOK),
        channel_source_kernel,
        hidden_source_kernel,
        probe_kernel_coefficients,
        cluster_scaling_factor[None, :],
        emitted_mapping_matrix,
        standardize_scaling[None, :],
        standardize_offset[None, :],
        chosen_specialist_ids[0].T,
        specialist_mixing_shares[0].T,
        specialist_gating_matrices[0],
        raising_matrices[0],
        lowering_matrices[0],
    )
    return out[None]


def solution(mesh):
    placed = (
        P("dp", "sp", None),
        P("dp", "sp", None),
        P("dp", "sp", None),
        P("dp", "sp", None),
        P("dp", "sp", None),
        P("dp", None, "sp"),
        P("dp", None, "sp"),
        P(),
        P(),
        P(),
        P(),
        P(),
        P(),
        P(),
        P(),
        P("dp", "sp", None),
        P("dp", "sp", None),
        P("sp", None, "dp"),
        P("sp", None, "dp"),
        P("sp", "dp", None),
    )
    return jax.shard_map(
        per_device, mesh=mesh, in_specs=placed, out_specs=P("dp", "sp", None), check_vma=False
    )
```

```python
import jax
import jax.numpy as jnp
from jax import lax
from jax.experimental import pallas as pl
from jax.experimental.pallas import tpu as pltpu
from jax.sharding import PartitionSpec as P

MESH = pl.DeviceIdType.MESH
HEADS = 16
HEAD_DIM = 64
TOK = 128
INNER = 1024
SLOTS = 24
NEAR = 1280
NEAR_BACK = 1280
rms_eps = 1e-06
norm_eps = 1e-05
BF16 = jnp.bfloat16
F32 = jnp.float32


def dot(a, b):
    return jnp.dot(a, b, preferred_element_type=F32)


def thirds(a):
    parts = []
    for _ in range(3):
        part = a.astype(BF16)
        parts.append(part)
        a = a - part.astype(F32)
    return jnp.concatenate(parts, axis=1)


def dot_nt(a, b):
    return lax.dot_general(a, b, (((1,), (1,)), ((), ())), preferred_element_type=F32)


def iota(shape, dim):
    return lax.broadcasted_iota(jnp.int32, shape, dim)


def layer_kernel(
    speed_in, skip_in, valve_in, chan, hid, probe, step_in, fade_in, tap_x_in, tap_b_in, tap_c_in,
    group_gain_in, out_w, gain_in, offset_in, ids, shares, gate_w, raise_w, lower_w,
    result,
    speed, tap_x, tap_b, tap_c, group_gain, gain, offset, skip, valve, joined, rim, steps_out, fades_out, steps, fades, names, parts, conv, state, decay, state_in, decay_in, entering,
    entered, inside, out_v, pre, normed, placing, weighing, outgoing, answers,
    tokens, far_rows, far_answers, token_sum, token_out, token_relay, token_in,
    gathered, partial, relayed, summed, gate_v, raise_v, lower_v, hidden,
    load_sem, rim_send, rim_recv, name_send, name_recv, step_send, step_recv,
    state_send, state_recv, enter_send, enter_recv,
    weight_sem, weight_send, weight_recv, go_send, go_recv, ring_send, ring_recv,
    sum_send, sum_recv, back_send, back_recv, token_send, token_recv, far_send, far_recv,
    home_send, home_recv, tsum_send, tsum_recv,
):
    sp = lax.axis_index("sp")
    dp = lax.axis_index("dp")
    z, y = lax.div(sp, 4), lax.rem(sp, 4)
    x, core = lax.div(dp, 2), lax.rem(dp, 2)
    right = (sp, lax.rem(x + 1, 4) * 2 + core)
    left = (sp, lax.rem(x + 3, 4) * 2 + core)
    across = (sp, lax.rem(x + 2, 4) * 2 + core)
    twin = (sp, x * 2 + 1 - core)
    width = skip_in.shape[1]
    part = gate_w.shape[1]

    def ahead(o):
        i = lax.rem(o, 4)
        return lax.rem(z + i, 4) * 4 + lax.rem(y + i + lax.div(o, 4), 4)

    def behind(o):
        i = lax.rem(o, 4)
        return lax.rem(z + 4 - i, 4) * 4 + lax.rem(y + 8 - i - lax.div(o, 4), 4)

    def each(low, high, work):
        def step(o, carry):
            work(o)
            return carry

        lax.fori_loop(low, high, step, 0)

    barrier = pltpu.get_barrier_semaphore()
    each(
        1, 16,
        lambda o: pl.semaphore_signal(
            barrier, inc=1, device_id=(ahead(o), dp), device_id_type=MESH
        ),
    )
    for friend in (left, right, across, twin):
        pl.semaphore_signal(barrier, inc=1, device_id=friend, device_id_type=MESH)

    spans = ((chan, 0, INNER), (hid, INNER, 256), (probe, INNER + 256, 256))
    own_loads = [
        pltpu.make_async_copy(
            ref, joined.at[:, :, pl.ds(low, size)], load_sem.at[k]
        )
        for k, (ref, low, size) in enumerate(spans)
    ]
    own_loads.append(pltpu.make_async_copy(step_in, steps_out, load_sem.at[3]))
    own_loads.append(pltpu.make_async_copy(fade_in, fades_out, load_sem.at[4]))
    own_loads.append(pltpu.make_async_copy(ids, names.at[0], load_sem.at[6]))
    own_loads.append(pltpu.make_async_copy(shares, parts.at[0], load_sem.at[7]))
    out_load = pltpu.make_async_copy(out_w, out_v, load_sem.at[5])
    for k, (source, target) in enumerate(
        ((tap_x_in, tap_x), (tap_b_in, tap_b), (tap_c_in, tap_c), (speed_in, speed))
    ):
        own_loads.append(pltpu.make_async_copy(source, target, load_sem.at[10 + k]))
    late_loads = [
        pltpu.make_async_copy(group_gain_in, group_gain, load_sem.at[14]),
        pltpu.make_async_copy(gain_in, gain, load_sem.at[15]),
        pltpu.make_async_copy(offset_in, offset, load_sem.at[16]),
        pltpu.make_async_copy(skip_in, skip, load_sem.at[8]),
        pltpu.make_async_copy(valve_in, valve, load_sem.at[9]),
    ]
    for copy in own_loads:
        copy.start()
    loads, gifts = [], []
    for k, (source, target) in enumerate(
        ((gate_w, gate_v), (raise_w, raise_v), (lower_w, lower_v))
    ):
        if k < 2:
            mine, theirs = target.at[:, pl.ds(0, part)], target.at[:, pl.ds(part, part)]
        else:
            mine, theirs = target.at[pl.ds(0, part)], target.at[pl.ds(part, part)]
        loads.append(pltpu.make_async_copy(source, mine, weight_sem.at[k]))
        gifts.append(
            pltpu.make_async_remote_copy(
                src_ref=source,
                dst_ref=theirs,
                send_sem=weight_send.at[k],
                recv_sem=weight_recv.at[k],
                device_id=twin,
                device_id_type=MESH,
            )
        )

    for copy in own_loads:
        copy.wait()
    for copy in late_loads:
        copy.start()
    out_load.start()
    for copy in loads:
        copy.start()

    def filtered(block, taps):
        high = block.shape[0] - 8
        running = taps[0:1] * block[5 : 5 + high]
        for k in range(1, 4):
            running = running + taps[k : k + 1] * block[5 + k : 5 + k + high]
        return jax.nn.silu(running).astype(BF16)

    def convolve(cols, taps):
        block = joined[:, :, cols].reshape(TOK, 256).astype(F32)
        block = jnp.concatenate([jnp.zeros((8, 256), F32), block], axis=0)
        conv[:, cols] = filtered(block, taps)

    def convolve_rim(cols, taps):
        before = rim[:, :, cols].reshape(8, 256).astype(F32) * (sp > 0).astype(F32)
        block = joined[0:2, :, cols].reshape(16, 256).astype(F32)
        conv[0:16, cols] = filtered(jnp.concatenate([before, block], axis=0), taps)

    def begin(work):
        def work_x(k):
            cols = pl.ds(pl.multiple_of(k * 256, 256), 256)
            work(cols, tap_x[:, cols])

        each(0, 4, work_x)
        work(pl.ds(INNER, 256), tap_b[...])
        work(pl.ds(INNER + 256, 256), tap_c[...])

    begin(convolve)
    pl.semaphore_wait(barrier, 19)

    def step_copy(o, source, target, which):
        return pltpu.make_async_remote_copy(
            src_ref=source.at[ahead(o)],
            dst_ref=target.at[sp],
            send_sem=step_send.at[which, o],
            recv_sem=step_recv.at[which, o],
            device_id=(ahead(o), dp),
            device_id_type=MESH,
        )

    def send_steps(o):
        step_copy(o, steps_out, steps, 0).start()
        step_copy(o, fades_out, fades, 1).start()

    each(1, 16, send_steps)
    steps[sp] = steps_out[sp]
    fades[sp] = fades_out[sp]
    rims = [
        pltpu.make_async_remote_copy(
            src_ref=joined.at[pl.ds(15, 1), :, pl.ds(low, size)],
            dst_ref=rim.at[:, :, pl.ds(low, size)],
            send_sem=rim_send.at[k],
            recv_sem=rim_recv.at[k],
            device_id=(lax.rem(sp + 1, 16), dp),
            device_id_type=MESH,
        )
        for k, (_, low, size) in enumerate(spans)
    ]
    for copy in rims:
        copy.start()
    notes = [
        pltpu.make_async_remote_copy(
            src_ref=target.at[0],
            dst_ref=target.at[k + 1],
            send_sem=name_send.at[which, k],
            recv_sem=name_recv.at[which, k],
            device_id=friend,
            device_id_type=MESH,
        )
        for which, target in enumerate((names, parts))
        for k, friend in enumerate((right, left, across))
    ]
    for copy in notes + gifts:
        copy.start()
    for copy in rims:
        copy.wait_recv()
    begin(convolve_rim)

    def wait_steps(o):
        step_copy(o, steps_out, steps, 0).wait_recv()
        step_copy(o, fades_out, fades, 1).wait_recv()

    each(1, 16, wait_steps)
    row = iota((HEADS, TOK), 0)
    speeds = jnp.zeros((HEADS, TOK), F32)
    for h in range(HEADS):
        speeds = jnp.where(row == h, speed[h], speeds)
    raw = steps[...].reshape(HEADS, TOK)
    step = jnp.maximum(raw, 0.0) + jnp.log1p(jnp.exp(-jnp.abs(raw)))
    fading = fades[...].reshape(HEADS, TOK) - speeds * step
    later = iota((TOK, TOK), 0)
    sooner = iota((TOK, TOK), 1)
    causal = later >= sooner
    triangle = causal.astype(F32).astype(BF16)
    triangle = jnp.concatenate([triangle] * 3, axis=1)
    same = (later == sooner).astype(F32).astype(BF16)
    fading_parts = thirds(fading)
    cum_row = dot_nt(fading_parts, triangle)
    cum_col = dot_nt(triangle, fading_parts)
    step_col = dot_nt(jnp.concatenate([same] * 3, axis=1), thirds(step))
    spread = (
        (lax.div(iota((3 * HEADS, INNER), 1), HEAD_DIM) == lax.rem(iota((3 * HEADS, INNER), 0), HEADS))
        .astype(F32)
        .astype(BF16)
    )
    last = cum_col[TOK - 1 : TOK]
    tail_wide = dot(thirds(jnp.exp(last - cum_col) * step_col), spread)
    decay_wide = dot(thirds(jnp.broadcast_to(jnp.exp(last), (8, HEADS))), spread)
    for k in range(4):
        decay[k] = decay_wide[0:1, 256 * k : 256 * k + 256]
    scaled = (conv[:, 0:INNER].astype(F32) * tail_wide).astype(BF16)
    for q in range(2):
        b_pair = conv[:, INNER + 128 * q : INNER + 128 * q + 128]
        both = dot(b_pair.T, scaled[:, 512 * q : 512 * q + 512])
        state[:, 512 * q : 512 * q + 256] = both[0:64, 0:256].astype(BF16)
        state[:, 512 * q + 256 : 512 * q + 512] = both[64:128, 256:512].astype(BF16)

    def place_of(k):
        return (
            pl.ds(pl.multiple_of(lax.div(k, 4) * 16, 16), 16),
            pl.ds(pl.multiple_of(lax.rem(k, 4) * 256, 256), 256),
        )

    def state_copy(o):
        rows, cols = place_of(ahead(o))
        return pltpu.make_async_remote_copy(
            src_ref=state.at[rows, cols],
            dst_ref=state_in.at[sp],
            send_sem=state_send.at[0, o],
            recv_sem=state_recv.at[0, o],
            device_id=(ahead(o), dp),
            device_id_type=MESH,
        )

    def decay_copy(o):
        return pltpu.make_async_remote_copy(
            src_ref=decay.at[lax.rem(ahead(o), 4)],
            dst_ref=decay_in.at[sp],
            send_sem=state_send.at[1, o],
            recv_sem=state_recv.at[1, o],
            device_id=(ahead(o), dp),
            device_id_type=MESH,
        )

    def send_state(o):
        decay_copy(o).start()
        state_copy(o).start()

    each(1, 16, send_state)
    my_rows, my_cols = place_of(sp)
    state_in[sp] = state[my_rows, my_cols]
    decay_in[sp] = decay[lax.rem(sp, 4)]

    low_half = iota((TOK, TOK), 1) < 64
    for q in range(2):
        b_pair = conv[:, INNER + 128 * q : INNER + 128 * q + 128]
        c_pair = conv[:, INNER + 256 + 128 * q : INNER + 256 + 128 * q + 128]
        for g in range(2):
            c_one = jnp.where(low_half == (g == 0), c_pair, jnp.zeros_like(c_pair))
            scores = dot_nt(c_one, b_pair)
            for i in range(2):
                first = 8 * q + 4 * g + 2 * i
                x_pair = conv[:, 64 * first : 64 * first + 128]
                total = None
                for h in (first, first + 1):
                    gap = jnp.where(
                        causal, cum_col[:, h : h + 1] - cum_row[h : h + 1, :], -1e30
                    )
                    mixing = (scores * jnp.exp(gap) * step[h : h + 1, :]).astype(BF16)
                    x_one = jnp.where(low_half == (h == first), x_pair, jnp.zeros_like(x_pair))
                    term = dot(mixing, x_one)
                    total = term if total is None else total + term
                inside[:, 64 * first : 64 * first + 128] = total

    def placing_rows(j):
        ids, shares = names[j], parts[j]
        expert = iota((16, TOK), 0)
        first, second = expert == ids[0:1, :], expert == ids[1:2, :]
        named = first | second
        share = jnp.where(first, shares[0:1, :], 0.0) + jnp.where(second, shares[1:2, :], 0.0)
        before = (later < sooner).astype(BF16)
        rank = dot(named.astype(F32).astype(BF16), before)
        rank = jnp.where(named, rank, -1.0)
        slot = iota((SLOTS, TOK), 0).astype(F32)
        chosen = jnp.concatenate(
            [(rank[e : e + 1, :] == slot).astype(F32) for e in range(16)], axis=0
        )
        weights = jnp.concatenate(
            [
                jnp.where(rank[e : e + 1, :] == slot, share[e : e + 1, :], 0.0)
                for e in range(16)
            ],
            axis=0,
        )
        placing[j] = chosen.astype(BF16)
        rest = weights.T
        for k in range(2):
            piece = rest.astype(BF16)
            weighing[j, pl.ds(TOK * k, TOK), :] = piece
            rest = rest - piece.astype(F32)

    placing_rows(0)
    for copy in notes:
        copy.wait_recv()
    for j in range(1, 4):
        placing_rows(j)

    def wait_state(o):
        decay_copy(o).wait_recv()
        state_copy(o).wait_recv()

    each(1, 16, wait_state)

    def advance(j, held):
        entering[j] = held.astype(BF16)
        return decay_in[j] * held + state_in[j].astype(F32)

    lax.fori_loop(0, 16, advance, jnp.zeros((16, 256), F32))

    def enter_copy(o):
        rows, cols = place_of(sp)
        return pltpu.make_async_remote_copy(
            src_ref=entering.at[ahead(o)],
            dst_ref=entered.at[rows, cols],
            send_sem=enter_send.at[o],
            recv_sem=enter_recv.at[o],
            device_id=(ahead(o), dp),
            device_id_type=MESH,
        )

    each(1, 16, lambda o: enter_copy(o).start())
    entered[my_rows, my_cols] = entering[sp]
    reach_wide = dot(thirds(jnp.exp(cum_col)), spread)
    each(1, 16, lambda o: enter_copy(o).wait_recv())

    for copy in late_loads:
        copy.wait()
    nothing = jnp.zeros((64, 256), BF16)
    blocks = []
    for q in range(2):
        c_pair = conv[:, INNER + 256 + 128 * q : INNER + 256 + 128 * q + 128]
        low, high = entered[:, 512 * q : 512 * q + 256], entered[:, 512 * q + 256 : 512 * q + 512]
        both = jnp.concatenate(
            [
                jnp.concatenate([low, nothing], axis=1),
                jnp.concatenate([nothing, high], axis=1),
            ],
            axis=0,
        )
        carried = dot(c_pair, both)
        for g in range(2):
            low_col = 512 * q + 256 * g
            mixed = (
                inside[:, low_col : low_col + 256]
                + reach_wide[:, low_col : low_col + 256] * carried[:, 256 * g : 256 * g + 256]
            ).astype(BF16)
            gated = mixed.astype(F32) * jax.nn.silu(valve[:, low_col : low_col + 256].astype(F32))
            level = lax.rsqrt(jnp.mean(gated * gated, axis=1, keepdims=True) + rms_eps)
            blocks.append(
                (gated * level * group_gain[:, low_col : low_col + 256]).astype(BF16)
            )
    group_normed = jnp.concatenate(blocks, axis=1)
    out_load.wait()

    def project(k):
        cols = pl.ds(512 * k, 512)
        pre[:, cols] = skip[:, cols].astype(F32) + dot(group_normed, out_v[:, cols])

    for k in range(width // 512):
        project(k)

    def standardize(k):
        rows = pl.ds(64 * k, 64)
        block = pre[rows, :]
        shifted = block - jnp.mean(block, axis=1, keepdims=True)
        level = lax.rsqrt(jnp.mean(shifted * shifted, axis=1, keepdims=True) + norm_eps)
        normed[rows, :] = (shifted * level * gain[...] + offset[...]).astype(BF16)

    far_cols = pl.ds(NEAR, width - NEAR)

    def token_copy(lane, half):
        rows = pl.ds(64 * half, 64)
        if lane < 2:
            source = normed.at[rows, far_cols]
        else:
            source = tokens.at[half, rows]
        return pltpu.make_async_remote_copy(
            src_ref=source,
            dst_ref=tokens.at[lane, rows],
            send_sem=token_send.at[lane, half],
            recv_sem=token_recv.at[lane, half],
            device_id=(right, left, (right, left)[half])[lane],
            device_id_type=MESH,
        )

    standardize(0)
    token_copy(0, 0).start()
    token_copy(1, 0).start()
    standardize(1)
    token_copy(1, 1).start()
    token_copy(0, 1).start()
    flat_outgoing = outgoing.reshape(16 * SLOTS, width)

    def route(k):
        cols = pl.ds(512 * k, 512)
        flat_outgoing[:, cols] = dot(placing[0], normed[:, cols]).astype(BF16)

    for k in range(width // 512):
        route(k)

    near_cols = pl.ds(0, NEAR)
    near_back = pl.ds(0, NEAR_BACK)
    far_back = pl.ds(NEAR_BACK, width - NEAR_BACK)

    def go(o, side=0):
        cols = (near_cols, far_cols)[side]
        return pltpu.make_async_remote_copy(
            src_ref=outgoing.at[pl.ds(3 * ahead(o), 3), :, cols],
            dst_ref=gathered.at[0, pl.ds(3 * o, 3), :, cols],
            send_sem=go_send.at[side, o],
            recv_sem=go_recv.at[side, o],
            device_id=(ahead(o), dp),
            device_id_type=MESH,
        )

    each(1, 16, lambda o: go(o).start())
    each(1, 16, lambda o: go(o, 1).start())
    gathered[0, 0:3] = outgoing[pl.ds(3 * sp, 3)]

    def group(g):
        return pl.ds(12 * g, 12)

    def ring(src_slot, dst_slot, g, target, lane):
        return pltpu.make_async_remote_copy(
            src_ref=gathered.at[src_slot, group(g), :, near_cols],
            dst_ref=gathered.at[dst_slot, group(g), :, near_cols],
            send_sem=ring_send.at[lane, g],
            recv_sem=ring_recv.at[dst_slot - 1, g],
            device_id=target,
            device_id_type=MESH,
        )

    def to_right(g):
        return ring(0, 1, g, right, 0)

    def to_left(g):
        return ring(0, 2, g, left, 1)

    def onward(g):
        return ring(1, 3, g, right, 2) if g < 2 else ring(2, 3, g, left, 2)

    def far_copy(j, o):
        return pltpu.make_async_remote_copy(
            src_ref=far_rows.at[j - 1, pl.ds(3 * ahead(o), 3)],
            dst_ref=gathered.at[j, pl.ds(3 * o, 3), :, far_cols],
            send_sem=far_send.at[j - 1, o],
            recv_sem=far_recv.at[j - 1, o],
            device_id=(ahead(o), dp),
            device_id_type=MESH,
        )

    def route_far(j):
        flat = far_rows.at[j - 1].reshape(16 * SLOTS, width - NEAR)
        flat[...] = dot(placing[j], tokens[j - 1]).astype(BF16)
        gathered[j, 0:3, :, NEAR:] = far_rows[j - 1, pl.ds(3 * sp, 3)]

    def send_far(j, half):
        each(max(8 * half, 1), 8 * half + 8, lambda o: far_copy(j, o).start())

    def wait_far(j, half):
        each(max(8 * half, 1), 8 * half + 8, lambda o: far_copy(j, o).wait_recv())

    def pass_on(g):
        each(max(4 * g, 1), 4 * g + 4, lambda o: go(o).wait_recv())
        to_right(g).start()
        to_left(g).start()

    token_copy(0, 0).wait_recv()
    token_copy(2, 0).start()
    token_copy(1, 1).wait_recv()
    token_copy(2, 1).start()
    token_copy(0, 1).wait_recv()
    route_far(1)
    send_far(1, 0)
    token_copy(1, 0).wait_recv()
    route_far(2)
    send_far(2, 0)
    send_far(2, 1)
    send_far(1, 1)
    pass_on(0)
    token_copy(2, 0).wait_recv()
    token_copy(2, 1).wait_recv()
    route_far(3)
    send_far(3, 0)
    send_far(3, 1)
    pass_on(1)
    pass_on(2)
    pass_on(3)
    for copy in loads:
        copy.wait()
    for copy in gifts:
        copy.wait()
    each(1, 8, lambda o: go(o, 1).wait_recv())

    tile = 256

    def home_copy(j, o):
        return pltpu.make_async_remote_copy(
            src_ref=partial.at[j, pl.ds(3 * o, 3), :, far_back],
            dst_ref=far_answers.at[j, pl.ds(3 * sp, 3)],
            send_sem=home_send.at[j, o],
            recv_sem=home_recv.at[j, o],
            device_id=(behind(o), dp),
            device_id_type=MESH,
        )

    def unit(slot, half):
        block = gathered.at[slot, pl.ds(24 * half, 24)].reshape(192, width)
        for k in range(2 * part // tile):
            cols = pl.ds(k * tile, tile)
            gate_val = dot(block[...], gate_v[:, cols])
            up_val = dot(block[...], raise_v[:, cols])
            hidden[:, cols] = (jax.nn.silu(gate_val) * up_val).astype(BF16)
        target = partial.at[slot, pl.ds(24 * half, 24)].reshape(192, width)
        for k in range(width // tile):
            cols = pl.ds(k * tile, tile)
            target[:, cols] = dot(hidden[...], lower_v[:, cols]).astype(BF16)
        each(jnp.maximum(8 * half, 1), 8 * half + 8, lambda o: home_copy(slot, o).start())

        @pl.when(half == 0)
        def _():
            far_answers[slot, pl.ds(3 * sp, 3)] = partial[slot, 0:3, :, NEAR_BACK:]

    def sum_direct(slot, g):
        side = 0 if slot == 2 else 1
        return pltpu.make_async_remote_copy(
            src_ref=partial.at[slot, group(g), :, near_back],
            dst_ref=summed.at[side, group(g)],
            send_sem=sum_send.at[side, g],
            recv_sem=sum_recv.at[side, g],
            device_id=right if slot == 2 else left,
            device_id_type=MESH,
        )

    def sum_relay(g):
        return pltpu.make_async_remote_copy(
            src_ref=partial.at[3, group(g), :, near_back],
            dst_ref=relayed.at[group(g)],
            send_sem=sum_send.at[2, g],
            recv_sem=sum_recv.at[2, g],
            device_id=right if g < 2 else left,
            device_id_type=MESH,
        )

    def combine(j):
        each(1, 16, lambda o: home_copy(j, o).wait_recv())
        flat = far_answers.at[j].reshape(16 * SLOTS, width - NEAR_BACK)
        terms = dot(weighing[j], flat[...])
        return terms[0:TOK] + terms[TOK : 2 * TOK]

    def tsum_copy(lane, half):
        rows = pl.ds(64 * half, 64)
        if lane == 2:
            source, target = token_out.at[2, rows], token_relay.at[rows]
            device = (right, left)[half]
        else:
            source, target = token_out.at[lane, rows], token_in.at[lane, rows]
            device = (right, left)[lane]
        return pltpu.make_async_remote_copy(
            src_ref=source,
            dst_ref=target,
            send_sem=tsum_send.at[lane, half],
            recv_sem=tsum_recv.at[lane, half],
            device_id=device,
            device_id_type=MESH,
        )

    def relay_add(g):
        slot = 2 if g < 2 else 1
        sum_relay(g).wait_recv()
        partial[slot, group(g), :, 0:NEAR_BACK] = (
            partial[slot, group(g), :, 0:NEAR_BACK].astype(F32) + relayed[group(g)].astype(F32)
        ).astype(BF16)
        sum_direct(slot, g).start()

    def before_own():
        each(8, 16, lambda o: go(o, 1).wait_recv())
        to_right(0).wait_recv()
        onward(0).start()

    def before_left():
        to_right(1).wait_recv()
        onward(1).start()
        wait_far(1, 0)

    def before_right():
        to_left(0).wait_recv()
        to_left(1).wait_recv()
        to_left(2).wait_recv()
        onward(2).start()
        wait_far(2, 0)

    def before_right_rest():
        to_left(3).wait_recv()
        onward(3).start()
        sum_direct(1, 0).start()
        sum_direct(1, 1).start()
        wait_far(2, 1)

    def before_left_rest():
        sum_direct(2, 2).start()
        sum_direct(2, 3).start()
        to_right(2).wait_recv()
        to_right(3).wait_recv()
        wait_far(1, 1)

    def before_across():
        onward(0).wait_recv()
        onward(1).wait_recv()
        wait_far(3, 0)

    def before_across_rest():
        sum_relay(0).start()
        sum_relay(1).start()
        onward(2).wait_recv()
        onward(3).wait_recv()
        wait_far(3, 1)

    befores = (
        before_own, before_left, before_right, before_right_rest, before_left_rest,
        before_across, before_across_rest,
    )

    def turn(u):
        for k, before in enumerate(befores):
            pl.when(u == k + 1)(before)
        slot = jnp.where(u < 2, 0, jnp.where(u >= 6, 3, jnp.where((u == 2) | (u == 5), 1, 2)))
        half = jnp.where((u == 1) | (u == 4) | (u == 5) | (u == 7), 1, 0)
        unit(slot, half)

    each(0, 8, turn)
    sum_relay(2).start()
    sum_relay(3).start()
    relay_add(0)
    relay_add(2)
    relay_add(1)
    relay_add(3)
    token_out[0] = combine(2).astype(BF16)
    tsum_copy(0, 1).start()
    token_out[1] = combine(1).astype(BF16)
    tsum_copy(1, 0).start()

    def back(o):
        return pltpu.make_async_remote_copy(
            src_ref=partial.at[0, pl.ds(3 * o, 3), :, near_back],
            dst_ref=answers.at[pl.ds(3 * sp, 3)],
            send_sem=back_send.at[o],
            recv_sem=back_recv.at[o],
            device_id=(behind(o), dp),
            device_id_type=MESH,
        )

    def settle(g):
        sum_direct(2, g).wait_recv()
        sum_direct(1, g).wait_recv()
        partial[0, group(g), :, 0:NEAR_BACK] = (
            partial[0, group(g), :, 0:NEAR_BACK].astype(F32)
            + summed[0, group(g)].astype(F32)
            + summed[1, group(g)].astype(F32)
        ).astype(BF16)
        each(max(4 * g, 1), 4 * g + 4, lambda o: back(o).start())
        if g == 0:
            answers[pl.ds(3 * sp, 3)] = partial[0, 0:3, :, 0:NEAR_BACK]

    settle(0)
    settle(2)
    token_out[2] = combine(3).astype(BF16)
    tsum_copy(2, 0).start()
    tsum_copy(2, 1).start()
    settle(1)
    settle(3)
    for half in range(2):
        lane, rows = half, pl.ds(64 * half, 64)
        tsum_copy(2, half).wait_recv()
        token_out[lane, rows] = (
            token_out[lane, rows].astype(F32) + token_relay[rows].astype(F32)
        ).astype(BF16)
        tsum_copy(lane, half).start()

    token_sum[...] = combine(0)
    for copy in rims + notes:
        copy.wait_send()
    for lane in range(3):
        for half in range(2):
            token_copy(lane, half).wait_send()
            tsum_copy(lane, half).wait_send()
            if lane < 2:
                tsum_copy(lane, half).wait_recv()
    result[:, NEAR_BACK:] = (
        normed[:, NEAR_BACK:].astype(F32)
        + token_sum[...]
        + token_in[0].astype(F32)
        + token_in[1].astype(F32)
    ).astype(BF16)
    for g in range(4):
        to_right(g).wait_send()
        to_left(g).wait_send()
        onward(g).wait_send()
        sum_direct(1, g).wait_send()
        sum_direct(2, g).wait_send()
        sum_relay(g).wait_send()

    def drain(o):
        step_copy(o, steps_out, steps, 0).wait_send()
        step_copy(o, fades_out, fades, 1).wait_send()
        decay_copy(o).wait_send()
        state_copy(o).wait_send()
        enter_copy(o).wait_send()
        go(o).wait_send()
        go(o, 1).wait_send()
        for j in range(4):
            if j > 0:
                far_copy(j, o).wait_send()
            home_copy(j, o).wait_send()
        back(o).wait_send()
        back(o).wait_recv()

    each(1, 16, drain)
    flat_answers = answers.reshape(16 * SLOTS, NEAR_BACK)

    def finish(k, size):
        cols = pl.ds(k, size)
        terms = dot(weighing[0], flat_answers[:, cols])
        routed = terms[0:TOK] + terms[TOK : 2 * TOK]
        result[:, cols] = (normed[:, cols].astype(F32) + routed).astype(BF16)

    for k in range(0, NEAR_BACK, 512):
        finish(k, min(512, NEAR_BACK - k))


def per_device(
    skip_connection_stream,
    emitted_valve_unscaled,
    channel_source_mapped,
    hidden_source_mapped,
    probe_mapped_values,
    increment_premapped,
    extra_log_fading,
    channel_fading_speed,
    channel_source_kernel,
    hidden_source_kernel,
    probe_kernel_coefficients,
    cluster_scaling_factor,
    emitted_mapping_matrix,
    standardize_scaling,
    standardize_offset,
    chosen_specialist_ids,
    specialist_mixing_shares,
    specialist_gating_matrices,
    raising_matrices,
    lowering_matrices,
):
    width = skip_connection_stream.shape[2]
    part = specialist_gating_matrices.shape[2]
    far = pl.BlockSpec(memory_space=pl.ANY)
    near = pl.BlockSpec(memory_space=pltpu.VMEM)
    dma = pltpu.SemaphoreType.DMA
    rows = 2 * SLOTS
    rest = width - NEAR_BACK
    out = pl.pallas_call(
        layer_kernel,
        out_shape=pltpu.VMEM((TOK, width), BF16),
        in_specs=[far] * 20,
        out_specs=near,
        scratch_shapes=[
            pltpu.SMEM((HEADS,), F32),
            pltpu.VMEM((4, INNER), F32),
            pltpu.VMEM((4, 256), F32),
            pltpu.VMEM((4, 256), F32),
            pltpu.VMEM((1, INNER), F32),
            pltpu.VMEM((1, width), F32),
            pltpu.VMEM((1, width), F32),
            pltpu.VMEM((TOK, width), BF16),
            pltpu.VMEM((TOK, INNER), BF16),
            pltpu.VMEM((16, 8, 1536), BF16),
            pltpu.VMEM((1, 8, 1536), BF16),
            pltpu.VMEM((HEADS, 1, TOK), F32),
            pltpu.VMEM((HEADS, 1, TOK), F32),
            pltpu.VMEM((HEADS, 1, TOK), F32),
            pltpu.VMEM((HEADS, 1, TOK), F32),
            pltpu.VMEM((4, 2, TOK), jnp.int32),
            pltpu.VMEM((4, 2, TOK), F32),
            pltpu.VMEM((TOK, 1536), BF16),
            pltpu.VMEM((64, INNER), BF16),
            pltpu.VMEM((4, 1, 256), F32),
            pltpu.VMEM((16, 16, 256), BF16),
            pltpu.VMEM((16, 1, 256), F32),
            pltpu.VMEM((16, 16, 256), BF16),
            pltpu.VMEM((64, INNER), BF16),
            pltpu.VMEM((TOK, INNER), F32),
            pltpu.VMEM((INNER, width), BF16),
            pltpu.VMEM((TOK, width), F32),
            pltpu.VMEM((TOK, width), BF16),
            pltpu.VMEM((4, 16 * SLOTS, TOK), BF16),
            pltpu.VMEM((4, 2 * TOK, 16 * SLOTS), BF16),
            pltpu.VMEM((rows, 8, width), BF16),
            pltpu.VMEM((rows, 8, NEAR_BACK), BF16),
            pltpu.VMEM((3, TOK, width - NEAR), BF16),
            pltpu.VMEM((3, rows, 8, width - NEAR), BF16),
            pltpu.VMEM((4, rows, 8, rest), BF16),
            pltpu.VMEM((TOK, rest), F32),
            pltpu.VMEM((3, TOK, rest), BF16),
            pltpu.VMEM((TOK, rest), BF16),
            pltpu.VMEM((2, TOK, rest), BF16),
            pltpu.VMEM((4, rows, 8, width), BF16),
            pltpu.VMEM((4, rows, 8, width), BF16),
            pltpu.VMEM((rows, 8, NEAR_BACK), BF16),
            pltpu.VMEM((2, rows, 8, NEAR_BACK), BF16),
            pltpu.VMEM((width, 2 * part), BF16),
            pltpu.VMEM((width, 2 * part), BF16),
            pltpu.VMEM((2 * part, width), BF16),
            pltpu.VMEM((192, 2 * part), BF16),
            dma((17,)), dma((3,)), dma((3,)), dma((2, 3)), dma((2, 3)), dma((2, 16)), dma((2, 16)), dma((2, 16)), dma((2, 16)),
            dma((16,)), dma((16,)), dma((3,)), dma((3,)), dma((3,)), dma((2, 16)), dma((2, 16)),
            dma((3, 4)), dma((3, 4)), dma((3, 4)), dma((3, 4)), dma((16,)), dma((16,)),
            dma((3, 2)), dma((3, 2)), dma((3, 16)), dma((3, 16)), dma((4, 16)), dma((4, 16)),
            dma((3, 2)), dma((3, 2)),
        ],
        compiler_params=pltpu.CompilerParams(
            collective_id=0, has_side_effects=True, vmem_limit_bytes=62 * 1024 * 1024
        ),
        name="layer",
    )(
        channel_fading_speed,
        skip_connection_stream[0],
        emitted_valve_unscaled[0],
        channel_source_mapped.reshape(16, 8, INNER),
        hidden_source_mapped.reshape(16, 8, 256),
        probe_mapped_values.reshape(16, 8, 256),
        increment_premapped.reshape(16, 1, TOK),
        extra_log_fading.reshape(16, 1, TOK),
        channel_source_kernel,
        hidden_source_kernel,
        probe_kernel_coefficients,
        cluster_scaling_factor[None, :],
        emitted_mapping_matrix,
        standardize_scaling[None, :],
        standardize_offset[None, :],
        chosen_specialist_ids[0].T,
        specialist_mixing_shares[0].T,
        specialist_gating_matrices[0],
        raising_matrices[0],
        lowering_matrices[0],
    )
    return out[None]


def solution(mesh):
    placed = (
        P("dp", "sp", None),
        P("dp", "sp", None),
        P("dp", "sp", None),
        P("dp", "sp", None),
        P("dp", "sp", None),
        P("dp", None, "sp"),
        P("dp", None, "sp"),
        P(),
        P(),
        P(),
        P(),
        P(),
        P(),
        P(),
        P(),
        P("dp", "sp", None),
        P("dp", "sp", None),
        P("sp", None, "dp"),
        P("sp", None, "dp"),
        P("sp", "dp", None),
    )
    return jax.shard_map(
        per_device, mesh=mesh, in_specs=placed, out_specs=P("dp", "sp", None), check_vma=False
    )
```

```python
import jax
import jax.numpy as jnp
from jax import lax
from jax.experimental import pallas as pl
from jax.experimental.pallas import tpu as pltpu
from jax.sharding import PartitionSpec as P

MESH = pl.DeviceIdType.MESH
HEADS = 16
HEAD_DIM = 64
TOK = 128
INNER = 1024
SLOTS = 24
NEAR = 1280
NEAR_BACK = 1280
rms_eps = 1e-06
norm_eps = 1e-05
BF16 = jnp.bfloat16
F32 = jnp.float32


def dot(a, b):
    return jnp.dot(a, b, preferred_element_type=F32)


def thirds(a):
    parts = []
    for _ in range(3):
        part = a.astype(BF16)
        parts.append(part)
        a = a - part.astype(F32)
    return jnp.concatenate(parts, axis=1)


def dot_nt(a, b):
    return lax.dot_general(a, b, (((1,), (1,)), ((), ())), preferred_element_type=F32)


def iota(shape, dim):
    return lax.broadcasted_iota(jnp.int32, shape, dim)


def layer_kernel(
    speed_in, skip_in, valve_in, chan, hid, probe, step_in, fade_in, tap_x_in, tap_b_in, tap_c_in,
    group_gain_in, out_w, gain_in, offset_in, ids, shares, gate_w, raise_w, lower_w,
    result,
    speed, tap_x, tap_b, tap_c, group_gain, gain, offset, skip, valve, joined, rim, steps_out, fades_out, steps, fades, names, parts, conv, state, decay, state_in, decay_in, entering,
    entered, inside, out_v, pre, normed, placing, weighing, outgoing, answers,
    tokens, far_rows, far_answers, token_sum, token_out, token_relay, token_in,
    gathered, partial, relayed, summed, gate_v, raise_v, lower_v, hidden,
    load_sem, rim_send, rim_recv, name_send, name_recv, step_send, step_recv,
    state_send, state_recv, enter_send, enter_recv,
    weight_sem, weight_send, weight_recv, go_send, go_recv, ring_send, ring_recv,
    sum_send, sum_recv, back_send, back_recv, token_send, token_recv, far_send, far_recv,
    home_send, home_recv, tsum_send, tsum_recv,
):
    sp = lax.axis_index("sp")
    dp = lax.axis_index("dp")
    z, y = lax.div(sp, 4), lax.rem(sp, 4)
    x, core = lax.div(dp, 2), lax.rem(dp, 2)
    right = (sp, lax.rem(x + 1, 4) * 2 + core)
    left = (sp, lax.rem(x + 3, 4) * 2 + core)
    across = (sp, lax.rem(x + 2, 4) * 2 + core)
    twin = (sp, x * 2 + 1 - core)
    width = skip_in.shape[1]
    part = gate_w.shape[1]

    def ahead(o):
        i = lax.rem(o, 4)
        return lax.rem(z + i, 4) * 4 + lax.rem(y + i + lax.div(o, 4), 4)

    def behind(o):
        i = lax.rem(o, 4)
        return lax.rem(z + 4 - i, 4) * 4 + lax.rem(y + 8 - i - lax.div(o, 4), 4)

    def each(low, high, work):
        def step(o, carry):
            work(o)
            return carry

        lax.fori_loop(low, high, step, 0)

    barrier = pltpu.get_barrier_semaphore()
    each(
        1, 16,
        lambda o: pl.semaphore_signal(
            barrier, inc=1, device_id=(ahead(o), dp), device_id_type=MESH
        ),
    )
    for friend in (left, right, across, twin):
        pl.semaphore_signal(barrier, inc=1, device_id=friend, device_id_type=MESH)

    spans = ((chan, 0, INNER), (hid, INNER, 256), (probe, INNER + 256, 256))
    own_loads = [
        pltpu.make_async_copy(
            ref, joined.at[:, :, pl.ds(low, size)], load_sem.at[k]
        )
        for k, (ref, low, size) in enumerate(spans)
    ]
    own_loads.append(pltpu.make_async_copy(step_in, steps_out, load_sem.at[3]))
    own_loads.append(pltpu.make_async_copy(fade_in, fades_out, load_sem.at[4]))
    own_loads.append(pltpu.make_async_copy(ids, names.at[0], load_sem.at[6]))
    own_loads.append(pltpu.make_async_copy(shares, parts.at[0], load_sem.at[7]))
    out_load = pltpu.make_async_copy(out_w, out_v, load_sem.at[5])
    for k, (source, target) in enumerate(
        ((tap_x_in, tap_x), (tap_b_in, tap_b), (tap_c_in, tap_c), (speed_in, speed))
    ):
        own_loads.append(pltpu.make_async_copy(source, target, load_sem.at[10 + k]))
    late_loads = [
        pltpu.make_async_copy(group_gain_in, group_gain, load_sem.at[14]),
        pltpu.make_async_copy(gain_in, gain, load_sem.at[15]),
        pltpu.make_async_copy(offset_in, offset, load_sem.at[16]),
        pltpu.make_async_copy(skip_in, skip, load_sem.at[8]),
        pltpu.make_async_copy(valve_in, valve, load_sem.at[9]),
    ]
    for copy in own_loads:
        copy.start()
    loads, gifts = [], []
    for k, (source, target) in enumerate(
        ((gate_w, gate_v), (raise_w, raise_v), (lower_w, lower_v))
    ):
        if k < 2:
            mine, theirs = target.at[:, pl.ds(0, part)], target.at[:, pl.ds(part, part)]
        else:
            mine, theirs = target.at[pl.ds(0, part)], target.at[pl.ds(part, part)]
        loads.append(pltpu.make_async_copy(source, mine, weight_sem.at[k]))
        gifts.append(
            pltpu.make_async_remote_copy(
                src_ref=source,
                dst_ref=theirs,
                send_sem=weight_send.at[k],
                recv_sem=weight_recv.at[k],
                device_id=twin,
                device_id_type=MESH,
            )
        )

    for copy in own_loads:
        copy.wait()
    for copy in late_loads:
        copy.start()
    out_load.start()
    for copy in loads:
        copy.start()

    def filtered(block, taps):
        high = block.shape[0] - 8
        running = taps[0:1] * block[5 : 5 + high]
        for k in range(1, 4):
            running = running + taps[k : k + 1] * block[5 + k : 5 + k + high]
        return jax.nn.silu(running).astype(BF16)

    def convolve(cols, taps):
        block = joined[:, :, cols].reshape(TOK, 256).astype(F32)
        block = jnp.concatenate([jnp.zeros((8, 256), F32), block], axis=0)
        conv[:, cols] = filtered(block, taps)

    def convolve_rim(cols, taps):
        before = rim[:, :, cols].reshape(8, 256).astype(F32) * (sp > 0).astype(F32)
        block = joined[0:2, :, cols].reshape(16, 256).astype(F32)
        conv[0:16, cols] = filtered(jnp.concatenate([before, block], axis=0), taps)

    def begin(work):
        def work_x(k):
            cols = pl.ds(pl.multiple_of(k * 256, 256), 256)
            work(cols, tap_x[:, cols])

        each(0, 4, work_x)
        work(pl.ds(INNER, 256), tap_b[...])
        work(pl.ds(INNER + 256, 256), tap_c[...])

    begin(convolve)
    pl.semaphore_wait(barrier, 19)

    def step_copy(o, source, target, which):
        return pltpu.make_async_remote_copy(
            src_ref=source.at[ahead(o)],
            dst_ref=target.at[sp],
            send_sem=step_send.at[which, o],
            recv_sem=step_recv.at[which, o],
            device_id=(ahead(o), dp),
            device_id_type=MESH,
        )

    def send_steps(o):
        step_copy(o, steps_out, steps, 0).start()
        step_copy(o, fades_out, fades, 1).start()

    each(1, 16, send_steps)
    steps[sp] = steps_out[sp]
    fades[sp] = fades_out[sp]
    rims = [
        pltpu.make_async_remote_copy(
            src_ref=joined.at[pl.ds(15, 1), :, pl.ds(low, size)],
            dst_ref=rim.at[:, :, pl.ds(low, size)],
            send_sem=rim_send.at[k],
            recv_sem=rim_recv.at[k],
            device_id=(lax.rem(sp + 1, 16), dp),
            device_id_type=MESH,
        )
        for k, (_, low, size) in enumerate(spans)
    ]
    for copy in rims:
        copy.start()
    notes = [
        pltpu.make_async_remote_copy(
            src_ref=target.at[0],
            dst_ref=target.at[k + 1],
            send_sem=name_send.at[which, k],
            recv_sem=name_recv.at[which, k],
            device_id=friend,
            device_id_type=MESH,
        )
        for which, target in enumerate((names, parts))
        for k, friend in enumerate((right, left, across))
    ]
    for copy in notes + gifts:
        copy.start()
    for copy in rims:
        copy.wait_recv()
    begin(convolve_rim)

    def wait_steps(o):
        step_copy(o, steps_out, steps, 0).wait_recv()
        step_copy(o, fades_out, fades, 1).wait_recv()

    each(1, 16, wait_steps)
    row = iota((HEADS, TOK), 0)
    speeds = jnp.zeros((HEADS, TOK), F32)
    for h in range(HEADS):
        speeds = jnp.where(row == h, speed[h], speeds)
    raw = steps[...].reshape(HEADS, TOK)
    step = jnp.maximum(raw, 0.0) + jnp.log1p(jnp.exp(-jnp.abs(raw)))
    fading = fades[...].reshape(HEADS, TOK) - speeds * step
    later = iota((TOK, TOK), 0)
    sooner = iota((TOK, TOK), 1)
    causal = later >= sooner
    triangle = causal.astype(F32).astype(BF16)
    triangle = jnp.concatenate([triangle] * 3, axis=1)
    same = (later == sooner).astype(F32).astype(BF16)
    fading_parts = thirds(fading)
    cum_row = dot_nt(fading_parts, triangle)
    cum_col = dot_nt(triangle, fading_parts)
    step_col = dot_nt(jnp.concatenate([same] * 3, axis=1), thirds(step))
    spread = (
        (lax.div(iota((3 * HEADS, INNER), 1), HEAD_DIM) == lax.rem(iota((3 * HEADS, INNER), 0), HEADS))
        .astype(F32)
        .astype(BF16)
    )
    last = cum_col[TOK - 1 : TOK]
    tail_wide = dot(thirds(jnp.exp(last - cum_col) * step_col), spread)
    decay_wide = dot(thirds(jnp.broadcast_to(jnp.exp(last), (8, HEADS))), spread)
    for k in range(4):
        decay[k] = decay_wide[0:1, 256 * k : 256 * k + 256]
    def decay_copy(o):
        return pltpu.make_async_remote_copy(
            src_ref=decay.at[lax.rem(ahead(o), 4)],
            dst_ref=decay_in.at[sp],
            send_sem=state_send.at[1, o],
            recv_sem=state_recv.at[1, o],
            device_id=(ahead(o), dp),
            device_id_type=MESH,
        )

    each(1, 16, lambda o: decay_copy(o).start())
    decay_in[sp] = decay[lax.rem(sp, 4)]
    scaled = (conv[:, 0:INNER].astype(F32) * tail_wide).astype(BF16)
    for q in range(2):
        b_pair = conv[:, INNER + 128 * q : INNER + 128 * q + 128]
        both = dot(b_pair.T, scaled[:, 512 * q : 512 * q + 512])
        state[:, 512 * q : 512 * q + 256] = both[0:64, 0:256].astype(BF16)
        state[:, 512 * q + 256 : 512 * q + 512] = both[64:128, 256:512].astype(BF16)

    def place_of(k):
        return (
            pl.ds(pl.multiple_of(lax.div(k, 4) * 16, 16), 16),
            pl.ds(pl.multiple_of(lax.rem(k, 4) * 256, 256), 256),
        )

    def state_copy(o):
        rows, cols = place_of(ahead(o))
        return pltpu.make_async_remote_copy(
            src_ref=state.at[rows, cols],
            dst_ref=state_in.at[sp],
            send_sem=state_send.at[0, o],
            recv_sem=state_recv.at[0, o],
            device_id=(ahead(o), dp),
            device_id_type=MESH,
        )

    def send_state(o):
        state_copy(o).start()

    each(1, 16, send_state)
    my_rows, my_cols = place_of(sp)
    state_in[sp] = state[my_rows, my_cols]

    low_half = iota((TOK, TOK), 1) < 64
    for q in range(2):
        b_pair = conv[:, INNER + 128 * q : INNER + 128 * q + 128]
        c_pair = conv[:, INNER + 256 + 128 * q : INNER + 256 + 128 * q + 128]
        for g in range(2):
            c_one = jnp.where(low_half == (g == 0), c_pair, jnp.zeros_like(c_pair))
            scores = dot_nt(c_one, b_pair)
            for i in range(2):
                first = 8 * q + 4 * g + 2 * i
                x_pair = conv[:, 64 * first : 64 * first + 128]
                total = None
                for h in (first, first + 1):
                    gap = jnp.where(
                        causal, cum_col[:, h : h + 1] - cum_row[h : h + 1, :], -1e30
                    )
                    mixing = (scores * jnp.exp(gap) * step[h : h + 1, :]).astype(BF16)
                    x_one = jnp.where(low_half == (h == first), x_pair, jnp.zeros_like(x_pair))
                    term = dot(mixing, x_one)
                    total = term if total is None else total + term
                inside[:, 64 * first : 64 * first + 128] = total

    def placing_rows(j):
        ids, shares = names[j], parts[j]
        expert = iota((16, TOK), 0)
        first, second = expert == ids[0:1, :], expert == ids[1:2, :]
        named = first | second
        share = jnp.where(first, shares[0:1, :], 0.0) + jnp.where(second, shares[1:2, :], 0.0)
        before = (later < sooner).astype(BF16)
        rank = dot(named.astype(F32).astype(BF16), before)
        rank = jnp.where(named, rank, -1.0)
        slot = iota((SLOTS, TOK), 0).astype(F32)
        chosen = jnp.concatenate(
            [(rank[e : e + 1, :] == slot).astype(F32) for e in range(16)], axis=0
        )
        weights = jnp.concatenate(
            [
                jnp.where(rank[e : e + 1, :] == slot, share[e : e + 1, :], 0.0)
                for e in range(16)
            ],
            axis=0,
        )
        placing[j] = chosen.astype(BF16)
        rest = weights.T
        for k in range(2):
            piece = rest.astype(BF16)
            weighing[j, pl.ds(TOK * k, TOK), :] = piece
            rest = rest - piece.astype(F32)

    placing_rows(0)
    for copy in notes:
        copy.wait_recv()
    for j in range(1, 4):
        placing_rows(j)

    def wait_state(o):
        decay_copy(o).wait_recv()
        state_copy(o).wait_recv()

    each(1, 16, wait_state)

    def advance(j, held):
        entering[j] = held.astype(BF16)
        return decay_in[j] * held + state_in[j].astype(F32)

    lax.fori_loop(0, 16, advance, jnp.zeros((16, 256), F32))

    def enter_copy(o):
        rows, cols = place_of(sp)
        return pltpu.make_async_remote_copy(
            src_ref=entering.at[ahead(o)],
            dst_ref=entered.at[rows, cols],
            send_sem=enter_send.at[o],
            recv_sem=enter_recv.at[o],
            device_id=(ahead(o), dp),
            device_id_type=MESH,
        )

    each(1, 16, lambda o: enter_copy(o).start())
    entered[my_rows, my_cols] = entering[sp]
    reach_wide = dot(thirds(jnp.exp(cum_col)), spread)
    each(1, 16, lambda o: enter_copy(o).wait_recv())

    for copy in late_loads:
        copy.wait()
    nothing = jnp.zeros((64, 256), BF16)
    blocks = []
    for q in range(2):
        c_pair = conv[:, INNER + 256 + 128 * q : INNER + 256 + 128 * q + 128]
        low, high = entered[:, 512 * q : 512 * q + 256], entered[:, 512 * q + 256 : 512 * q + 512]
        both = jnp.concatenate(
            [
                jnp.concatenate([low, nothing], axis=1),
                jnp.concatenate([nothing, high], axis=1),
            ],
            axis=0,
        )
        carried = dot(c_pair, both)
        for g in range(2):
            low_col = 512 * q + 256 * g
            mixed = (
                inside[:, low_col : low_col + 256]
                + reach_wide[:, low_col : low_col + 256] * carried[:, 256 * g : 256 * g + 256]
            ).astype(BF16)
            gated = mixed.astype(F32) * jax.nn.silu(valve[:, low_col : low_col + 256].astype(F32))
            level = lax.rsqrt(jnp.mean(gated * gated, axis=1, keepdims=True) + rms_eps)
            blocks.append(
                (gated * level * group_gain[:, low_col : low_col + 256]).astype(BF16)
            )
    group_normed = jnp.concatenate(blocks, axis=1)
    out_load.wait()

    def project(k):
        cols = pl.ds(512 * k, 512)
        pre[:, cols] = skip[:, cols].astype(F32) + dot(group_normed, out_v[:, cols])

    for k in range(width // 512):
        project(k)

    def standardize(k):
        rows = pl.ds(64 * k, 64)
        block = pre[rows, :]
        shifted = block - jnp.mean(block, axis=1, keepdims=True)
        level = lax.rsqrt(jnp.mean(shifted * shifted, axis=1, keepdims=True) + norm_eps)
        normed[rows, :] = (shifted * level * gain[...] + offset[...]).astype(BF16)

    far_cols = pl.ds(NEAR, width - NEAR)

    def token_copy(lane, half):
        rows = pl.ds(64 * half, 64)
        if lane < 2:
            source = normed.at[rows, far_cols]
        else:
            source = tokens.at[half, rows]
        return pltpu.make_async_remote_copy(
            src_ref=source,
            dst_ref=tokens.at[lane, rows],
            send_sem=token_send.at[lane, half],
            recv_sem=token_recv.at[lane, half],
            device_id=(right, left, (right, left)[half])[lane],
            device_id_type=MESH,
        )

    standardize(0)
    token_copy(0, 0).start()
    token_copy(1, 0).start()
    standardize(1)
    token_copy(1, 1).start()
    token_copy(0, 1).start()
    flat_outgoing = outgoing.reshape(16 * SLOTS, width)

    def route(k):
        cols = pl.ds(256 * k, 256)
        flat_outgoing[:, cols] = dot(placing[0], normed[:, cols]).astype(BF16)

    for k in range(NEAR // 256):
        route(k)

    near_cols = pl.ds(0, NEAR)
    near_back = pl.ds(0, NEAR_BACK)
    far_back = pl.ds(NEAR_BACK, width - NEAR_BACK)

    def go(o, side=0):
        cols = (near_cols, far_cols)[side]
        return pltpu.make_async_remote_copy(
            src_ref=outgoing.at[pl.ds(3 * ahead(o), 3), :, cols],
            dst_ref=gathered.at[0, pl.ds(3 * o, 3), :, cols],
            send_sem=go_send.at[side, o],
            recv_sem=go_recv.at[side, o],
            device_id=(ahead(o), dp),
            device_id_type=MESH,
        )

    each(1, 16, lambda o: go(o).start())
    for k in range(NEAR // 256, width // 256):
        route(k)
    each(1, 16, lambda o: go(o, 1).start())
    gathered[0, 0:3] = outgoing[pl.ds(3 * sp, 3)]

    def group(g):
        return pl.ds(12 * g, 12)

    def ring(src_slot, dst_slot, g, target, lane):
        return pltpu.make_async_remote_copy(
            src_ref=gathered.at[src_slot, group(g), :, near_cols],
            dst_ref=gathered.at[dst_slot, group(g), :, near_cols],
            send_sem=ring_send.at[lane, g],
            recv_sem=ring_recv.at[dst_slot - 1, g],
            device_id=target,
            device_id_type=MESH,
        )

    def to_right(g):
        return ring(0, 1, g, right, 0)

    def to_left(g):
        return ring(0, 2, g, left, 1)

    def onward(g):
        return ring(1, 3, g, right, 2) if g < 2 else ring(2, 3, g, left, 2)

    def far_copy(j, o):
        return pltpu.make_async_remote_copy(
            src_ref=far_rows.at[j - 1, pl.ds(3 * ahead(o), 3)],
            dst_ref=gathered.at[j, pl.ds(3 * o, 3), :, far_cols],
            send_sem=far_send.at[j - 1, o],
            recv_sem=far_recv.at[j - 1, o],
            device_id=(ahead(o), dp),
            device_id_type=MESH,
        )

    def route_far(j):
        flat = far_rows.at[j - 1].reshape(16 * SLOTS, width - NEAR)
        flat[...] = dot(placing[j], tokens[j - 1]).astype(BF16)
        gathered[j, 0:3, :, NEAR:] = far_rows[j - 1, pl.ds(3 * sp, 3)]

    def send_far(j, half):
        each(max(8 * half, 1), 8 * half + 8, lambda o: far_copy(j, o).start())

    def wait_far(j, half):
        each(max(8 * half, 1), 8 * half + 8, lambda o: far_copy(j, o).wait_recv())

    def pass_on(g):
        each(max(4 * g, 1), 4 * g + 4, lambda o: go(o).wait_recv())
        to_right(g).start()
        to_left(g).start()

    token_copy(0, 0).wait_recv()
    token_copy(2, 0).start()
    token_copy(1, 1).wait_recv()
    token_copy(2, 1).start()
    token_copy(0, 1).wait_recv()
    route_far(1)
    send_far(1, 0)
    token_copy(1, 0).wait_recv()
    route_far(2)
    send_far(2, 0)
    send_far(2, 1)
    send_far(1, 1)
    pass_on(0)
    token_copy(2, 0).wait_recv()
    token_copy(2, 1).wait_recv()
    route_far(3)
    send_far(3, 0)
    send_far(3, 1)
    pass_on(1)
    pass_on(2)
    pass_on(3)
    for copy in loads:
        copy.wait()
    for copy in gifts:
        copy.wait()
    each(1, 8, lambda o: go(o, 1).wait_recv())

    tile = 256

    def home_copy(j, o):
        return pltpu.make_async_remote_copy(
            src_ref=partial.at[j, pl.ds(3 * o, 3), :, far_back],
            dst_ref=far_answers.at[j, pl.ds(3 * sp, 3)],
            send_sem=home_send.at[j, o],
            recv_sem=home_recv.at[j, o],
            device_id=(behind(o), dp),
            device_id_type=MESH,
        )

    def unit(slot, half):
        block = gathered.at[slot, pl.ds(24 * half, 24)].reshape(192, width)
        for k in range(2 * part // tile):
            cols = pl.ds(k * tile, tile)
            gate_val = dot(block[...], gate_v[:, cols])
            up_val = dot(block[...], raise_v[:, cols])
            hidden[:, cols] = (jax.nn.silu(gate_val) * up_val).astype(BF16)
        target = partial.at[slot, pl.ds(24 * half, 24)].reshape(192, width)
        for k in range(width // tile):
            cols = pl.ds(k * tile, tile)
            target[:, cols] = dot(hidden[...], lower_v[:, cols]).astype(BF16)
        each(jnp.maximum(8 * half, 1), 8 * half + 8, lambda o: home_copy(slot, o).start())

        @pl.when(half == 0)
        def _():
            far_answers[slot, pl.ds(3 * sp, 3)] = partial[slot, 0:3, :, NEAR_BACK:]

    def sum_direct(slot, g):
        side = 0 if slot == 2 else 1
        return pltpu.make_async_remote_copy(
            src_ref=partial.at[slot, group(g), :, near_back],
            dst_ref=summed.at[side, group(g)],
            send_sem=sum_send.at[side, g],
            recv_sem=sum_recv.at[side, g],
            device_id=right if slot == 2 else left,
            device_id_type=MESH,
        )

    def sum_relay(g):
        return pltpu.make_async_remote_copy(
            src_ref=partial.at[3, group(g), :, near_back],
            dst_ref=relayed.at[group(g)],
            send_sem=sum_send.at[2, g],
            recv_sem=sum_recv.at[2, g],
            device_id=right if g < 2 else left,
            device_id_type=MESH,
        )

    def combine(j):
        each(1, 16, lambda o: home_copy(j, o).wait_recv())
        flat = far_answers.at[j].reshape(16 * SLOTS, width - NEAR_BACK)
        terms = dot(weighing[j], flat[...])
        return terms[0:TOK] + terms[TOK : 2 * TOK]

    def tsum_copy(lane, half):
        rows = pl.ds(64 * half, 64)
        if lane == 2:
            source, target = token_out.at[2, rows], token_relay.at[rows]
            device = (right, left)[half]
        else:
            source, target = token_out.at[lane, rows], token_in.at[lane, rows]
            device = (right, left)[lane]
        return pltpu.make_async_remote_copy(
            src_ref=source,
            dst_ref=target,
            send_sem=tsum_send.at[lane, half],
            recv_sem=tsum_recv.at[lane, half],
            device_id=device,
            device_id_type=MESH,
        )

    def relay_add(g):
        slot = 2 if g < 2 else 1
        sum_relay(g).wait_recv()
        partial[slot, group(g), :, 0:NEAR_BACK] = (
            partial[slot, group(g), :, 0:NEAR_BACK].astype(F32) + relayed[group(g)].astype(F32)
        ).astype(BF16)
        sum_direct(slot, g).start()

    def before_own():
        each(8, 16, lambda o: go(o, 1).wait_recv())
        to_right(0).wait_recv()
        onward(0).start()

    def before_left():
        to_right(1).wait_recv()
        onward(1).start()
        wait_far(1, 0)

    def before_right():
        to_left(0).wait_recv()
        to_left(1).wait_recv()
        to_left(2).wait_recv()
        onward(2).start()
        wait_far(2, 0)

    def before_right_rest():
        to_left(3).wait_recv()
        onward(3).start()
        sum_direct(1, 0).start()
        sum_direct(1, 1).start()
        wait_far(2, 1)

    def before_left_rest():
        sum_direct(2, 2).start()
        sum_direct(2, 3).start()
        to_right(2).wait_recv()
        to_right(3).wait_recv()
        wait_far(1, 1)

    def before_across():
        onward(0).wait_recv()
        onward(1).wait_recv()
        wait_far(3, 0)

    def before_across_rest():
        sum_relay(0).start()
        sum_relay(1).start()
        onward(2).wait_recv()
        onward(3).wait_recv()
        wait_far(3, 1)

    befores = (
        before_own, before_left, before_right, before_right_rest, before_left_rest,
        before_across, before_across_rest,
    )

    def turn(u):
        for k, before in enumerate(befores):
            pl.when(u == k + 1)(before)
        slot = jnp.where(u < 2, 0, jnp.where(u >= 6, 3, jnp.where((u == 2) | (u == 5), 1, 2)))
        half = jnp.where((u == 1) | (u == 4) | (u == 5) | (u == 7), 1, 0)
        unit(slot, half)

    each(0, 8, turn)
    sum_relay(2).start()
    sum_relay(3).start()
    relay_add(0)
    relay_add(2)
    relay_add(1)
    relay_add(3)
    token_out[0] = combine(2).astype(BF16)
    tsum_copy(0, 1).start()
    token_out[1] = combine(1).astype(BF16)
    tsum_copy(1, 0).start()

    def back(o):
        return pltpu.make_async_remote_copy(
            src_ref=partial.at[0, pl.ds(3 * o, 3), :, near_back],
            dst_ref=answers.at[pl.ds(3 * sp, 3)],
            send_sem=back_send.at[o],
            recv_sem=back_recv.at[o],
            device_id=(behind(o), dp),
            device_id_type=MESH,
        )

    def settle(g):
        sum_direct(2, g).wait_recv()
        sum_direct(1, g).wait_recv()
        partial[0, group(g), :, 0:NEAR_BACK] = (
            partial[0, group(g), :, 0:NEAR_BACK].astype(F32)
            + summed[0, group(g)].astype(F32)
            + summed[1, group(g)].astype(F32)
        ).astype(BF16)
        each(max(4 * g, 1), 4 * g + 4, lambda o: back(o).start())
        if g == 0:
            answers[pl.ds(3 * sp, 3)] = partial[0, 0:3, :, 0:NEAR_BACK]

    token_out[2] = combine(3).astype(BF16)
    tsum_copy(2, 0).start()
    tsum_copy(2, 1).start()
    settle(0)
    settle(2)

    def drain_early(o):
        step_copy(o, steps_out, steps, 0).wait_send()
        step_copy(o, fades_out, fades, 1).wait_send()
        decay_copy(o).wait_send()
        state_copy(o).wait_send()
        enter_copy(o).wait_send()
        go(o).wait_send()
        go(o, 1).wait_send()
        for j in range(1, 4):
            far_copy(j, o).wait_send()

    each(1, 16, drain_early)
    settle(1)
    settle(3)
    for half in range(2):
        lane, rows = half, pl.ds(64 * half, 64)
        tsum_copy(2, half).wait_recv()
        token_out[lane, rows] = (
            token_out[lane, rows].astype(F32) + token_relay[rows].astype(F32)
        ).astype(BF16)
        tsum_copy(lane, half).start()

    token_sum[...] = combine(0)
    for copy in rims + notes:
        copy.wait_send()
    for lane in range(3):
        for half in range(2):
            token_copy(lane, half).wait_send()
            tsum_copy(lane, half).wait_send()
            if lane < 2:
                tsum_copy(lane, half).wait_recv()
    result[:, NEAR_BACK:] = (
        normed[:, NEAR_BACK:].astype(F32)
        + token_sum[...]
        + token_in[0].astype(F32)
        + token_in[1].astype(F32)
    ).astype(BF16)
    for g in range(4):
        to_right(g).wait_send()
        to_left(g).wait_send()
        onward(g).wait_send()
        sum_direct(1, g).wait_send()
        sum_direct(2, g).wait_send()
        sum_relay(g).wait_send()

    each(1, 16, lambda o: back(o).wait_recv())
    flat_answers = answers.reshape(16 * SLOTS, NEAR_BACK)

    def finish(k, size):
        cols = pl.ds(k, size)
        terms = dot(weighing[0], flat_answers[:, cols])
        routed = terms[0:TOK] + terms[TOK : 2 * TOK]
        result[:, cols] = (normed[:, cols].astype(F32) + routed).astype(BF16)

    for k in range(0, NEAR_BACK, 512):
        finish(k, min(512, NEAR_BACK - k))

    def drain(o):
        for j in range(4):
            home_copy(j, o).wait_send()
        back(o).wait_send()

    each(1, 16, drain)


def per_device(
    skip_connection_stream,
    emitted_valve_unscaled,
    channel_source_mapped,
    hidden_source_mapped,
    probe_mapped_values,
    increment_premapped,
    extra_log_fading,
    channel_fading_speed,
    channel_source_kernel,
    hidden_source_kernel,
    probe_kernel_coefficients,
    cluster_scaling_factor,
    emitted_mapping_matrix,
    standardize_scaling,
    standardize_offset,
    chosen_specialist_ids,
    specialist_mixing_shares,
    specialist_gating_matrices,
    raising_matrices,
    lowering_matrices,
):
    width = skip_connection_stream.shape[2]
    part = specialist_gating_matrices.shape[2]
    far = pl.BlockSpec(memory_space=pl.ANY)
    near = pl.BlockSpec(memory_space=pltpu.VMEM)
    dma = pltpu.SemaphoreType.DMA
    rows = 2 * SLOTS
    rest = width - NEAR_BACK
    out = pl.pallas_call(
        layer_kernel,
        out_shape=pltpu.VMEM((TOK, width), BF16),
        in_specs=[far] * 20,
        out_specs=near,
        scratch_shapes=[
            pltpu.SMEM((HEADS,), F32),
            pltpu.VMEM((4, INNER), F32),
            pltpu.VMEM((4, 256), F32),
            pltpu.VMEM((4, 256), F32),
            pltpu.VMEM((1, INNER), F32),
            pltpu.VMEM((1, width), F32),
            pltpu.VMEM((1, width), F32),
            pltpu.VMEM((TOK, width), BF16),
            pltpu.VMEM((TOK, INNER), BF16),
            pltpu.VMEM((16, 8, 1536), BF16),
            pltpu.VMEM((1, 8, 1536), BF16),
            pltpu.VMEM((HEADS, 1, TOK), F32),
            pltpu.VMEM((HEADS, 1, TOK), F32),
            pltpu.VMEM((HEADS, 1, TOK), F32),
            pltpu.VMEM((HEADS, 1, TOK), F32),
            pltpu.VMEM((4, 2, TOK), jnp.int32),
            pltpu.VMEM((4, 2, TOK), F32),
            pltpu.VMEM((TOK, 1536), BF16),
            pltpu.VMEM((64, INNER), BF16),
            pltpu.VMEM((4, 1, 256), F32),
            pltpu.VMEM((16, 16, 256), BF16),
            pltpu.VMEM((16, 1, 256), F32),
            pltpu.VMEM((16, 16, 256), BF16),
            pltpu.VMEM((64, INNER), BF16),
            pltpu.VMEM((TOK, INNER), F32),
            pltpu.VMEM((INNER, width), BF16),
            pltpu.VMEM((TOK, width), F32),
            pltpu.VMEM((TOK, width), BF16),
            pltpu.VMEM((4, 16 * SLOTS, TOK), BF16),
            pltpu.VMEM((4, 2 * TOK, 16 * SLOTS), BF16),
            pltpu.VMEM((rows, 8, width), BF16),
            pltpu.VMEM((rows, 8, NEAR_BACK), BF16),
            pltpu.VMEM((3, TOK, width - NEAR), BF16),
            pltpu.VMEM((3, rows, 8, width - NEAR), BF16),
            pltpu.VMEM((4, rows, 8, rest), BF16),
            pltpu.VMEM((TOK, rest), F32),
            pltpu.VMEM((3, TOK, rest), BF16),
            pltpu.VMEM((TOK, rest), BF16),
            pltpu.VMEM((2, TOK, rest), BF16),
            pltpu.VMEM((4, rows, 8, width), BF16),
            pltpu.VMEM((4, rows, 8, width), BF16),
            pltpu.VMEM((rows, 8, NEAR_BACK), BF16),
            pltpu.VMEM((2, rows, 8, NEAR_BACK), BF16),
            pltpu.VMEM((width, 2 * part), BF16),
            pltpu.VMEM((width, 2 * part), BF16),
            pltpu.VMEM((2 * part, width), BF16),
            pltpu.VMEM((192, 2 * part), BF16),
            dma((17,)), dma((3,)), dma((3,)), dma((2, 3)), dma((2, 3)), dma((2, 16)), dma((2, 16)), dma((2, 16)), dma((2, 16)),
            dma((16,)), dma((16,)), dma((3,)), dma((3,)), dma((3,)), dma((2, 16)), dma((2, 16)),
            dma((3, 4)), dma((3, 4)), dma((3, 4)), dma((3, 4)), dma((16,)), dma((16,)),
            dma((3, 2)), dma((3, 2)), dma((3, 16)), dma((3, 16)), dma((4, 16)), dma((4, 16)),
            dma((3, 2)), dma((3, 2)),
        ],
        compiler_params=pltpu.CompilerParams(
            collective_id=0, has_side_effects=True, vmem_limit_bytes=62 * 1024 * 1024
        ),
        name="layer",
    )(
        channel_fading_speed,
        skip_connection_stream[0],
        emitted_valve_unscaled[0],
        channel_source_mapped.reshape(16, 8, INNER),
        hidden_source_mapped.reshape(16, 8, 256),
        probe_mapped_values.reshape(16, 8, 256),
        increment_premapped.reshape(16, 1, TOK),
        extra_log_fading.reshape(16, 1, TOK),
        channel_source_kernel,
        hidden_source_kernel,
        probe_kernel_coefficients,
        cluster_scaling_factor[None, :],
        emitted_mapping_matrix,
        standardize_scaling[None, :],
        standardize_offset[None, :],
        chosen_specialist_ids[0].T,
        specialist_mixing_shares[0].T,
        specialist_gating_matrices[0],
        raising_matrices[0],
        lowering_matrices[0],
    )
    return out[None]


def solution(mesh):
    placed = (
        P("dp", "sp", None),
        P("dp", "sp", None),
        P("dp", "sp", None),
        P("dp", "sp", None),
        P("dp", "sp", None),
        P("dp", None, "sp"),
        P("dp", None, "sp"),
        P(),
        P(),
        P(),
        P(),
        P(),
        P(),
        P(),
        P(),
        P("dp", "sp", None),
        P("dp", "sp", None),
        P("sp", None, "dp"),
        P("sp", None, "dp"),
        P("sp", "dp", None),
    )
    return jax.shard_map(
        per_device, mesh=mesh, in_specs=placed, out_specs=P("dp", "sp", None), check_vma=False
    )
```
